32 devices in a mesh: sp: 16 (over z, y, x), tp: 2 (over core).
Axes of the slice: x: 2, y: 2, z: 4, core: 2. Of those that a mesh axis runs over, the one named last changes fastest.
Arguments:
- tokens: bfloat16 [2048, 2048], P('sp', 'tp'), may hold values from -6 to 6
- norm_gain: float32 [2048], replicated, may hold values from 0.1 to 1.9
- w_value: bfloat16 [2048, 2048], P('sp', 'tp'), may hold values from -0.125 to 0.125
- w_gate: bfloat16 [2048, 2048], P('sp', 'tp'), may hold values from -0.125 to 0.125
- conv_taps: bfloat16 [31, 2048], P(None, 'tp'), may hold values from -1 to 1
- conv_gain: float32 [2048], P('tp'), may hold values from 0.1 to 1.9
- w_query: bfloat16 [2048, 3072], P(None, 'tp'), may hold values from -5.303301 to 5.303301
- latent_down_weight: bfloat16 [2048, 512], P('sp'), may hold values from -0.125 to 0.125
- latent_norm_gain: float32 [512], replicated, may hold values from 0.1 to 1.9
- w_rope_key: bfloat16 [2048, 64], P('sp'), may hold values from -0.125 to 0.125
- key_up_weight: bfloat16 [512, 2048], P(None, 'tp'), may hold values from -0.5 to 0.5
- value_up_weight: bfloat16 [512, 2048], P(None, 'tp'), may hold values from -0.25 to 0.25
- w_merge_conv: bfloat16 [2048, 2048], P('tp'), may hold values from -0.09375 to 0.09375
- w_merge_attn: bfloat16 [2048, 2048], P('tp'), may hold values from -0.28125 to 0.28125
Outputs:
- merged: bfloat16 [2048, 2048], P(('sp', 'tp'))
- log_sums: float32 [2048, 16], P('sp', 'tp')
The draws below stay inside these ranges and needn't reach their ends.
All inputs are finite; a program needn't handle non-finite values.
Results may differ from the reference program's by a relative error of at most 0.025.
The reference program's roundings to bfloat16 on the way count: a program that leaves them out, or rounds other values in their place, can miss the bound.
Values may be sent and summed in bfloat16 or wider, within the bound.
No kernel may reach another device: no remote copies, remote signals or barrier semaphores. Data moves between devices by JAX's collectives and lax.ppermute only.
A program may use at most 64 MiB of HBM per device.

```python
import jax
import jax.numpy as jnp
from jax import lax

MODEL_WIDTH = 2048
CC = 2048
HEAD_TOTAL = 16
KEY_VALUE_RANK = 512
PLAIN_QK_WIDTH = 128
QK_ROPE = 64
VALUE_HEAD_WIDTH = 128
CONV_WIDTH = 31
TOKEN_TOTAL = 2048
N_TP = 2


def draw_w_query(key, part):
    values = jnp.clip(jax.random.normal(key, (MODEL_WIDTH, HEAD_TOTAL * (PLAIN_QK_WIDTH + QK_ROPE)), jnp.float32), -6.0, 6.0) * MODEL_WIDTH ** (-0.5)
    return values.astype(jnp.bfloat16)


def block_scale(rng, shape, split, smallest, largest):
    level, own = 1.0, jax.random.fold_in(rng, 6)
    for axis_at, blocks in split:
        heights = jnp.exp(jax.random.uniform(jax.random.fold_in(own, axis_at), (blocks,), jnp.float32, smallest / len(split), largest / len(split)))
        level = level * jnp.repeat(heights, shape[axis_at] // blocks).reshape([-1 if axis == axis_at else 1 for axis in range(len(shape))])
    return level


def normal_values(own_key, extent, scale, limit, pieces=(), held_as=jnp.bfloat16):
    array = scale * jax.random.normal(own_key, extent, jnp.float32)
    if pieces:
        array = array * block_scale(own_key, extent, pieces, -0.22, 0.18)
    return jnp.clip(array, -limit, limit).astype(held_as)


def setup_inputs(seed: int = 0) -> dict:
    seeds = jax.random.split(jax.random.key(seed), 15)
    return {
        "tokens": normal_values(seeds[0], (TOKEN_TOTAL, MODEL_WIDTH), 1.0, 6.0, ((0, 16), (1, 2))),
        "norm_gain": jnp.clip(1.0 + 0.18 * jax.random.normal(seeds[1], (MODEL_WIDTH,), jnp.float32), 0.1, 1.9),
        "w_value": normal_values(seeds[2], (MODEL_WIDTH, CC), MODEL_WIDTH ** -0.5, 0.125, ((0, 16), (1, 2))),
        "w_gate": normal_values(seeds[3], (MODEL_WIDTH, CC), MODEL_WIDTH ** -0.5, 0.125, ((0, 16), (1, 2))),
        "conv_taps": normal_values(seeds[4], (CONV_WIDTH, CC), CONV_WIDTH ** -0.5, 1.0, ((1, 2),)),
        "conv_gain": jnp.clip(1.0 + 0.18 * jax.random.normal(seeds[5], (CC,), jnp.float32), 0.1, 1.9),
        "w_query": draw_w_query(jax.random.fold_in(seeds[14], 71), 0),
        "latent_down_weight": normal_values(seeds[7], (MODEL_WIDTH, KEY_VALUE_RANK), MODEL_WIDTH ** -0.5, 0.125, ((0, 16),)),
        "latent_norm_gain": jnp.clip(1.0 + 0.18 * jax.random.normal(seeds[8], (KEY_VALUE_RANK,), jnp.float32), 0.1, 1.9),
        "w_rope_key": normal_values(seeds[9], (MODEL_WIDTH, QK_ROPE), MODEL_WIDTH ** -0.5, 0.125, ((0, 16),)),
        "key_up_weight": normal_values(seeds[10], (KEY_VALUE_RANK, HEAD_TOTAL * PLAIN_QK_WIDTH), PLAIN_QK_WIDTH ** -0.5, 0.5, ((1, 2),)),
        "value_up_weight": normal_values(seeds[11], (KEY_VALUE_RANK, HEAD_TOTAL * VALUE_HEAD_WIDTH), KEY_VALUE_RANK ** -0.5, 0.25, ((1, 2),)),
        "w_merge_conv": normal_values(seeds[12], (CC, MODEL_WIDTH), (CC + HEAD_TOTAL * VALUE_HEAD_WIDTH) ** -0.5, 0.09375, ((0, 2),)),
        "w_merge_attn": normal_values(seeds[13], (HEAD_TOTAL * VALUE_HEAD_WIDTH, MODEL_WIDTH), (3.0 / (CC + HEAD_TOTAL * VALUE_HEAD_WIDTH) ** 0.5), 0.28125, ((0, 2),)),
    }


epsilon = 1e-06
rope_base = 10000.0
masked_score = -1e+30

def angles_at(positions, width):
    inverse = rope_base ** (-2.0 * jnp.arange(width // 2, dtype=jnp.float32) / width)
    return positions[:, None] * inverse[None, :]

def rotate(halves, angle):
    middle = halves.shape[-1] // 2
    first, second = (halves[..., :middle], halves[..., middle:])
    cosine, sine = (jnp.cos(angle), jnp.sin(angle))
    return jnp.concatenate([first * cosine - second * sine, first * sine + second * cosine], axis=-1)

def reference(tokens, norm_gain, w_value, w_gate, conv_taps, conv_gain, w_query, latent_down_weight, latent_norm_gain, w_rope_key, key_up_weight, value_up_weight, w_merge_conv, w_merge_attn):
    features = tokens.astype(jnp.float32)
    normed = (features * lax.rsqrt(lax.optimization_barrier(jnp.mean(features * features, axis=-1, keepdims=True)) + epsilon) * norm_gain).astype(jnp.bfloat16)
    value_pre = jnp.dot(normed, w_value, preferred_element_type=jnp.float32)
    gate_pre = jnp.dot(normed, w_gate, preferred_element_type=jnp.float32)
    gated_rows = (value_pre * jax.nn.sigmoid(gate_pre)).astype(jnp.bfloat16)
    conv_reach = CONV_WIDTH - 1
    padded = jnp.concatenate([jnp.zeros((conv_reach, CC), jnp.bfloat16), gated_rows], axis=0).astype(jnp.float32)
    mixed = jnp.zeros((TOKEN_TOTAL, CC), jnp.float32)
    for tap_index in range(CONV_WIDTH):
        mixed = mixed + conv_taps[tap_index].astype(jnp.float32) * padded[tap_index:tap_index + TOKEN_TOTAL]
    channel_mean = lax.optimization_barrier(jnp.mean(mixed, axis=-1, keepdims=True))
    channel_var = lax.optimization_barrier(jnp.mean(jnp.square(mixed - channel_mean), axis=-1, keepdims=True))
    conv_out = jax.nn.silu((mixed - channel_mean) * lax.rsqrt(channel_var + epsilon) * conv_gain).astype(jnp.bfloat16)
    positions = jnp.arange(TOKEN_TOTAL, dtype=jnp.float32)
    rope_angles = angles_at(positions, QK_ROPE)
    query = jnp.dot(normed, w_query, preferred_element_type=jnp.float32).astype(jnp.bfloat16).reshape(TOKEN_TOTAL, HEAD_TOTAL, PLAIN_QK_WIDTH + QK_ROPE)
    query_rope = rotate(query[..., PLAIN_QK_WIDTH:].astype(jnp.float32), rope_angles[:, None, :]).astype(jnp.bfloat16)
    key_expanded = key_up_weight.astype(jnp.float32).reshape(KEY_VALUE_RANK, HEAD_TOTAL, PLAIN_QK_WIDTH)
    query_latent = jnp.einsum('thd,lhd->thl', query[..., :PLAIN_QK_WIDTH].astype(jnp.float32), key_expanded).astype(jnp.bfloat16)
    latent_pre = jnp.dot(normed, latent_down_weight, preferred_element_type=jnp.float32)
    latent = (latent_pre * lax.rsqrt(lax.optimization_barrier(jnp.mean(latent_pre * latent_pre, axis=-1, keepdims=True)) + epsilon) * latent_norm_gain).astype(jnp.bfloat16)
    key_rope = rotate(jnp.dot(normed, w_rope_key, preferred_element_type=jnp.float32), rope_angles).astype(jnp.bfloat16)
    score_scale = (PLAIN_QK_WIDTH + QK_ROPE) ** (-0.5)
    query_block = min(512, TOKEN_TOTAL)
    key_index = jnp.arange(TOKEN_TOTAL, dtype=jnp.int32)
    latent_wide = latent.astype(jnp.float32)
    rope_wide = key_rope.astype(jnp.float32)

    def one_block(block_start):
        block_latent = lax.dynamic_slice_in_dim(query_latent, block_start, query_block, 0).astype(jnp.float32)
        block_rope = lax.dynamic_slice_in_dim(query_rope, block_start, query_block, 0).astype(jnp.float32)
        scores = (jnp.einsum('thl,kl->thk', block_latent, latent_wide) + jnp.einsum('thr,kr->thk', block_rope, rope_wide)) * score_scale
        query_index = block_start + jnp.arange(query_block, dtype=jnp.int32)
        allowed = key_index[None, None, :] <= query_index[:, None, None]
        scores = jnp.where(allowed, scores, masked_score)
        row_max = lax.optimization_barrier(jnp.max(scores, axis=-1))
        weights = jnp.where(allowed, jnp.exp(scores - row_max[..., None]), 0.0)
        weight_sum = lax.optimization_barrier(jnp.sum(weights, axis=-1))
        weighted = jnp.einsum('thk,kl->thl', weights.astype(jnp.bfloat16).astype(jnp.float32), latent_wide)
        return ((weighted / weight_sum[..., None]).astype(jnp.bfloat16), row_max + jnp.log(weight_sum))
    block_starts = jnp.arange(TOKEN_TOTAL // query_block, dtype=jnp.int32) * query_block
    latent_result, log_sums = lax.map(one_block, block_starts)
    latent_result = latent_result.reshape(TOKEN_TOTAL, HEAD_TOTAL, KEY_VALUE_RANK)
    log_sums = log_sums.reshape(TOKEN_TOTAL, HEAD_TOTAL)
    value_expanded = value_up_weight.astype(jnp.float32).reshape(KEY_VALUE_RANK, HEAD_TOTAL, VALUE_HEAD_WIDTH)
    attention = jnp.einsum('thl,lhv->thv', latent_result.astype(jnp.float32), value_expanded).astype(jnp.bfloat16).reshape(TOKEN_TOTAL, HEAD_TOTAL * VALUE_HEAD_WIDTH)
    channel_share = CC // N_TP
    head_share = HEAD_TOTAL * VALUE_HEAD_WIDTH // N_TP
    merged = jnp.zeros((TOKEN_TOTAL, MODEL_WIDTH), jnp.float32)
    for group_index in range(N_TP):
        channel_part = conv_out[:, group_index * channel_share:(group_index + 1) * channel_share]
        head_part = attention[:, group_index * head_share:(group_index + 1) * head_share]
        partial_value = jnp.dot(channel_part, w_merge_conv[group_index * channel_share:(group_index + 1) * channel_share], preferred_element_type=jnp.float32)
        partial_value = partial_value + jnp.dot(head_part, w_merge_attn[group_index * head_share:(group_index + 1) * head_share], preferred_element_type=jnp.float32)
        merged = merged + partial_value.astype(jnp.bfloat16).astype(jnp.float32)
    return (merged.astype(jnp.bfloat16), log_sums)
```

```python
import functools
import math

import jax
import jax.numpy as jnp
from jax import lax
from jax.experimental import pallas as pl
from jax.experimental.pallas import tpu as pltpu
from jax.sharding import PartitionSpec as P

PLAIN_QK_WIDTH = 128
QK_ROPE = 64
VALUE_HEAD_WIDTH = 128


epsilon = 1e-06
rope_base = 10000.0
masked_score = -1e30


def angles_at(positions, width):
    inverse = rope_base ** (-2.0 * jnp.arange(width // 2, dtype=jnp.float32) / width)
    return positions[:, None] * inverse[None, :]


def rotate(halves, angle):
    middle = halves.shape[-1] // 2
    first, second = (halves[..., :middle], halves[..., middle:])
    cosine, sine = (jnp.cos(angle), jnp.sin(angle))
    return jnp.concatenate(
        [first * cosine - second * sine, first * sine + second * cosine], axis=-1
    )


class Place:
    def __init__(self):
        self.sp_count = lax.axis_size("sp")
        self.tp_count = lax.axis_size("tp")
        self.inner = math.gcd(self.sp_count, 4)
        self.outer = self.sp_count // self.inner

    def indices(self):
        index = lax.axis_index("sp")
        return index // self.inner, index % self.inner, lax.axis_index("tp")

    def outer_shift(self, block, distance):
        route = [
            (i, ((i // self.inner + distance) % self.outer) * self.inner + i % self.inner)
            for i in range(self.sp_count)
        ]
        return lax.ppermute(block, "sp", route)

    def inner_swap(self, block, mask):
        return lax.ppermute(block, "sp", [(i, i ^ mask) for i in range(self.sp_count)])

    def tp_shift(self, block, distance):
        route = [(i, (i + distance) % self.tp_count) for i in range(self.tp_count)]
        return lax.ppermute(block, "tp", route)

    def outer_gather(self, block):
        return [block] + [self.outer_shift(block, j) for j in range(1, self.outer)]

    def inner_gather(self, block):
        return [block] + [self.inner_swap(block, k) for k in range(1, self.inner)]

    def tp_gather(self, blocks):
        return [blocks] + [
            [self.tp_shift(b, t) for b in blocks] for t in range(1, self.tp_count)
        ]


def behind(index, distance, count):
    return lax.rem(index - distance + count, count)


def copy_all(pairs, sem):
    copies = [pltpu.make_async_copy(s, d, sem.at[n]) for n, (s, d) in enumerate(pairs)]
    for c in copies:
        c.start()
    return copies


def any_specs(n):
    return [pl.BlockSpec(memory_space=pl.ANY)] * n


def whole_vmem():
    return pl.BlockSpec(memory_space=pltpu.VMEM)


def latent_kernel(place, rank, share, *refs):
    outer, inner, tp = place.outer, place.inner, place.tp_count
    tables = tp if share else 1
    n_rows, n_w = outer, tables * inner
    row_refs, w_refs = refs[:n_rows], refs[n_rows : n_rows + n_w]
    gain_ref, cos_ref, sin_ref, out_ref, rows, weight, sem_r, sem_w = refs[n_rows + n_w :]
    zi, xi, ti = place.indices()
    piece = w_refs[0].shape[1]
    block = piece * tables
    count = row_refs[0].shape[0]
    pairs = []
    for t in range(tables):
        owner = behind(ti, t, tp) if share else 0
        for k in range(inner):
            for j in range(outer):
                start = (behind(zi, j, outer) * inner + (xi ^ k)) * block + owner * piece
                pairs.append(
                    (
                        w_refs[t * inner + k].at[j],
                        weight.at[pl.ds(pl.multiple_of(start, piece), piece)],
                    )
                )
    w_copies = copy_all(pairs, sem_w)
    r_copies = copy_all(
        [(row_refs[j], rows.at[pl.ds(j * count, count)]) for j in range(outer)], sem_r
    )
    for c in w_copies + r_copies:
        c.wait()
    pre = jnp.dot(rows[...], weight[...], preferred_element_type=jnp.float32)
    plain = pre[:, :rank]
    scale = lax.rsqrt(jnp.mean(plain * plain, axis=-1, keepdims=True) + epsilon)
    out_ref[:, :rank] = (plain * scale * gain_ref[...]).astype(jnp.bfloat16)
    rope = pre[:, rank:]
    half = rope.shape[1] // 2
    first, second = rope[:, :half], rope[:, half:]
    cosine, sine = cos_ref[...], sin_ref[...]
    out_ref[:, rank:] = jnp.concatenate(
        [first * cosine - second * sine, first * sine + second * cosine], axis=-1
    ).astype(jnp.bfloat16)


def gated_kernel(place, *refs):
    outer, inner, tp = place.outer, place.inner, place.tp_count
    n_rows = tp * outer
    row_refs, w_refs = refs[:n_rows], refs[n_rows : n_rows + inner]
    outs = refs[n_rows + inner : n_rows + inner + outer]
    rows, weight, sem_r, sem_w = refs[n_rows + inner + outer :]
    zi, xi, ti = place.indices()
    block = w_refs[0].shape[1]
    count = row_refs[0].shape[0]
    pairs = []
    for k in range(inner):
        for j in range(outer):
            start = (behind(zi, j, outer) * inner + (xi ^ k)) * block
            pairs.append(
                (w_refs[k].at[j], weight.at[pl.ds(pl.multiple_of(start, block), block)])
            )
    w_copies = copy_all(pairs, sem_w)
    pairs = []
    for t in range(tp):
        owner = behind(ti, t, tp)
        for j in range(outer):
            start = j * tp * count + owner * count
            pairs.append(
                (
                    row_refs[t * outer + j],
                    rows.at[pl.ds(pl.multiple_of(start, count), count)],
                )
            )
    r_copies = copy_all(pairs, sem_r)
    for c in w_copies + r_copies:
        c.wait()
    chunk = tp * count
    width = outs[0].shape[1]
    for j in range(outer):
        pre = jnp.dot(
            rows[pl.ds(j * chunk, chunk)], weight[...], preferred_element_type=jnp.float32
        )
        value, gate = pre[:, :width], pre[:, width:]
        outs[j][...] = (value * jax.nn.sigmoid(gate)).astype(jnp.bfloat16)


def attention_kernel(place, scale, ql_ref, qr_ref, up_ref, *refs):
    outer, inner, tp = place.outer, place.inner, place.tp_count
    n_k = tp * inner
    key_refs = refs[:n_k]
    out_ref, lse_ref, keys, sem = refs[n_k:]
    zi, xi, ti = place.indices()
    heads, count, rank = ql_ref.shape
    piece = key_refs[0].shape[0]
    share = piece // outer
    copies = copy_all(
        [(key_refs[n], keys.at[pl.ds(n * piece, piece)]) for n in range(n_k)], sem
    )
    lane = lax.broadcasted_iota(jnp.int32, (1, piece), 1)
    step = lax.shift_right_logical(lane, share.bit_length() - 1)
    within = jnp.bitwise_and(lane, share - 1)
    back = zi - step
    back = jnp.where(back < 0, back + outer, back)
    parts = []
    for t in range(tp):
        owner = behind(ti, t, tp)
        for k in range(inner):
            parts.append((back * inner + (xi ^ k)) * count + owner * share + within)
    key_index = jnp.concatenate(parts, axis=1)
    first_row = (zi * inner + xi) * count
    query_index = first_row + lax.broadcasted_iota(jnp.int32, (count, 1), 0)
    allowed = key_index <= query_index
    for c in copies:
        c.wait()
    for h in range(heads):
        scores = lax.dot_general(
            ql_ref[h], keys[:, :rank], (((1,), (1,)), ((), ())),
            preferred_element_type=jnp.float32,
        )
        scores = scores + lax.dot_general(
            qr_ref[h], keys[:, rank:], (((1,), (1,)), ((), ())),
            preferred_element_type=jnp.float32,
        )
        scores = jnp.where(allowed, scores * scale, masked_score)
        top = jnp.max(scores, axis=-1, keepdims=True)
        weights = jnp.exp(scores - top)
        total = jnp.sum(weights, axis=-1, keepdims=True)
        weighted = jnp.dot(
            weights.astype(jnp.bfloat16), keys[:, :rank], preferred_element_type=jnp.float32
        )
        latent_out = (weighted / total).astype(jnp.bfloat16)
        lse_ref[:, h : h + 1] = top + jnp.log(total)
        width = VALUE_HEAD_WIDTH
        out_ref[:, h * width : (h + 1) * width] = jnp.dot(
            latent_out,
            up_ref[:, h * width : (h + 1) * width],
            preferred_element_type=jnp.float32,
        ).astype(jnp.bfloat16)


def local(
    tokens,
    norm_gain,
    w_value,
    w_gate,
    conv_taps,
    conv_gain,
    w_query,
    latent_down_weight,
    latent_norm_gain,
    w_rope_key,
    key_up_weight,
    value_up_weight,
    w_merge_conv,
    w_merge_attn,
):
    place = Place()
    outer, inner, tp_count = place.outer, place.inner, place.tp_count
    zi, xi, ti = place.indices()
    row_count = tokens.shape[0]
    share = row_count // tp_count
    depth = latent_down_weight.shape[0]
    rank = latent_down_weight.shape[1]

    split_rows = depth % (16 * tp_count) == 0
    own_table = jnp.concatenate([latent_down_weight, w_rope_key], axis=1)
    if split_rows:
        piece = depth // tp_count
        own_table = lax.dynamic_slice_in_dim(own_table, ti * piece, piece, 0)
    table = jnp.stack(place.outer_gather(own_table))
    tables = place.inner_gather(table)
    if split_rows:
        tables = sum(place.tp_gather(tables), [])

    gathered = lax.all_gather(tokens, "tp", axis=1, tiled=True)
    features = gathered.astype(jnp.float32)
    normed = (
        features
        * lax.rsqrt(jnp.mean(features * features, axis=-1, keepdims=True) + epsilon)
        * norm_gain
    ).astype(jnp.bfloat16)

    own_rows = lax.dynamic_slice_in_dim(normed, ti * share, share, 0)
    rows = place.outer_gather(own_rows)
    width = w_value.shape[1] // outer
    columns = []
    for j in range(outer):
        start = lax.rem(zi + j, outer) * width
        block = jnp.concatenate(
            [
                lax.dynamic_slice_in_dim(w_value, start, width, 1),
                lax.dynamic_slice_in_dim(w_gate, start, width, 1),
            ],
            axis=1,
        )
        columns.append(block if j == 0 else place.outer_shift(block, j))
    weight_blocks = place.inner_gather(jnp.stack(columns))

    head_count = key_up_weight.shape[1] // PLAIN_QK_WIDTH
    query_index = lax.axis_index("sp") * row_count + jnp.arange(row_count, dtype=jnp.int32)
    query = (
        jnp.dot(normed, w_query, preferred_element_type=jnp.float32)
        .astype(jnp.bfloat16)
        .reshape(row_count, head_count, PLAIN_QK_WIDTH + QK_ROPE)
    )
    query_angles = angles_at(query_index.astype(jnp.float32), QK_ROPE)
    query_rope = rotate(
        query[..., PLAIN_QK_WIDTH:].astype(jnp.float32), query_angles[:, None, :]
    ).astype(jnp.bfloat16)
    key_expanded = key_up_weight.reshape(rank, head_count, PLAIN_QK_WIDTH)
    query_latent = jnp.einsum(
        "thd,lhd->htl",
        query[..., :PLAIN_QK_WIDTH],
        key_expanded,
        preferred_element_type=jnp.float32,
    ).astype(jnp.bfloat16)
    query_rope = query_rope.transpose(1, 0, 2)

    back = jnp.arange(outer, dtype=jnp.int32)
    back = lax.rem(zi - back + outer, outer)
    key_index = (
        ((back * inner + xi) * row_count + ti * share)[:, None]
        + jnp.arange(share, dtype=jnp.int32)[None, :]
    ).reshape(-1)
    key_angles = angles_at(key_index.astype(jnp.float32), QK_ROPE)
    bf16 = jnp.bfloat16
    model = normed.shape[1]
    latent = pl.pallas_call(
        functools.partial(latent_kernel, place, rank, split_rows),
        out_shape=jax.ShapeDtypeStruct((outer * share, rank + QK_ROPE), bf16),
        in_specs=any_specs(outer + len(tables)) + [whole_vmem()] * 3,
        out_specs=whole_vmem(),
        scratch_shapes=[
            pltpu.VMEM((outer * share, model), bf16),
            pltpu.VMEM((model, rank + QK_ROPE), bf16),
            pltpu.SemaphoreType.DMA((outer,)),
            pltpu.SemaphoreType.DMA((len(tables) * outer,)),
        ],
        compiler_params=pltpu.CompilerParams(vmem_limit_bytes=16 << 20),
        cost_estimate=pl.CostEstimate(
            flops=2 * outer * share * model * (rank + QK_ROPE),
            bytes_accessed=2 * model * (rank + QK_ROPE + outer * share),
            transcendentals=0,
        ),
        name="latents",
    )(*rows, *tables, latent_norm_gain[None, :], jnp.cos(key_angles), jnp.sin(key_angles))
    latents = sum(place.tp_gather(place.inner_gather(latent)), [])

    all_rows = sum(place.tp_gather(rows), [])
    gated = pl.pallas_call(
        functools.partial(gated_kernel, place),
        out_shape=[jax.ShapeDtypeStruct((row_count, width), bf16)] * outer,
        in_specs=any_specs(len(all_rows) + inner),
        out_specs=[whole_vmem()] * outer,
        scratch_shapes=[
            pltpu.VMEM((outer * row_count, model), bf16),
            pltpu.VMEM((model, 2 * width), bf16),
            pltpu.SemaphoreType.DMA((len(all_rows),)),
            pltpu.SemaphoreType.DMA((inner * outer,)),
        ],
        compiler_params=pltpu.CompilerParams(vmem_limit_bytes=24 << 20),
        cost_estimate=pl.CostEstimate(
            flops=4 * outer * row_count * model * width,
            bytes_accessed=2 * model * (2 * width + outer * row_count),
            transcendentals=outer * row_count * width,
        ),
        name="gated",
    )(*all_rows, *weight_blocks)
    home = [gated[0]] + [
        place.outer_shift(gated[(outer - j) % outer], j) for j in range(1, outer)
    ]
    in_order = [home[(outer - b) % outer] for b in range(outer)]
    gated_rows = lax.dynamic_slice_in_dim(
        jnp.concatenate(in_order + in_order, axis=1),
        lax.rem(outer - zi, outer) * width,
        outer * width,
        1,
    )

    conv_reach = conv_taps.shape[0] - 1
    prior_rows = lax.ppermute(
        gated_rows[row_count - conv_reach :],
        "sp",
        [(i, i + 1) for i in range(place.sp_count - 1)],
    )
    padded = jnp.concatenate([prior_rows, gated_rows], axis=0).astype(jnp.float32)
    mixed = jnp.zeros(gated_rows.shape, jnp.float32)
    for tap_index in range(conv_taps.shape[0]):
        mixed = (
            mixed
            + conv_taps[tap_index].astype(jnp.float32) * padded[tap_index : tap_index + row_count]
        )
    channel_total = mixed.shape[1] * tp_count
    stat_sum, stat_squares = lax.psum(
        (jnp.sum(mixed, axis=1), jnp.sum(mixed * mixed, axis=1)), "tp"
    )
    channel_mean = stat_sum / channel_total
    channel_var = stat_squares / channel_total - channel_mean * channel_mean
    conv_out = jax.nn.silu(
        (mixed - channel_mean[:, None]) * lax.rsqrt(channel_var + epsilon)[:, None] * conv_gain
    ).astype(bf16)

    score_scale = (PLAIN_QK_WIDTH + QK_ROPE) ** (-0.5)
    key_total = place.sp_count * row_count
    attention, log_sums = pl.pallas_call(
        functools.partial(attention_kernel, place, score_scale),
        out_shape=[
            jax.ShapeDtypeStruct((row_count, head_count * VALUE_HEAD_WIDTH), bf16),
            jax.ShapeDtypeStruct((row_count, head_count), jnp.float32),
        ],
        in_specs=[whole_vmem()] * 3 + any_specs(len(latents)),
        out_specs=[whole_vmem()] * 2,
        scratch_shapes=[
            pltpu.VMEM((key_total, rank + QK_ROPE), bf16),
            pltpu.SemaphoreType.DMA((len(latents),)),
        ],
        compiler_params=pltpu.CompilerParams(vmem_limit_bytes=40 << 20),
        cost_estimate=pl.CostEstimate(
            flops=2 * row_count * head_count * key_total * (2 * rank + QK_ROPE),
            bytes_accessed=2 * key_total * (rank + QK_ROPE),
            transcendentals=row_count * head_count * key_total,
        ),
        name="attention",
    )(query_latent, query_rope, value_up_weight, *latents)

    partial = (
        jnp.dot(conv_out, w_merge_conv, preferred_element_type=jnp.float32)
        + jnp.dot(attention, w_merge_attn, preferred_element_type=jnp.float32)
    ).astype(bf16)
    merged = lax.dynamic_slice_in_dim(partial, ti * share, share, 0).astype(jnp.float32)
    for t in range(1, tp_count):
        away = lax.dynamic_slice_in_dim(partial, lax.rem(ti + t, tp_count) * share, share, 0)
        merged = merged + place.tp_shift(away, t).astype(jnp.float32)
    return (merged.astype(bf16), log_sums)


def solution(mesh):
    return jax.shard_map(
        local,
        mesh=mesh,
        in_specs=(
            P("sp", "tp"),
            P(),
            P("sp", "tp"),
            P("sp", "tp"),
            P(None, "tp"),
            P("tp"),
            P(None, "tp"),
            P("sp", None),
            P(),
            P("sp", None),
            P(None, "tp"),
            P(None, "tp"),
            P("tp", None),
            P("tp", None),
        ),
        out_specs=(P(("sp", "tp"), None), P("sp", "tp")),
        check_vma=False,
    )
```

```python
import functools
import math

import jax
import jax.numpy as jnp
from jax import lax
from jax.experimental import pallas as pl
from jax.experimental.pallas import tpu as pltpu
from jax.sharding import PartitionSpec as P

PLAIN_QK_WIDTH = 128
QK_ROPE = 64
VALUE_HEAD_WIDTH = 128


epsilon = 1e-06
rope_base = 10000.0
masked_score = -1e30


def angles_at(positions, width):
    inverse = rope_base ** (-2.0 * jnp.arange(width // 2, dtype=jnp.float32) / width)
    return positions[:, None] * inverse[None, :]


def rotate(halves, angle):
    middle = halves.shape[-1] // 2
    first, second = (halves[..., :middle], halves[..., middle:])
    cosine, sine = (jnp.cos(angle), jnp.sin(angle))
    return jnp.concatenate(
        [first * cosine - second * sine, first * sine + second * cosine], axis=-1
    )


class Place:
    def __init__(self):
        self.sp_count = lax.axis_size("sp")
        self.tp_count = lax.axis_size("tp")
        self.inner = math.gcd(self.sp_count, 4)
        self.outer = self.sp_count // self.inner

    def indices(self):
        index = lax.axis_index("sp")
        return index // self.inner, index % self.inner, lax.axis_index("tp")

    def outer_shift(self, block, distance):
        route = [
            (i, ((i // self.inner + distance) % self.outer) * self.inner + i % self.inner)
            for i in range(self.sp_count)
        ]
        return lax.ppermute(block, "sp", route)

    def inner_swap(self, block, mask):
        return lax.ppermute(block, "sp", [(i, i ^ mask) for i in range(self.sp_count)])

    def tp_shift(self, block, distance):
        route = [(i, (i + distance) % self.tp_count) for i in range(self.tp_count)]
        return lax.ppermute(block, "tp", route)

    def outer_gather(self, block):
        return [block] + [self.outer_shift(block, j) for j in range(1, self.outer)]

    def inner_gather(self, block):
        return [block] + [self.inner_swap(block, k) for k in range(1, self.inner)]

    def tp_gather(self, blocks):
        return [blocks] + [
            [self.tp_shift(b, t) for b in blocks] for t in range(1, self.tp_count)
        ]


def behind(index, distance, count):
    return lax.rem(index - distance + count, count)


def copy_all(pairs, sem):
    copies = [pltpu.make_async_copy(s, d, sem.at[n]) for n, (s, d) in enumerate(pairs)]
    for c in copies:
        c.start()
    return copies


def any_specs(n):
    return [pl.BlockSpec(memory_space=pl.ANY)] * n


def whole_vmem():
    return pl.BlockSpec(memory_space=pltpu.VMEM)


def turned(first, second, cosine, sine):
    return jnp.concatenate(
        [first * cosine - second * sine, first * sine + second * cosine], axis=-1
    ).astype(jnp.bfloat16)


def query_kernel(normed_ref, w_ref, up_ref, cos_ref, sin_ref, ql_ref, qr_ref, w, up, sem):
    heads, count, rank = ql_ref.shape
    plain, half = PLAIN_QK_WIDTH, QK_ROPE // 2
    head = plain + QK_ROPE
    span = 2 * head
    pairs = heads // 2
    copies = copy_all(
        [
            (w_ref.at[:, p * span : (p + 1) * span], w.at[:, p * span : (p + 1) * span])
            for p in range(pairs)
        ]
        + [(up_ref, up)],
        sem,
    )
    cosine, sine = cos_ref[:count], sin_ref[:count]
    for p in range(pairs):
        copies[p].wait()
        query = jnp.dot(
            normed_ref[...], w[:, p * span : (p + 1) * span], preferred_element_type=jnp.float32
        ).astype(jnp.bfloat16)
        if p == 0:
            copies[pairs].wait()
        for i in range(2):
            h = 2 * p + i
            own = query[:, i * head : (i + 1) * head]
            ql_ref[h] = lax.dot_general(
                own[:, :plain],
                up[:, h * plain : (h + 1) * plain],
                (((1,), (1,)), ((), ())),
                preferred_element_type=jnp.float32,
            ).astype(jnp.bfloat16)
            rope = own[:, plain:].astype(jnp.float32)
            qr_ref[h] = turned(rope[:, :half], rope[:, half:], cosine, sine)


def latent_kernel(place, rank, share, *refs):
    outer, inner, tp = place.outer, place.inner, place.tp_count
    tables = tp if share else 1
    n_rows, n_w = outer, tables * inner
    row_refs, w_refs = refs[:n_rows], refs[n_rows : n_rows + n_w]
    gain_ref, cos_ref, sin_ref, out_ref, rows, weight, sem_r, sem_w = refs[n_rows + n_w :]
    zi, xi, ti = place.indices()
    piece = w_refs[0].shape[1]
    block = piece * tables
    count = row_refs[0].shape[0]
    pairs = []
    for t in range(tables):
        owner = behind(ti, t, tp) if share else 0
        for k in range(inner):
            for j in range(outer):
                start = (behind(zi, j, outer) * inner + (xi ^ k)) * block + owner * piece
                pairs.append(
                    (
                        w_refs[t * inner + k].at[j],
                        weight.at[pl.ds(pl.multiple_of(start, piece), piece)],
                    )
                )
    w_copies = copy_all(pairs, sem_w)
    r_copies = copy_all(
        [(row_refs[j], rows.at[pl.ds(j * count, count)]) for j in range(outer)], sem_r
    )
    for c in w_copies + r_copies:
        c.wait()
    pre = jnp.dot(rows[...], weight[...], preferred_element_type=jnp.float32)
    plain = pre[:, :rank]
    scale = lax.rsqrt(jnp.mean(plain * plain, axis=-1, keepdims=True) + epsilon)
    out_ref[:, :rank] = (plain * scale * gain_ref[...]).astype(jnp.bfloat16)
    rope = pre[:, rank:]
    half = rope.shape[1] // 2
    total = outer * count
    cosine, sine = cos_ref[cos_ref.shape[0] - total :], sin_ref[sin_ref.shape[0] - total :]
    out_ref[:, rank:] = turned(rope[:, :half], rope[:, half:], cosine, sine)


def gated_kernel(place, *refs):
    outer, inner, tp = place.outer, place.inner, place.tp_count
    n_rows = tp * outer
    row_refs, w_refs = refs[:n_rows], refs[n_rows : n_rows + inner]
    outs = refs[n_rows + inner : n_rows + inner + outer]
    rows, weight, sem_r, sem_w = refs[n_rows + inner + outer :]
    zi, xi, ti = place.indices()
    block = w_refs[0].shape[1]
    count = row_refs[0].shape[0]
    pairs = []
    for k in range(inner):
        for j in range(outer):
            start = (behind(zi, j, outer) * inner + (xi ^ k)) * block
            pairs.append(
                (w_refs[k].at[j], weight.at[pl.ds(pl.multiple_of(start, block), block)])
            )
    w_copies = copy_all(pairs, sem_w)
    pairs = []
    for t in range(tp):
        owner = behind(ti, t, tp)
        for j in range(outer):
            start = j * tp * count + owner * count
            pairs.append(
                (
                    row_refs[t * outer + j],
                    rows.at[pl.ds(pl.multiple_of(start, count), count)],
                )
            )
    r_copies = copy_all(pairs, sem_r)
    for c in w_copies + r_copies:
        c.wait()
    chunk = tp * count
    width = outs[0].shape[1]
    for j in range(outer):
        pre = jnp.dot(
            rows[pl.ds(j * chunk, chunk)], weight[...], preferred_element_type=jnp.float32
        )
        value, gate = pre[:, :width], pre[:, width:]
        outs[j][...] = (value * jax.nn.sigmoid(gate)).astype(jnp.bfloat16)


def attention_kernel(place, scale, ql_ref, qr_ref, up_ref, *refs):
    outer, inner, tp = place.outer, place.inner, place.tp_count
    n_k = tp * inner
    key_refs = refs[:n_k]
    out_ref, lse_ref, keys, sem = refs[n_k:]
    zi, xi, ti = place.indices()
    heads, count, rank = ql_ref.shape
    piece = key_refs[0].shape[0]
    share = piece // outer
    copies = copy_all(
        [(key_refs[n], keys.at[pl.ds(n * piece, piece)]) for n in range(n_k)], sem
    )
    lane = lax.broadcasted_iota(jnp.int32, (1, piece), 1)
    step = lax.shift_right_logical(lane, share.bit_length() - 1)
    within = jnp.bitwise_and(lane, share - 1)
    back = zi - step
    back = jnp.where(back < 0, back + outer, back)
    parts = []
    for t in range(tp):
        owner = behind(ti, t, tp)
        for k in range(inner):
            parts.append((back * inner + (xi ^ k)) * count + owner * share + within)
    key_index = jnp.concatenate(parts, axis=1)
    first_row = (zi * inner + xi) * count
    query_index = first_row + lax.broadcasted_iota(jnp.int32, (count, 1), 0)
    allowed = key_index <= query_index
    for c in copies:
        c.wait()
    for h in range(heads):
        scores = lax.dot_general(
            ql_ref[h], keys[:, :rank], (((1,), (1,)), ((), ())),
            preferred_element_type=jnp.float32,
        )
        scores = scores + lax.dot_general(
            qr_ref[h], keys[:, rank:], (((1,), (1,)), ((), ())),
            preferred_element_type=jnp.float32,
        )
        scores = jnp.where(allowed, scores * scale, masked_score)
        top = jnp.max(scores, axis=-1, keepdims=True)
        weights = jnp.exp(scores - top)
        total = jnp.sum(weights, axis=-1, keepdims=True)
        weighted = jnp.dot(
            weights.astype(jnp.bfloat16), keys[:, :rank], preferred_element_type=jnp.float32
        )
        latent_out = (weighted / total).astype(jnp.bfloat16)
        lse_ref[:, h : h + 1] = top + jnp.log(total)
        width = VALUE_HEAD_WIDTH
        out_ref[:, h * width : (h + 1) * width] = jnp.dot(
            latent_out,
            up_ref[:, h * width : (h + 1) * width],
            preferred_element_type=jnp.float32,
        ).astype(jnp.bfloat16)


def local(
    tokens,
    norm_gain,
    w_value,
    w_gate,
    conv_taps,
    conv_gain,
    w_query,
    latent_down_weight,
    latent_norm_gain,
    w_rope_key,
    key_up_weight,
    value_up_weight,
    w_merge_conv,
    w_merge_attn,
):
    place = Place()
    outer, inner, tp_count = place.outer, place.inner, place.tp_count
    zi, xi, ti = place.indices()
    row_count = tokens.shape[0]
    share = row_count // tp_count
    depth = latent_down_weight.shape[0]
    rank = latent_down_weight.shape[1]

    split_rows = depth % (16 * tp_count) == 0
    own_table = jnp.concatenate([latent_down_weight, w_rope_key], axis=1)
    if split_rows:
        piece = depth // tp_count
        own_table = lax.dynamic_slice_in_dim(own_table, ti * piece, piece, 0)
    own_table, w_value, w_gate = lax.optimization_barrier((own_table, w_value, w_gate))
    table_parts = place.outer_gather(own_table)

    width = w_value.shape[1] // outer
    columns = []
    for j in range(outer):
        start = lax.rem(zi + j, outer) * width
        block = jnp.concatenate(
            [
                lax.dynamic_slice_in_dim(w_value, start, width, 1),
                lax.dynamic_slice_in_dim(w_gate, start, width, 1),
            ],
            axis=1,
        )
        columns.append(block if j == 0 else place.outer_shift(block, j))

    table = jnp.stack(table_parts)
    table, tokens = lax.optimization_barrier((table, tokens))
    tables = place.inner_gather(table)

    gathered = lax.all_gather(tokens, "tp", axis=1, tiled=True)
    features = gathered.astype(jnp.float32)
    normed = (
        features
        * lax.rsqrt(jnp.mean(features * features, axis=-1, keepdims=True) + epsilon)
        * norm_gain
    ).astype(jnp.bfloat16)

    own_rows = lax.dynamic_slice_in_dim(normed, ti * share, share, 0)
    rows = place.outer_gather(own_rows)
    weight_block = jnp.stack(columns)
    weight_block, query_rows = lax.optimization_barrier((weight_block, normed))
    weight_blocks = place.inner_gather(weight_block)

    bf16 = jnp.bfloat16
    model = normed.shape[1]
    head_count = key_up_weight.shape[1] // PLAIN_QK_WIDTH
    query_index = lax.axis_index("sp") * row_count + jnp.arange(row_count, dtype=jnp.int32)
    back = jnp.arange(outer, dtype=jnp.int32)
    back = lax.rem(zi - back + outer, outer)
    key_index = (
        ((back * inner + xi) * row_count + ti * share)[:, None]
        + jnp.arange(share, dtype=jnp.int32)[None, :]
    ).reshape(-1)
    angles = angles_at(
        jnp.concatenate([query_index, key_index]).astype(jnp.float32), QK_ROPE
    )
    cosine, sine = jnp.cos(angles), jnp.sin(angles)

    query_width = w_query.shape[1]
    query_latent, query_rope = pl.pallas_call(
        query_kernel,
        out_shape=[
            jax.ShapeDtypeStruct((head_count, row_count, rank), bf16),
            jax.ShapeDtypeStruct((head_count, row_count, QK_ROPE), bf16),
        ],
        in_specs=[whole_vmem()] + [pl.BlockSpec(memory_space=pltpu.HBM)] * 2 + [whole_vmem()] * 2,
        out_specs=[whole_vmem()] * 2,
        scratch_shapes=[
            pltpu.VMEM((model, query_width), bf16),
            pltpu.VMEM(key_up_weight.shape, bf16),
            pltpu.SemaphoreType.DMA((head_count // 2 + 1,)),
        ],
        compiler_params=pltpu.CompilerParams(vmem_limit_bytes=52 << 20),
        cost_estimate=pl.CostEstimate(
            flops=2 * row_count * model * query_width,
            bytes_accessed=2 * model * query_width,
            transcendentals=0,
        ),
        name="queries",
    )(query_rows, w_query, key_up_weight, cosine, sine)

    rows, tables, _ = lax.optimization_barrier((rows, tables, query_rope))
    if split_rows:
        tables = sum(place.tp_gather(tables), [])

    latent = pl.pallas_call(
        functools.partial(latent_kernel, place, rank, split_rows),
        out_shape=jax.ShapeDtypeStruct((outer * share, rank + QK_ROPE), bf16),
        in_specs=any_specs(outer + len(tables)) + [whole_vmem()] * 3,
        out_specs=whole_vmem(),
        scratch_shapes=[
            pltpu.VMEM((outer * share, model), bf16),
            pltpu.VMEM((model, rank + QK_ROPE), bf16),
            pltpu.SemaphoreType.DMA((outer,)),
            pltpu.SemaphoreType.DMA((len(tables) * outer,)),
        ],
        compiler_params=pltpu.CompilerParams(vmem_limit_bytes=16 << 20),
        cost_estimate=pl.CostEstimate(
            flops=2 * outer * share * model * (rank + QK_ROPE),
            bytes_accessed=2 * model * (rank + QK_ROPE + outer * share),
            transcendentals=0,
        ),
        name="latents",
    )(*rows, *tables, latent_norm_gain[None, :], cosine, sine)
    _, *weight_blocks = lax.optimization_barrier((latent, *weight_blocks))
    latents = sum(place.tp_gather(place.inner_gather(latent)), [])

    all_rows = sum(place.tp_gather(rows), [])
    gated = pl.pallas_call(
        functools.partial(gated_kernel, place),
        out_shape=[jax.ShapeDtypeStruct((row_count, width), bf16)] * outer,
        in_specs=any_specs(len(all_rows) + inner),
        out_specs=[whole_vmem()] * outer,
        scratch_shapes=[
            pltpu.VMEM((outer * row_count, model), bf16),
            pltpu.VMEM((model, 2 * width), bf16),
            pltpu.SemaphoreType.DMA((len(all_rows),)),
            pltpu.SemaphoreType.DMA((inner * outer,)),
        ],
        compiler_params=pltpu.CompilerParams(vmem_limit_bytes=24 << 20),
        cost_estimate=pl.CostEstimate(
            flops=4 * outer * row_count * model * width,
            bytes_accessed=2 * model * (2 * width + outer * row_count),
            transcendentals=outer * row_count * width,
        ),
        name="gated",
    )(*all_rows, *weight_blocks)
    home = [gated[0]] + [
        place.outer_shift(gated[(outer - j) % outer], j) for j in range(1, outer)
    ]
    in_order = [home[(outer - b) % outer] for b in range(outer)]
    gated_rows = lax.dynamic_slice_in_dim(
        jnp.concatenate(in_order + in_order, axis=1),
        lax.rem(outer - zi, outer) * width,
        outer * width,
        1,
    )

    conv_reach = conv_taps.shape[0] - 1
    prior_rows = lax.ppermute(
        gated_rows[row_count - conv_reach :],
        "sp",
        [(i, i + 1) for i in range(place.sp_count - 1)],
    )
    padded = jnp.concatenate([prior_rows, gated_rows], axis=0).astype(jnp.float32)
    mixed = jnp.zeros(gated_rows.shape, jnp.float32)
    for tap_index in range(conv_taps.shape[0]):
        mixed = (
            mixed
            + conv_taps[tap_index].astype(jnp.float32) * padded[tap_index : tap_index + row_count]
        )
    channel_total = mixed.shape[1] * tp_count
    stat_sum, stat_squares = lax.psum(
        (jnp.sum(mixed, axis=1), jnp.sum(mixed * mixed, axis=1)), "tp"
    )
    channel_mean = stat_sum / channel_total
    channel_var = stat_squares / channel_total - channel_mean * channel_mean
    conv_out = jax.nn.silu(
        (mixed - channel_mean[:, None]) * lax.rsqrt(channel_var + epsilon)[:, None] * conv_gain
    ).astype(bf16)

    score_scale = (PLAIN_QK_WIDTH + QK_ROPE) ** (-0.5)
    key_total = place.sp_count * row_count
    attention, log_sums = pl.pallas_call(
        functools.partial(attention_kernel, place, score_scale),
        out_shape=[
            jax.ShapeDtypeStruct((row_count, head_count * VALUE_HEAD_WIDTH), bf16),
            jax.ShapeDtypeStruct((row_count, head_count), jnp.float32),
        ],
        in_specs=[whole_vmem()] * 3 + any_specs(len(latents)),
        out_specs=[whole_vmem()] * 2,
        scratch_shapes=[
            pltpu.VMEM((key_total, rank + QK_ROPE), bf16),
            pltpu.SemaphoreType.DMA((len(latents),)),
        ],
        compiler_params=pltpu.CompilerParams(vmem_limit_bytes=40 << 20),
        cost_estimate=pl.CostEstimate(
            flops=2 * row_count * head_count * key_total * (2 * rank + QK_ROPE),
            bytes_accessed=2 * key_total * (rank + QK_ROPE),
            transcendentals=row_count * head_count * key_total,
        ),
        name="attention",
    )(query_latent, query_rope, value_up_weight, *latents)

    partial = (
        jnp.dot(conv_out, w_merge_conv, preferred_element_type=jnp.float32)
        + jnp.dot(attention, w_merge_attn, preferred_element_type=jnp.float32)
    ).astype(bf16)
    merged = lax.dynamic_slice_in_dim(partial, ti * share, share, 0).astype(jnp.float32)
    for t in range(1, tp_count):
        away = lax.dynamic_slice_in_dim(partial, lax.rem(ti + t, tp_count) * share, share, 0)
        merged = merged + place.tp_shift(away, t).astype(jnp.float32)
    return (merged.astype(bf16), log_sums)


def solution(mesh):
    return jax.shard_map(
        local,
        mesh=mesh,
        in_specs=(
            P("sp", "tp"),
            P(),
            P("sp", "tp"),
            P("sp", "tp"),
            P(None, "tp"),
            P("tp"),
            P(None, "tp"),
            P("sp", None),
            P(),
            P("sp", None),
            P(None, "tp"),
            P(None, "tp"),
            P("tp", None),
            P("tp", None),
        ),
        out_specs=(P(("sp", "tp"), None), P("sp", "tp")),
        check_vma=False,
    )
```

```python
import functools
import math

import jax
import jax.numpy as jnp
from jax import lax
from jax.experimental import pallas as pl
from jax.experimental.pallas import tpu as pltpu
from jax.sharding import PartitionSpec as P


PLAIN_QK_WIDTH = 128
QK_ROPE = 64
VALUE_HEAD_WIDTH = 128


epsilon = 1e-06
rope_base = 10000.0
masked_score = -1e30


def angles_at(positions, width):
    inverse = rope_base ** (-2.0 * jnp.arange(width // 2, dtype=jnp.float32) / width)
    return positions[:, None] * inverse[None, :]


class Place:
    def __init__(self):
        self.sp_count = lax.axis_size("sp")
        self.tp_count = lax.axis_size("tp")
        self.inner = math.gcd(self.sp_count, 4)
        self.outer = self.sp_count // self.inner

    def indices(self):
        index = lax.axis_index("sp")
        return index // self.inner, index % self.inner, lax.axis_index("tp")

    def outer_swap(self, block, mask):
        mask = mask * self.inner
        return lax.ppermute(block, "sp", [(i, i ^ mask) for i in range(self.sp_count)])

    def inner_swap(self, block, mask):
        return lax.ppermute(block, "sp", [(i, i ^ mask) for i in range(self.sp_count)])

    def tp_shift(self, block, distance):
        route = [(i, (i + distance) % self.tp_count) for i in range(self.tp_count)]
        return lax.ppermute(block, "tp", route)

    def outer_gather(self, block):
        return [block] + [self.outer_swap(block, j) for j in range(1, self.outer)]

    def inner_gather(self, block):
        return [block] + [self.inner_swap(block, k) for k in range(1, self.inner)]

    def tp_gather(self, blocks):
        return [blocks] + [
            [self.tp_shift(b, t) for b in blocks] for t in range(1, self.tp_count)
        ]


def behind(index, distance, count):
    return lax.rem(index - distance + count, count)


def untangled(blocks, index):
    bit = 1
    while bit < len(blocks):
        flag = (index & bit) > 0
        blocks = [jnp.where(flag, blocks[i ^ bit], b) for i, b in enumerate(blocks)]
        bit *= 2
    return blocks


def copy_all(pairs, sem):
    copies = [pltpu.make_async_copy(s, d, sem.at[n]) for n, (s, d) in enumerate(pairs)]
    for c in copies:
        c.start()
    return copies


def any_specs(n):
    return [pl.BlockSpec(memory_space=pl.ANY)] * n


def whole_vmem():
    return pl.BlockSpec(memory_space=pltpu.VMEM)


def turned(first, second, cosine, sine):
    return jnp.concatenate(
        [first * cosine - second * sine, first * sine + second * cosine], axis=-1
    ).astype(jnp.bfloat16)


def query_kernel(rank, normed_ref, w_ref, up_ref, cos_ref, sin_ref, out_ref, w, up, sem):
    heads, count, _ = out_ref.shape
    plain, half = PLAIN_QK_WIDTH, QK_ROPE // 2
    head = plain + QK_ROPE
    span = 2 * head
    pairs = heads // 2
    copies = copy_all(
        [
            (w_ref.at[:, p * span : (p + 1) * span], w.at[:, p * span : (p + 1) * span])
            for p in range(pairs)
        ]
        + [(up_ref, up)],
        sem,
    )
    cosine, sine = cos_ref[:count], sin_ref[:count]
    for p in range(pairs):
        copies[p].wait()
        query = jnp.dot(
            normed_ref[...], w[:, p * span : (p + 1) * span], preferred_element_type=jnp.float32
        ).astype(jnp.bfloat16)
        if p == 0:
            copies[pairs].wait()
        for i in range(2):
            h = 2 * p + i
            own = query[:, i * head : (i + 1) * head]
            out_ref[h, :, :rank] = lax.dot_general(
                own[:, :plain],
                up[:, h * plain : (h + 1) * plain],
                (((1,), (1,)), ((), ())),
                preferred_element_type=jnp.float32,
            ).astype(jnp.bfloat16)
            rope = own[:, plain:].astype(jnp.float32)
            out_ref[h, :, rank:] = turned(rope[:, :half], rope[:, half:], cosine, sine)


def latent_kernel(place, rank, share, *refs):
    outer, inner, tp = place.outer, place.inner, place.tp_count
    tables = tp if share else 1
    n_rows, n_w = outer, tables * inner
    row_refs, w_refs = refs[:n_rows], refs[n_rows : n_rows + n_w]
    gain_ref, cos_ref, sin_ref, out_ref, rows, weight, sem_r, sem_w = refs[n_rows + n_w :]
    zi, xi, ti = place.indices()
    piece = w_refs[0].shape[1]
    block = piece * tables
    count = row_refs[0].shape[0]
    pairs = []
    for t in range(tables):
        owner = behind(ti, t, tp) if share else 0
        for k in range(inner):
            for j in range(outer):
                start = ((zi ^ j) * inner + (xi ^ k)) * block + owner * piece
                pairs.append(
                    (
                        w_refs[t * inner + k].at[j],
                        weight.at[pl.ds(pl.multiple_of(start, piece), piece)],
                    )
                )
    w_copies = copy_all(pairs, sem_w)
    r_copies = copy_all(
        [(row_refs[j], rows.at[pl.ds(j * count, count)]) for j in range(outer)], sem_r
    )
    for c in w_copies + r_copies:
        c.wait()
    pre = jnp.dot(rows[...], weight[...], preferred_element_type=jnp.float32)
    plain = pre[:, :rank]
    scale = lax.rsqrt(jnp.mean(plain * plain, axis=-1, keepdims=True) + epsilon)
    out_ref[:, :rank] = (plain * scale * gain_ref[...]).astype(jnp.bfloat16)
    rope = pre[:, rank:]
    half = rope.shape[1] // 2
    total = outer * count
    cosine, sine = cos_ref[cos_ref.shape[0] - total :], sin_ref[sin_ref.shape[0] - total :]
    out_ref[:, rank:] = turned(rope[:, :half], rope[:, half:], cosine, sine)


def gated_kernel(place, *refs):
    outer, inner, tp = place.outer, place.inner, place.tp_count
    n_rows = tp * outer
    row_refs, w_refs = refs[:n_rows], refs[n_rows : n_rows + inner]
    outs = refs[n_rows + inner : n_rows + inner + outer]
    rows, weight, sem_r, sem_w = refs[n_rows + inner + outer :]
    zi, xi, ti = place.indices()
    block = w_refs[0].shape[1]
    count = row_refs[0].shape[0]
    pairs = []
    for k in range(inner):
        for j in range(outer):
            start = ((zi ^ j) * inner + (xi ^ k)) * block
            pairs.append(
                (w_refs[k].at[j], weight.at[pl.ds(pl.multiple_of(start, block), block)])
            )
    w_copies = copy_all(pairs, sem_w)
    pairs = []
    for t in range(tp):
        owner = behind(ti, t, tp)
        for j in range(outer):
            start = j * tp * count + owner * count
            pairs.append(
                (
                    row_refs[t * outer + j],
                    rows.at[pl.ds(pl.multiple_of(start, count), count)],
                )
            )
    r_copies = copy_all(pairs, sem_r)
    for c in w_copies + r_copies:
        c.wait()
    chunk = tp * count
    width = outs[0].shape[1]
    for j in range(outer):
        pre = jnp.dot(
            rows[pl.ds(j * chunk, chunk)], weight[...], preferred_element_type=jnp.float32
        )
        value, gate = pre[:, :width], pre[:, width:]
        outs[j][...] = (value * jax.nn.sigmoid(gate)).astype(jnp.bfloat16)


def attention_kernel(place, scale, rank, q_ref, up_ref, *refs):
    outer, inner, tp = place.outer, place.inner, place.tp_count
    n_k = tp * inner
    key_refs = refs[:n_k]
    out_ref, lse_ref, keys, sem = refs[n_k:]
    zi, xi, ti = place.indices()
    heads, count, depth = q_ref.shape
    piece = key_refs[0].shape[0]
    share = piece // outer
    copies = copy_all(
        [(key_refs[n], keys.at[pl.ds(n * piece, piece)]) for n in range(n_k)], sem
    )
    lane = lax.broadcasted_iota(jnp.int32, (1, piece), 1)
    back = zi ^ lax.shift_right_logical(lane, share.bit_length() - 1)
    within = jnp.bitwise_and(lane, share - 1)
    parts = []
    for t in range(tp):
        owner = behind(ti, t, tp)
        for k in range(inner):
            parts.append((back * inner + (xi ^ k)) * count + owner * share + within)
    key_index = jnp.concatenate(parts, axis=1)
    first_row = (zi * inner + xi) * count
    together = math.gcd(heads, 4)
    size = together * count
    query_index = lax.broadcasted_iota(jnp.int32, (count, 1), 0) + first_row
    allowed = key_index <= jnp.concatenate([query_index] * together, axis=0)
    width = VALUE_HEAD_WIDTH
    sums = []
    for c in copies:
        c.wait()
    for g in range(heads // together):
        queries = q_ref[g * together : (g + 1) * together].reshape(size, depth)
        scores = lax.dot_general(
            queries, keys[...], (((1,), (1,)), ((), ())), preferred_element_type=jnp.float32
        )
        scores = jnp.where(allowed, scores, masked_score)
        top = jnp.max(scores, axis=-1, keepdims=True)
        weights = jnp.exp2((scores - top) * (scale * math.log2(math.e)))
        total = jnp.sum(weights, axis=-1, keepdims=True)
        weighted = jnp.dot(
            weights.astype(jnp.bfloat16), keys[:, :rank], preferred_element_type=jnp.float32
        )
        latent_out = (weighted / total).astype(jnp.bfloat16)
        group_sums = top * scale + jnp.log(total)
        for i in range(together):
            h = g * together + i
            part = slice(i * count, (i + 1) * count)
            sums.append(group_sums[part])
            out_ref[:, h * width : (h + 1) * width] = jnp.dot(
                latent_out[part],
                up_ref[:, h * width : (h + 1) * width],
                preferred_element_type=jnp.float32,
            ).astype(jnp.bfloat16)
    spare = [jnp.zeros((count, 128 - heads), jnp.float32)]
    lse_ref[...] = jnp.concatenate(sums + spare, axis=1).T[:heads]


def local(
    tokens,
    norm_gain,
    w_value,
    w_gate,
    conv_taps,
    conv_gain,
    w_query,
    latent_down_weight,
    latent_norm_gain,
    w_rope_key,
    key_up_weight,
    value_up_weight,
    w_merge_conv,
    w_merge_attn,
):
    place = Place()
    outer, inner, tp_count = place.outer, place.inner, place.tp_count
    zi, xi, ti = place.indices()
    row_count = tokens.shape[0]
    share = row_count // tp_count
    depth = latent_down_weight.shape[0]
    rank = latent_down_weight.shape[1]

    split_rows = depth % (16 * tp_count) == 0
    own_table = jnp.concatenate([latent_down_weight, w_rope_key], axis=1)
    if split_rows:
        piece = depth // tp_count
        own_table = lax.dynamic_slice_in_dim(own_table, ti * piece, piece, 0)
    own_table, w_value, w_gate = lax.optimization_barrier((own_table, w_value, w_gate))
    table_parts = place.outer_gather(own_table)

    width = w_value.shape[1] // outer
    columns = []
    for j in range(outer):
        start = (zi ^ j) * width
        block = jnp.concatenate(
            [
                lax.dynamic_slice_in_dim(w_value, start, width, 1),
                lax.dynamic_slice_in_dim(w_gate, start, width, 1),
            ],
            axis=1,
        )
        columns.append(block if j == 0 else place.outer_swap(block, j))

    table = jnp.stack(table_parts)
    table, tokens = lax.optimization_barrier((table, tokens))
    tables = place.inner_gather(table)

    gathered = lax.all_gather(tokens, "tp", axis=1, tiled=True)
    features = gathered.astype(jnp.float32)
    normed = (
        features
        * lax.rsqrt(jnp.mean(features * features, axis=-1, keepdims=True) + epsilon)
        * norm_gain
    ).astype(jnp.bfloat16)

    own_rows = lax.dynamic_slice_in_dim(normed, ti * share, share, 0)
    rows = place.outer_gather(own_rows)
    weight_block = jnp.stack(columns)
    weight_block, query_rows = lax.optimization_barrier((weight_block, normed))
    weight_blocks = place.inner_gather(weight_block)

    bf16 = jnp.bfloat16
    model = normed.shape[1]
    head_count = key_up_weight.shape[1] // PLAIN_QK_WIDTH
    query_index = lax.axis_index("sp") * row_count + jnp.arange(row_count, dtype=jnp.int32)
    back = zi ^ jnp.arange(outer, dtype=jnp.int32)
    key_index = (
        ((back * inner + xi) * row_count + ti * share)[:, None]
        + jnp.arange(share, dtype=jnp.int32)[None, :]
    ).reshape(-1)
    angles = angles_at(
        jnp.concatenate([query_index, key_index]).astype(jnp.float32), QK_ROPE
    )
    cosine, sine = jnp.cos(angles), jnp.sin(angles)

    query_width = w_query.shape[1]
    queries = pl.pallas_call(
        functools.partial(query_kernel, rank),
        out_shape=jax.ShapeDtypeStruct((head_count, row_count, rank + QK_ROPE), bf16),
        in_specs=[whole_vmem()] + [pl.BlockSpec(memory_space=pltpu.HBM)] * 2 + [whole_vmem()] * 2,
        out_specs=whole_vmem(),
        scratch_shapes=[
            pltpu.VMEM((model, query_width), bf16),
            pltpu.VMEM(key_up_weight.shape, bf16),
            pltpu.SemaphoreType.DMA((head_count // 2 + 1,)),
        ],
        compiler_params=pltpu.CompilerParams(vmem_limit_bytes=52 << 20),
        cost_estimate=pl.CostEstimate(
            flops=2 * row_count * model * query_width,
            bytes_accessed=2 * model * query_width,
            transcendentals=0,
        ),
        name="queries",
    )(query_rows, w_query, key_up_weight, cosine, sine)

    rows, tables, _ = lax.optimization_barrier((rows, tables, queries))
    if split_rows:
        tables = sum(place.tp_gather(tables), [])

    latent = pl.pallas_call(
        functools.partial(latent_kernel, place, rank, split_rows),
        out_shape=jax.ShapeDtypeStruct((outer * share, rank + QK_ROPE), bf16),
        in_specs=any_specs(outer + len(tables)) + [whole_vmem()] * 3,
        out_specs=whole_vmem(),
        scratch_shapes=[
            pltpu.VMEM((outer * share, model), bf16),
            pltpu.VMEM((model, rank + QK_ROPE), bf16),
            pltpu.SemaphoreType.DMA((outer,)),
            pltpu.SemaphoreType.DMA((len(tables) * outer,)),
        ],
        compiler_params=pltpu.CompilerParams(vmem_limit_bytes=16 << 20),
        cost_estimate=pl.CostEstimate(
            flops=2 * outer * share * model * (rank + QK_ROPE),
            bytes_accessed=2 * model * (rank + QK_ROPE + outer * share),
            transcendentals=0,
        ),
        name="latents",
    )(*rows, *tables, latent_norm_gain[None, :], cosine, sine)
    _, *weight_blocks = lax.optimization_barrier((latent, *weight_blocks))
    latents = place.inner_gather(latent)
    latents = sum(place.tp_gather(latents), [])

    all_rows = sum(place.tp_gather(rows), [])
    gated = pl.pallas_call(
        functools.partial(gated_kernel, place),
        out_shape=[jax.ShapeDtypeStruct((row_count, width), bf16)] * outer,
        in_specs=any_specs(len(all_rows) + inner),
        out_specs=[whole_vmem()] * outer,
        scratch_shapes=[
            pltpu.VMEM((outer * row_count, model), bf16),
            pltpu.VMEM((model, 2 * width), bf16),
            pltpu.SemaphoreType.DMA((len(all_rows),)),
            pltpu.SemaphoreType.DMA((inner * outer,)),
        ],
        compiler_params=pltpu.CompilerParams(vmem_limit_bytes=24 << 20),
        cost_estimate=pl.CostEstimate(
            flops=4 * outer * row_count * model * width,
            bytes_accessed=2 * model * (2 * width + outer * row_count),
            transcendentals=outer * row_count * width,
        ),
        name="gated",
    )(*all_rows, *weight_blocks)
    home = [gated[0]] + [place.outer_swap(gated[j], j) for j in range(1, outer)]
    gated_rows = jnp.concatenate(untangled(home, zi), axis=1)

    conv_reach = conv_taps.shape[0] - 1
    prior_rows = lax.ppermute(
        gated_rows[row_count - conv_reach :],
        "sp",
        [(i, i + 1) for i in range(place.sp_count - 1)],
    )
    padded = jnp.concatenate([prior_rows, gated_rows], axis=0).astype(jnp.float32)
    mixed = jnp.zeros(gated_rows.shape, jnp.float32)
    for tap_index in range(conv_taps.shape[0]):
        mixed = (
            mixed
            + conv_taps[tap_index].astype(jnp.float32) * padded[tap_index : tap_index + row_count]
        )
    channel_total = mixed.shape[1] * tp_count
    stats = jnp.stack([jnp.sum(mixed, axis=1), jnp.sum(mixed * mixed, axis=1)])
    stat_sum, stat_squares = sum(
        [place.tp_shift(stats, t) for t in range(1, tp_count)], start=stats
    )
    channel_mean = stat_sum / channel_total
    channel_var = stat_squares / channel_total - channel_mean * channel_mean
    conv_out = jax.nn.silu(
        (mixed - channel_mean[:, None]) * lax.rsqrt(channel_var + epsilon)[:, None] * conv_gain
    ).astype(bf16)

    score_scale = (PLAIN_QK_WIDTH + QK_ROPE) ** (-0.5)
    key_total = place.sp_count * row_count
    attention, log_sums = pl.pallas_call(
        functools.partial(attention_kernel, place, score_scale, rank),
        out_shape=[
            jax.ShapeDtypeStruct((row_count, head_count * VALUE_HEAD_WIDTH), bf16),
            jax.ShapeDtypeStruct((head_count, row_count), jnp.float32),
        ],
        in_specs=[whole_vmem()] * 2 + any_specs(len(latents)),
        out_specs=[whole_vmem()] * 2,
        scratch_shapes=[
            pltpu.VMEM((key_total, rank + QK_ROPE), bf16),
            pltpu.SemaphoreType.DMA((len(latents),)),
        ],
        compiler_params=pltpu.CompilerParams(vmem_limit_bytes=40 << 20),
        cost_estimate=pl.CostEstimate(
            flops=2 * row_count * head_count * key_total * (2 * rank + QK_ROPE),
            bytes_accessed=2 * key_total * (rank + QK_ROPE),
            transcendentals=row_count * head_count * key_total,
        ),
        name="attention",
    )(queries, value_up_weight, *latents)

    partial = (
        jnp.dot(conv_out, w_merge_conv, preferred_element_type=jnp.float32)
        + jnp.dot(attention, w_merge_attn, preferred_element_type=jnp.float32)
    ).astype(bf16)
    merged = lax.dynamic_slice_in_dim(partial, ti * share, share, 0).astype(jnp.float32)
    for t in range(1, tp_count):
        away = lax.dynamic_slice_in_dim(partial, lax.rem(ti + t, tp_count) * share, share, 0)
        merged = merged + place.tp_shift(away, t).astype(jnp.float32)
    return (merged.astype(bf16), log_sums.T)


def solution(mesh):
    return jax.shard_map(
        local,
        mesh=mesh,
        in_specs=(
            P("sp", "tp"),
            P(),
            P("sp", "tp"),
            P("sp", "tp"),
            P(None, "tp"),
            P("tp"),
            P(None, "tp"),
            P("sp", None),
            P(),
            P("sp", None),
            P(None, "tp"),
            P(None, "tp"),
            P("tp", None),
            P("tp", None),
        ),
        out_specs=(P(("sp", "tp"), None), P("sp", "tp")),
        check_vma=False,
    )
```

```python
import functools
import math

import jax
import jax.numpy as jnp
from jax import lax
from jax.experimental import pallas as pl
from jax.experimental.pallas import tpu as pltpu
from jax.sharding import PartitionSpec as P


PLAIN_QK_WIDTH = 128
QK_ROPE = 64
VALUE_HEAD_WIDTH = 128


epsilon = 1e-06
rope_base = 10000.0
masked_score = -1e30


def angles_at(positions, width):
    inverse = rope_base ** (-2.0 * jnp.arange(width // 2, dtype=jnp.float32) / width)
    return positions[:, None] * inverse[None, :]


class Place:
    def __init__(self):
        self.sp_count = lax.axis_size("sp")
        self.tp_count = lax.axis_size("tp")
        self.inner = math.gcd(self.sp_count, 4)
        self.outer = self.sp_count // self.inner

    def indices(self):
        index = lax.axis_index("sp")
        return index // self.inner, index % self.inner, lax.axis_index("tp")

    def outer_swap(self, block, mask):
        mask = mask * self.inner
        return lax.ppermute(block, "sp", [(i, i ^ mask) for i in range(self.sp_count)])

    def inner_swap(self, block, mask):
        return lax.ppermute(block, "sp", [(i, i ^ mask) for i in range(self.sp_count)])

    def tp_shift(self, block, distance):
        route = [(i, (i + distance) % self.tp_count) for i in range(self.tp_count)]
        return lax.ppermute(block, "tp", route)

    def outer_gather(self, block):
        return [block] + [self.outer_swap(block, j) for j in range(1, self.outer)]

    def inner_gather(self, block):
        return [block] + [self.inner_swap(block, k) for k in range(1, self.inner)]

    def tp_gather(self, blocks):
        return [blocks] + [
            [self.tp_shift(b, t) for b in blocks] for t in range(1, self.tp_count)
        ]


def behind(index, distance, count):
    return lax.rem(index - distance + count, count)


def untangled(blocks, index):
    bit = 1
    while bit < len(blocks):
        flag = (index & bit) > 0
        blocks = [jnp.where(flag, blocks[i ^ bit], b) for i, b in enumerate(blocks)]
        bit *= 2
    return blocks


def copy_all(pairs, sem):
    copies = [pltpu.make_async_copy(s, d, sem.at[n]) for n, (s, d) in enumerate(pairs)]
    for c in copies:
        c.start()
    return copies


def whole_vmem():
    return pl.BlockSpec(memory_space=pltpu.VMEM)


def turned(first, second, cosine, sine):
    return jnp.concatenate(
        [first * cosine - second * sine, first * sine + second * cosine], axis=-1
    ).astype(jnp.bfloat16)


def query_kernel(rank, normed_ref, w_ref, up_ref, cos_ref, sin_ref, out_ref, w, up, sem):
    heads, count, _ = out_ref.shape
    plain, half = PLAIN_QK_WIDTH, QK_ROPE // 2
    head = plain + QK_ROPE
    span = 2 * head
    pairs = heads // 2
    copies = copy_all(
        [
            (w_ref.at[:, p * span : (p + 1) * span], w.at[:, p * span : (p + 1) * span])
            for p in range(pairs)
        ]
        + [(up_ref, up)],
        sem,
    )
    cosine, sine = cos_ref[:count], sin_ref[:count]
    for p in range(pairs):
        copies[p].wait()
        query = jnp.dot(
            normed_ref[...], w[:, p * span : (p + 1) * span], preferred_element_type=jnp.float32
        ).astype(jnp.bfloat16)
        if p == 0:
            copies[pairs].wait()
        for i in range(2):
            h = 2 * p + i
            own = query[:, i * head : (i + 1) * head]
            out_ref[h, :, :rank] = lax.dot_general(
                own[:, :plain],
                up[:, h * plain : (h + 1) * plain],
                (((1,), (1,)), ((), ())),
                preferred_element_type=jnp.float32,
            ).astype(jnp.bfloat16)
            rope = own[:, plain:].astype(jnp.float32)
            out_ref[h, :, rank:] = turned(rope[:, :half], rope[:, half:], cosine, sine)


def latent_kernel(place, rank, share, *refs):
    outer, inner, tp = place.outer, place.inner, place.tp_count
    tables = tp if share else 1
    n_rows, n_w = outer, tables * inner
    row_refs, w_refs = refs[:n_rows], refs[n_rows : n_rows + n_w]
    gain_ref, cos_ref, sin_ref, out_ref, rows, weight = refs[n_rows + n_w :]
    zi, xi, ti = place.indices()
    piece = w_refs[0].shape[1]
    block = piece * tables
    count = row_refs[0].shape[0]
    for t in range(tables):
        owner = behind(ti, t, tp) if share else 0
        for k in range(inner):
            for j in range(outer):
                start = ((zi ^ j) * inner + (xi ^ k)) * block + owner * piece
                weight[pl.ds(pl.multiple_of(start, piece), piece)] = w_refs[t * inner + k][j]
    for j in range(outer):
        rows[j * count : (j + 1) * count] = row_refs[j][...]
    pre = jnp.dot(rows[...], weight[...], preferred_element_type=jnp.float32)
    plain = pre[:, :rank]
    scale = lax.rsqrt(jnp.mean(plain * plain, axis=-1, keepdims=True) + epsilon)
    out_ref[:, :rank] = (plain * scale * gain_ref[...]).astype(jnp.bfloat16)
    rope = pre[:, rank:]
    half = rope.shape[1] // 2
    total = outer * count
    cosine, sine = cos_ref[cos_ref.shape[0] - total :], sin_ref[sin_ref.shape[0] - total :]
    out_ref[:, rank:] = turned(rope[:, :half], rope[:, half:], cosine, sine)


def gated_kernel(place, *refs):
    outer, inner, tp = place.outer, place.inner, place.tp_count
    n_rows = tp * outer
    row_refs, w_refs = refs[:n_rows], refs[n_rows : n_rows + inner]
    outs = refs[n_rows + inner : n_rows + inner + outer]
    rows, weight = refs[n_rows + inner + outer :]
    zi, xi, ti = place.indices()
    block = w_refs[0].shape[1]
    count = row_refs[0].shape[0]
    for k in range(inner):
        for j in range(outer):
            start = ((zi ^ j) * inner + (xi ^ k)) * block
            weight[pl.ds(pl.multiple_of(start, block), block)] = w_refs[k][j]
    for t in range(tp):
        owner = behind(ti, t, tp)
        for j in range(outer):
            start = j * tp * count + owner * count
            rows[pl.ds(pl.multiple_of(start, count), count)] = row_refs[t * outer + j][...]
    chunk = tp * count
    width = outs[0].shape[1]
    pre = jnp.dot(rows[...], weight[...], preferred_element_type=jnp.float32)
    for j in range(outer):
        part = pre[j * chunk : (j + 1) * chunk]
        value, gate = part[:, :width], part[:, width:]
        outs[j][...] = (value * jax.nn.sigmoid(gate)).astype(jnp.bfloat16)


def attention_kernel(place, scale, rank, q_ref, up_ref, *refs):
    outer, inner, tp = place.outer, place.inner, place.tp_count
    n_k = tp * inner
    key_refs = refs[:n_k]
    out_ref, lse_ref, keys = refs[n_k:]
    zi, xi, ti = place.indices()
    heads, count, depth = q_ref.shape
    piece = key_refs[0].shape[0]
    share = piece // outer
    for n in range(n_k):
        keys[n * piece : (n + 1) * piece] = key_refs[n][...]
    lane = lax.broadcasted_iota(jnp.int32, (1, piece), 1)
    back = zi ^ lax.shift_right_logical(lane, share.bit_length() - 1)
    within = jnp.bitwise_and(lane, share - 1)
    parts = []
    for t in range(tp):
        owner = behind(ti, t, tp)
        for k in range(inner):
            parts.append((back * inner + (xi ^ k)) * count + owner * share + within)
    key_index = jnp.concatenate(parts, axis=1)
    first_row = (zi * inner + xi) * count
    together = math.gcd(heads, 4)
    size = together * count
    query_index = lax.broadcasted_iota(jnp.int32, (count, 1), 0) + first_row
    allowed = key_index <= jnp.concatenate([query_index] * together, axis=0)
    width = VALUE_HEAD_WIDTH
    sums = []
    for g in range(heads // together):
        queries = q_ref[g * together : (g + 1) * together].reshape(size, depth)
        scores = lax.dot_general(
            queries, keys[...], (((1,), (1,)), ((), ())), preferred_element_type=jnp.float32
        )
        scores = jnp.where(allowed, scores, masked_score)
        top = jnp.max(scores, axis=-1, keepdims=True)
        weights = jnp.exp2((scores - top) * (scale * math.log2(math.e)))
        total = jnp.sum(weights, axis=-1, keepdims=True)
        weighted = jnp.dot(
            weights.astype(jnp.bfloat16), keys[:, :rank], preferred_element_type=jnp.float32
        )
        latent_out = (weighted / total).astype(jnp.bfloat16)
        group_sums = top * scale + jnp.log(total)
        for i in range(together):
            h = g * together + i
            part = slice(i * count, (i + 1) * count)
            sums.append(group_sums[part])
            out_ref[:, h * width : (h + 1) * width] = jnp.dot(
                latent_out[part],
                up_ref[:, h * width : (h + 1) * width],
                preferred_element_type=jnp.float32,
            ).astype(jnp.bfloat16)
    spare = [jnp.zeros((count, 128 - heads), jnp.float32)]
    lse_ref[...] = jnp.concatenate(sums + spare, axis=1).T[:heads]


def local(
    tokens,
    norm_gain,
    w_value,
    w_gate,
    conv_taps,
    conv_gain,
    w_query,
    latent_down_weight,
    latent_norm_gain,
    w_rope_key,
    key_up_weight,
    value_up_weight,
    w_merge_conv,
    w_merge_attn,
):
    place = Place()
    outer, inner, tp_count = place.outer, place.inner, place.tp_count
    zi, xi, ti = place.indices()
    row_count = tokens.shape[0]
    share = row_count // tp_count
    depth = latent_down_weight.shape[0]
    rank = latent_down_weight.shape[1]

    split_rows = depth % (16 * tp_count) == 0
    own_table = jnp.concatenate([latent_down_weight, w_rope_key], axis=1)
    if split_rows:
        piece = depth // tp_count
        own_table = lax.dynamic_slice_in_dim(own_table, ti * piece, piece, 0)
    own_table, w_value, w_gate = lax.optimization_barrier((own_table, w_value, w_gate))
    table_parts = place.outer_gather(own_table)

    width = w_value.shape[1] // outer
    columns = []
    for j in range(outer):
        start = (zi ^ j) * width
        block = jnp.concatenate(
            [
                lax.dynamic_slice_in_dim(w_value, start, width, 1),
                lax.dynamic_slice_in_dim(w_gate, start, width, 1),
            ],
            axis=1,
        )
        columns.append(block if j == 0 else place.outer_swap(block, j))

    table = jnp.stack(table_parts)
    table, tokens = lax.optimization_barrier((table, tokens))
    tables = place.inner_gather(table)

    gathered = lax.all_gather(tokens, "tp", axis=1, tiled=True)
    features = gathered.astype(jnp.float32)
    normed = (
        features
        * lax.rsqrt(jnp.mean(features * features, axis=-1, keepdims=True) + epsilon)
        * norm_gain
    ).astype(jnp.bfloat16)

    own_rows = lax.dynamic_slice_in_dim(normed, ti * share, share, 0)
    rows = place.outer_gather(own_rows)
    weight_block = jnp.stack(columns)
    weight_block, query_rows = lax.optimization_barrier((weight_block, normed))
    weight_blocks = place.inner_gather(weight_block)

    bf16 = jnp.bfloat16
    model = normed.shape[1]
    head_count = key_up_weight.shape[1] // PLAIN_QK_WIDTH
    query_index = lax.axis_index("sp") * row_count + jnp.arange(row_count, dtype=jnp.int32)
    back = zi ^ jnp.arange(outer, dtype=jnp.int32)
    key_index = (
        ((back * inner + xi) * row_count + ti * share)[:, None]
        + jnp.arange(share, dtype=jnp.int32)[None, :]
    ).reshape(-1)
    angles = angles_at(
        jnp.concatenate([query_index, key_index]).astype(jnp.float32), QK_ROPE
    )
    cosine, sine = jnp.cos(angles), jnp.sin(angles)

    query_width = w_query.shape[1]
    queries = pl.pallas_call(
        functools.partial(query_kernel, rank),
        out_shape=jax.ShapeDtypeStruct((head_count, row_count, rank + QK_ROPE), bf16),
        in_specs=[whole_vmem()] + [pl.BlockSpec(memory_space=pltpu.HBM)] * 2 + [whole_vmem()] * 2,
        out_specs=whole_vmem(),
        scratch_shapes=[
            pltpu.VMEM((model, query_width), bf16),
            pltpu.VMEM(key_up_weight.shape, bf16),
            pltpu.SemaphoreType.DMA((head_count // 2 + 1,)),
        ],
        compiler_params=pltpu.CompilerParams(vmem_limit_bytes=52 << 20),
        cost_estimate=pl.CostEstimate(
            flops=2 * row_count * model * query_width,
            bytes_accessed=2 * model * query_width,
            transcendentals=0,
        ),
        name="queries",
    )(query_rows, w_query, key_up_weight, cosine, sine)

    rows, tables, _ = lax.optimization_barrier((rows, tables, queries))
    if split_rows:
        tables = sum(place.tp_gather(tables), [])

    latent = pl.pallas_call(
        functools.partial(latent_kernel, place, rank, split_rows),
        out_shape=jax.ShapeDtypeStruct((outer * share, rank + QK_ROPE), bf16),
        in_specs=[whole_vmem()] * (outer + len(tables) + 3),
        out_specs=whole_vmem(),
        scratch_shapes=[
            pltpu.VMEM((outer * share, model), bf16),
            pltpu.VMEM((model, rank + QK_ROPE), bf16),
        ],
        compiler_params=pltpu.CompilerParams(vmem_limit_bytes=16 << 20),
        cost_estimate=pl.CostEstimate(
            flops=2 * outer * share * model * (rank + QK_ROPE),
            bytes_accessed=2 * model * (rank + QK_ROPE + outer * share),
            transcendentals=0,
        ),
        name="latents",
    )(*rows, *tables, latent_norm_gain[None, :], cosine, sine)
    _, *weight_blocks = lax.optimization_barrier((latent, *weight_blocks))
    latents = place.inner_gather(latent)
    latents = sum(place.tp_gather(latents), [])

    all_rows = sum(place.tp_gather(rows), [])
    gated = pl.pallas_call(
        functools.partial(gated_kernel, place),
        out_shape=[jax.ShapeDtypeStruct((row_count, width), bf16)] * outer,
        in_specs=[whole_vmem()] * (len(all_rows) + inner),
        out_specs=[whole_vmem()] * outer,
        scratch_shapes=[
            pltpu.VMEM((outer * row_count, model), bf16),
            pltpu.VMEM((model, 2 * width), bf16),
        ],
        compiler_params=pltpu.CompilerParams(vmem_limit_bytes=24 << 20),
        cost_estimate=pl.CostEstimate(
            flops=4 * outer * row_count * model * width,
            bytes_accessed=2 * model * (2 * width + outer * row_count),
            transcendentals=outer * row_count * width,
        ),
        name="gated",
    )(*all_rows, *weight_blocks)
    home = [gated[0]] + [place.outer_swap(gated[j], j) for j in range(1, outer)]
    gated_rows = jnp.concatenate(untangled(home, zi), axis=1)

    conv_reach = conv_taps.shape[0] - 1
    prior_rows = lax.ppermute(
        gated_rows[row_count - conv_reach :],
        "sp",
        [(i, i + 1) for i in range(place.sp_count - 1)],
    )
    score_scale = (PLAIN_QK_WIDTH + QK_ROPE) ** (-0.5)
    key_total = place.sp_count * row_count
    attention, log_sums = pl.pallas_call(
        functools.partial(attention_kernel, place, score_scale, rank),
        out_shape=[
            jax.ShapeDtypeStruct((row_count, head_count * VALUE_HEAD_WIDTH), bf16),
            jax.ShapeDtypeStruct((head_count, row_count), jnp.float32),
        ],
        in_specs=[whole_vmem()] * (2 + len(latents)),
        out_specs=[whole_vmem()] * 2,
        scratch_shapes=[
            pltpu.VMEM((key_total, rank + QK_ROPE), bf16),
        ],
        compiler_params=pltpu.CompilerParams(vmem_limit_bytes=32 << 20),
        cost_estimate=pl.CostEstimate(
            flops=2 * row_count * head_count * key_total * (2 * rank + QK_ROPE),
            bytes_accessed=2 * key_total * (rank + QK_ROPE),
            transcendentals=row_count * head_count * key_total,
        ),
        name="attention",
    )(queries, value_up_weight, *latents)

    prior_rows, gated_rows, _ = lax.optimization_barrier((prior_rows, gated_rows, attention))
    padded = jnp.concatenate([prior_rows, gated_rows], axis=0).astype(jnp.float32)
    mixed = jnp.zeros(gated_rows.shape, jnp.float32)
    for tap_index in range(conv_taps.shape[0]):
        mixed = (
            mixed
            + conv_taps[tap_index].astype(jnp.float32) * padded[tap_index : tap_index + row_count]
        )
    channel_total = mixed.shape[1] * tp_count
    stats = jnp.stack([jnp.sum(mixed, axis=1), jnp.sum(mixed * mixed, axis=1)])
    stat_sum, stat_squares = sum(
        [place.tp_shift(stats, t) for t in range(1, tp_count)], start=stats
    )
    channel_mean = stat_sum / channel_total
    channel_var = stat_squares / channel_total - channel_mean * channel_mean
    conv_out = jax.nn.silu(
        (mixed - channel_mean[:, None]) * lax.rsqrt(channel_var + epsilon)[:, None] * conv_gain
    ).astype(bf16)

    partial = (
        jnp.dot(conv_out, w_merge_conv, preferred_element_type=jnp.float32)
        + jnp.dot(attention, w_merge_attn, preferred_element_type=jnp.float32)
    ).astype(bf16)
    merged = lax.dynamic_slice_in_dim(partial, ti * share, share, 0).astype(jnp.float32)
    for t in range(1, tp_count):
        away = lax.dynamic_slice_in_dim(partial, lax.rem(ti + t, tp_count) * share, share, 0)
        merged = merged + place.tp_shift(away, t).astype(jnp.float32)
    return (merged.astype(bf16), log_sums.T)


def solution(mesh):
    return jax.shard_map(
        local,
        mesh=mesh,
        in_specs=(
            P("sp", "tp"),
            P(),
            P("sp", "tp"),
            P("sp", "tp"),
            P(None, "tp"),
            P("tp"),
            P(None, "tp"),
            P("sp", None),
            P(),
            P("sp", None),
            P(None, "tp"),
            P(None, "tp"),
            P("tp", None),
            P("tp", None),
        ),
        out_specs=(P(("sp", "tp"), None), P("sp", "tp")),
        check_vma=False,
    )
```

```python
import functools
import math

import jax
import jax.numpy as jnp
from jax import lax
from jax.experimental import pallas as pl
from jax.experimental.pallas import tpu as pltpu
from jax.sharding import PartitionSpec as P


PLAIN_QK_WIDTH = 128
QK_ROPE = 64
VALUE_HEAD_WIDTH = 128


epsilon = 1e-06
rope_base = 10000.0
masked_score = -1e30


def angles_at(positions, width):
    inverse = rope_base ** (-2.0 * jnp.arange(width // 2, dtype=jnp.float32) / width)
    return positions[:, None] * inverse[None, :]


class Place:
    def __init__(self):
        self.sp_count = lax.axis_size("sp")
        self.tp_count = lax.axis_size("tp")
        self.inner = math.gcd(self.sp_count, 4)
        self.outer = self.sp_count // self.inner

    def indices(self):
        index = lax.axis_index("sp")
        return index // self.inner, index % self.inner, lax.axis_index("tp")

    def outer_swap(self, block, mask):
        mask = mask * self.inner
        return lax.ppermute(block, "sp", [(i, i ^ mask) for i in range(self.sp_count)])

    def inner_swap(self, block, mask):
        return lax.ppermute(block, "sp", [(i, i ^ mask) for i in range(self.sp_count)])

    def tp_shift(self, block, distance):
        route = [(i, (i + distance) % self.tp_count) for i in range(self.tp_count)]
        return lax.ppermute(block, "tp", route)

    def outer_gather(self, block):
        return [block] + [self.outer_swap(block, j) for j in range(1, self.outer)]

    def inner_gather(self, block):
        return [block] + [self.inner_swap(block, k) for k in range(1, self.inner)]

    def tp_gather(self, blocks):
        return [blocks] + [
            [self.tp_shift(b, t) for b in blocks] for t in range(1, self.tp_count)
        ]


def behind(index, distance, count):
    return lax.rem(index - distance + count, count)


def untangled(blocks, index):
    bit = 1
    while bit < len(blocks):
        flag = (index & bit) > 0
        blocks = [jnp.where(flag, blocks[i ^ bit], b) for i, b in enumerate(blocks)]
        bit *= 2
    return blocks


def copy_all(pairs, sem):
    copies = [pltpu.make_async_copy(s, d, sem.at[n]) for n, (s, d) in enumerate(pairs)]
    for c in copies:
        c.start()
    return copies


def whole_vmem():
    return pl.BlockSpec(memory_space=pltpu.VMEM)


def turned(first, second, cosine, sine):
    return jnp.concatenate(
        [first * cosine - second * sine, first * sine + second * cosine], axis=-1
    ).astype(jnp.bfloat16)


def query_kernel(rank, normed_ref, w_ref, up_ref, cos_ref, sin_ref, out_ref, w, up, sem):
    heads, count, _ = out_ref.shape
    plain, half = PLAIN_QK_WIDTH, QK_ROPE // 2
    head = plain + QK_ROPE
    span = 2 * head
    pairs = heads // 2
    copies = copy_all(
        [
            (w_ref.at[:, p * span : (p + 1) * span], w.at[:, p * span : (p + 1) * span])
            for p in range(pairs)
        ]
        + [(up_ref, up)],
        sem,
    )
    cosine, sine = cos_ref[:count], sin_ref[:count]
    for p in range(pairs):
        copies[p].wait()
        query = jnp.dot(
            normed_ref[...], w[:, p * span : (p + 1) * span], preferred_element_type=jnp.float32
        ).astype(jnp.bfloat16)
        if p == 0:
            copies[pairs].wait()
        for i in range(2):
            h = 2 * p + i
            own = query[:, i * head : (i + 1) * head]
            out_ref[h, :, :rank] = lax.dot_general(
                own[:, :plain],
                up[:, h * plain : (h + 1) * plain],
                (((1,), (1,)), ((), ())),
                preferred_element_type=jnp.float32,
            ).astype(jnp.bfloat16)
            rope = own[:, plain:].astype(jnp.float32)
            out_ref[h, :, rank:] = turned(rope[:, :half], rope[:, half:], cosine, sine)


def latent_kernel(place, rank, share, *refs):
    outer, inner, tp = place.outer, place.inner, place.tp_count
    tables = tp if share else 1
    n_rows, n_w = outer, tables * inner
    row_refs, w_refs = refs[:n_rows], refs[n_rows : n_rows + n_w]
    gain_ref, cos_ref, sin_ref, out_ref, rows, weight = refs[n_rows + n_w :]
    zi, xi, ti = place.indices()
    piece = w_refs[0].shape[1]
    block = piece * tables
    count = row_refs[0].shape[0]
    for t in range(tables):
        owner = behind(ti, t, tp) if share else 0
        for k in range(inner):
            for j in range(outer):
                start = ((zi ^ j) * inner + (xi ^ k)) * block + owner * piece
                weight[pl.ds(pl.multiple_of(start, piece), piece)] = w_refs[t * inner + k][j]
    for j in range(outer):
        rows[j * count : (j + 1) * count] = row_refs[j][...]
    pre = jnp.dot(rows[...], weight[...], preferred_element_type=jnp.float32)
    plain = pre[:, :rank]
    scale = lax.rsqrt(jnp.mean(plain * plain, axis=-1, keepdims=True) + epsilon)
    out_ref[:, :rank] = (plain * scale * gain_ref[...]).astype(jnp.bfloat16)
    rope = pre[:, rank:]
    half = rope.shape[1] // 2
    total = outer * count
    cosine, sine = cos_ref[cos_ref.shape[0] - total :], sin_ref[sin_ref.shape[0] - total :]
    out_ref[:, rank:] = turned(rope[:, :half], rope[:, half:], cosine, sine)


def gated_kernel(place, *refs):
    outer, inner, tp = place.outer, place.inner, place.tp_count
    n_rows = tp * outer
    row_refs, w_refs = refs[:n_rows], refs[n_rows : n_rows + inner]
    outs = refs[n_rows + inner : n_rows + inner + outer]
    rows, weight = refs[n_rows + inner + outer :]
    zi, xi, ti = place.indices()
    block = w_refs[0].shape[1]
    count = row_refs[0].shape[0]
    for k in range(inner):
        for j in range(outer):
            start = ((zi ^ j) * inner + (xi ^ k)) * block
            weight[pl.ds(pl.multiple_of(start, block), block)] = w_refs[k][j]
    for t in range(tp):
        owner = behind(ti, t, tp)
        for j in range(outer):
            start = j * tp * count + owner * count
            rows[pl.ds(pl.multiple_of(start, count), count)] = row_refs[t * outer + j][...]
    chunk = tp * count
    width = outs[0].shape[1]
    pre = jnp.dot(rows[...], weight[...], preferred_element_type=jnp.float32)
    for j in range(outer):
        part = pre[j * chunk : (j + 1) * chunk]
        value, gate = part[:, :width], part[:, width:]
        outs[j][...] = (value * jax.nn.sigmoid(gate)).astype(jnp.bfloat16)


def attention_kernel(place, scale, rank, q_ref, up_ref, conv_ref, wc_ref, wa_ref, *refs):
    outer, inner, tp = place.outer, place.inner, place.tp_count
    n_k = tp * inner
    key_refs = refs[:n_k]
    out_ref, lse_ref, keys, attended, conv_weight, attn_weight, sem = refs[n_k:]
    copies = copy_all([(wc_ref, conv_weight), (wa_ref, attn_weight)], sem)
    zi, xi, ti = place.indices()
    heads, count, depth = q_ref.shape
    piece = key_refs[0].shape[0]
    share = piece // outer
    for n in range(n_k):
        keys[n * piece : (n + 1) * piece] = key_refs[n][...]
    lane = lax.broadcasted_iota(jnp.int32, (1, piece), 1)
    back = zi ^ lax.shift_right_logical(lane, share.bit_length() - 1)
    within = jnp.bitwise_and(lane, share - 1)
    parts = []
    for t in range(tp):
        owner = behind(ti, t, tp)
        for k in range(inner):
            parts.append((back * inner + (xi ^ k)) * count + owner * share + within)
    key_index = jnp.concatenate(parts, axis=1)
    first_row = (zi * inner + xi) * count
    together = math.gcd(heads, 4)
    size = together * count
    query_index = lax.broadcasted_iota(jnp.int32, (count, 1), 0) + first_row
    allowed = key_index <= jnp.concatenate([query_index] * together, axis=0)
    width = VALUE_HEAD_WIDTH
    sums = []
    for g in range(heads // together):
        queries = q_ref[g * together : (g + 1) * together].reshape(size, depth)
        scores = lax.dot_general(
            queries, keys[...], (((1,), (1,)), ((), ())), preferred_element_type=jnp.float32
        )
        scores = jnp.where(allowed, scores, masked_score)
        top = jnp.max(scores, axis=-1, keepdims=True)
        weights = jnp.exp2((scores - top) * (scale * math.log2(math.e)))
        total = jnp.sum(weights, axis=-1, keepdims=True)
        weighted = jnp.dot(
            weights.astype(jnp.bfloat16), keys[:, :rank], preferred_element_type=jnp.float32
        )
        latent_out = (weighted / total).astype(jnp.bfloat16)
        group_sums = top * scale + jnp.log(total)
        for i in range(together):
            h = g * together + i
            part = slice(i * count, (i + 1) * count)
            sums.append(group_sums[part])
            attended[:, h * width : (h + 1) * width] = jnp.dot(
                latent_out[part],
                up_ref[:, h * width : (h + 1) * width],
                preferred_element_type=jnp.float32,
            ).astype(jnp.bfloat16)
    spare = [jnp.zeros((count, 128 - heads), jnp.float32)]
    lse_ref[...] = jnp.concatenate(sums + spare, axis=1).T[:heads]
    for c in copies:
        c.wait()
    out_ref[...] = (
        jnp.dot(conv_ref[...], conv_weight[...], preferred_element_type=jnp.float32)
        + jnp.dot(attended[...], attn_weight[...], preferred_element_type=jnp.float32)
    ).astype(jnp.bfloat16)


def local(
    tokens,
    norm_gain,
    w_value,
    w_gate,
    conv_taps,
    conv_gain,
    w_query,
    latent_down_weight,
    latent_norm_gain,
    w_rope_key,
    key_up_weight,
    value_up_weight,
    w_merge_conv,
    w_merge_attn,
):
    place = Place()
    outer, inner, tp_count = place.outer, place.inner, place.tp_count
    zi, xi, ti = place.indices()
    row_count = tokens.shape[0]
    share = row_count // tp_count
    depth = latent_down_weight.shape[0]
    rank = latent_down_weight.shape[1]

    split_rows = depth % (16 * tp_count) == 0
    own_table = jnp.concatenate([latent_down_weight, w_rope_key], axis=1)
    if split_rows:
        piece = depth // tp_count
        own_table = lax.dynamic_slice_in_dim(own_table, ti * piece, piece, 0)
    own_table, w_value, w_gate = lax.optimization_barrier((own_table, w_value, w_gate))
    table_parts = place.outer_gather(own_table)

    width = w_value.shape[1] // outer
    columns = []
    for j in range(outer):
        start = (zi ^ j) * width
        block = jnp.concatenate(
            [
                lax.dynamic_slice_in_dim(w_value, start, width, 1),
                lax.dynamic_slice_in_dim(w_gate, start, width, 1),
            ],
            axis=1,
        )
        columns.append(block if j == 0 else place.outer_swap(block, j))

    table = jnp.stack(table_parts)
    table, tokens = lax.optimization_barrier((table, tokens))
    tables = place.inner_gather(table)

    gathered = lax.all_gather(tokens, "tp", axis=1, tiled=True)
    features = gathered.astype(jnp.float32)
    normed = (
        features
        * lax.rsqrt(jnp.mean(features * features, axis=-1, keepdims=True) + epsilon)
        * norm_gain
    ).astype(jnp.bfloat16)

    own_rows = lax.dynamic_slice_in_dim(normed, ti * share, share, 0)
    rows = place.outer_gather(own_rows)
    weight_block = jnp.stack(columns)
    weight_block, query_rows = lax.optimization_barrier((weight_block, normed))
    weight_blocks = place.inner_gather(weight_block)

    bf16 = jnp.bfloat16
    model = normed.shape[1]
    head_count = key_up_weight.shape[1] // PLAIN_QK_WIDTH
    query_index = lax.axis_index("sp") * row_count + jnp.arange(row_count, dtype=jnp.int32)
    back = zi ^ jnp.arange(outer, dtype=jnp.int32)
    key_index = (
        ((back * inner + xi) * row_count + ti * share)[:, None]
        + jnp.arange(share, dtype=jnp.int32)[None, :]
    ).reshape(-1)
    angles = angles_at(
        jnp.concatenate([query_index, key_index]).astype(jnp.float32), QK_ROPE
    )
    cosine, sine = jnp.cos(angles), jnp.sin(angles)

    query_width = w_query.shape[1]
    queries = pl.pallas_call(
        functools.partial(query_kernel, rank),
        out_shape=jax.ShapeDtypeStruct((head_count, row_count, rank + QK_ROPE), bf16),
        in_specs=[whole_vmem()] + [pl.BlockSpec(memory_space=pltpu.HBM)] * 2 + [whole_vmem()] * 2,
        out_specs=whole_vmem(),
        scratch_shapes=[
            pltpu.VMEM((model, query_width), bf16),
            pltpu.VMEM(key_up_weight.shape, bf16),
            pltpu.SemaphoreType.DMA((head_count // 2 + 1,)),
        ],
        compiler_params=pltpu.CompilerParams(vmem_limit_bytes=52 << 20),
        cost_estimate=pl.CostEstimate(
            flops=2 * row_count * model * query_width,
            bytes_accessed=2 * model * query_width,
            transcendentals=0,
        ),
        name="queries",
    )(query_rows, w_query, key_up_weight, cosine, sine)

    rows, tables, _ = lax.optimization_barrier((rows, tables, queries))
    if split_rows:
        tables = sum(place.tp_gather(tables), [])

    latent = pl.pallas_call(
        functools.partial(latent_kernel, place, rank, split_rows),
        out_shape=jax.ShapeDtypeStruct((outer * share, rank + QK_ROPE), bf16),
        in_specs=[whole_vmem()] * (outer + len(tables) + 3),
        out_specs=whole_vmem(),
        scratch_shapes=[
            pltpu.VMEM((outer * share, model), bf16),
            pltpu.VMEM((model, rank + QK_ROPE), bf16),
        ],
        compiler_params=pltpu.CompilerParams(vmem_limit_bytes=16 << 20),
        cost_estimate=pl.CostEstimate(
            flops=2 * outer * share * model * (rank + QK_ROPE),
            bytes_accessed=2 * model * (rank + QK_ROPE + outer * share),
            transcendentals=0,
        ),
        name="latents",
    )(*rows, *tables, latent_norm_gain[None, :], cosine, sine)
    _, *weight_blocks = lax.optimization_barrier((latent, *weight_blocks))
    latents = place.inner_gather(latent)
    latents = sum(place.tp_gather(latents), [])

    all_rows = sum(place.tp_gather(rows), [])
    gated = pl.pallas_call(
        functools.partial(gated_kernel, place),
        out_shape=[jax.ShapeDtypeStruct((row_count, width), bf16)] * outer,
        in_specs=[whole_vmem()] * (len(all_rows) + inner),
        out_specs=[whole_vmem()] * outer,
        scratch_shapes=[
            pltpu.VMEM((outer * row_count, model), bf16),
            pltpu.VMEM((model, 2 * width), bf16),
        ],
        compiler_params=pltpu.CompilerParams(vmem_limit_bytes=24 << 20),
        cost_estimate=pl.CostEstimate(
            flops=4 * outer * row_count * model * width,
            bytes_accessed=2 * model * (2 * width + outer * row_count),
            transcendentals=outer * row_count * width,
        ),
        name="gated",
    )(*all_rows, *weight_blocks)
    home = [gated[0]] + [place.outer_swap(gated[j], j) for j in range(1, outer)]
    gated_rows = jnp.concatenate(untangled(home, zi), axis=1)

    conv_reach = conv_taps.shape[0] - 1
    prior_rows = lax.ppermute(
        gated_rows[row_count - conv_reach :],
        "sp",
        [(i, i + 1) for i in range(place.sp_count - 1)],
    )
    padded = jnp.concatenate([prior_rows, gated_rows], axis=0).astype(jnp.float32)
    mixed = jnp.zeros(gated_rows.shape, jnp.float32)
    for tap_index in range(conv_taps.shape[0]):
        mixed = (
            mixed
            + conv_taps[tap_index].astype(jnp.float32) * padded[tap_index : tap_index + row_count]
        )
    channel_total = mixed.shape[1] * tp_count
    stats = jnp.stack([jnp.sum(mixed, axis=1), jnp.sum(mixed * mixed, axis=1)])
    stat_sum, stat_squares = sum(
        [place.tp_shift(stats, t) for t in range(1, tp_count)], start=stats
    )
    channel_mean = stat_sum / channel_total
    channel_var = stat_squares / channel_total - channel_mean * channel_mean
    conv_out = jax.nn.silu(
        (mixed - channel_mean[:, None]) * lax.rsqrt(channel_var + epsilon)[:, None] * conv_gain
    ).astype(bf16)

    score_scale = (PLAIN_QK_WIDTH + QK_ROPE) ** (-0.5)
    key_total = place.sp_count * row_count
    out_width = w_merge_conv.shape[1]
    partial, log_sums = pl.pallas_call(
        functools.partial(attention_kernel, place, score_scale, rank),
        out_shape=[
            jax.ShapeDtypeStruct((row_count, out_width), bf16),
            jax.ShapeDtypeStruct((head_count, row_count), jnp.float32),
        ],
        in_specs=[whole_vmem()] * 3
        + [pl.BlockSpec(memory_space=pltpu.HBM)] * 2
        + [whole_vmem()] * len(latents),
        out_specs=[whole_vmem()] * 2,
        scratch_shapes=[
            pltpu.VMEM((key_total, rank + QK_ROPE), bf16),
            pltpu.VMEM((row_count, w_merge_attn.shape[0]), bf16),
            pltpu.VMEM(w_merge_conv.shape, bf16),
            pltpu.VMEM(w_merge_attn.shape, bf16),
            pltpu.SemaphoreType.DMA((2,)),
        ],
        compiler_params=pltpu.CompilerParams(vmem_limit_bytes=52 << 20),
        cost_estimate=pl.CostEstimate(
            flops=2 * row_count * head_count * key_total * (2 * rank + QK_ROPE),
            bytes_accessed=2 * key_total * (rank + QK_ROPE),
            transcendentals=row_count * head_count * key_total,
        ),
        name="attention",
    )(queries, value_up_weight, conv_out, w_merge_conv, w_merge_attn, *latents)

    merged = lax.dynamic_slice_in_dim(partial, ti * share, share, 0).astype(jnp.float32)
    for t in range(1, tp_count):
        away = lax.dynamic_slice_in_dim(partial, lax.rem(ti + t, tp_count) * share, share, 0)
        merged = merged + place.tp_shift(away, t).astype(jnp.float32)
    return (merged.astype(bf16), log_sums.T)


def solution(mesh):
    return jax.shard_map(
        local,
        mesh=mesh,
        in_specs=(
            P("sp", "tp"),
            P(),
            P("sp", "tp"),
            P("sp", "tp"),
            P(None, "tp"),
            P("tp"),
            P(None, "tp"),
            P("sp", None),
            P(),
            P("sp", None),
            P(None, "tp"),
            P(None, "tp"),
            P("tp", None),
            P("tp", None),
        ),
        out_specs=(P(("sp", "tp"), None), P("sp", "tp")),
        check_vma=False,
    )
```

```python
import functools
import math

import jax
import jax.numpy as jnp
from jax import lax
from jax.experimental import pallas as pl
from jax.experimental.pallas import tpu as pltpu
from jax.sharding import PartitionSpec as P


PLAIN_QK_WIDTH = 128
QK_ROPE = 64
VALUE_HEAD_WIDTH = 128


epsilon = 1e-06
rope_base = 10000.0
masked_score = -1e30


def angles_at(positions, width):
    inverse = rope_base ** (-2.0 * jnp.arange(width // 2, dtype=jnp.float32) / width)
    return positions[:, None] * inverse[None, :]


class Place:
    def __init__(self):
        self.sp_count = lax.axis_size("sp")
        self.tp_count = lax.axis_size("tp")
        self.inner = math.gcd(self.sp_count, 4)
        self.outer = self.sp_count // self.inner

    def indices(self):
        index = lax.axis_index("sp")
        return index // self.inner, index % self.inner, lax.axis_index("tp")

    def outer_swap(self, block, mask):
        mask = mask * self.inner
        return lax.ppermute(block, "sp", [(i, i ^ mask) for i in range(self.sp_count)])

    def inner_swap(self, block, mask):
        return lax.ppermute(block, "sp", [(i, i ^ mask) for i in range(self.sp_count)])

    def tp_shift(self, block, distance):
        route = [(i, (i + distance) % self.tp_count) for i in range(self.tp_count)]
        return lax.ppermute(block, "tp", route)

    def outer_gather(self, block):
        return [block] + [self.outer_swap(block, j) for j in range(1, self.outer)]

    def outer_forward(self, block):
        blocks = [block]
        for j in range(1, self.outer):
            near = j & -j
            blocks.append(self.outer_swap(blocks[j ^ near], near))
        return blocks

    def inner_gather(self, block):
        return [block] + [self.inner_swap(block, k) for k in range(1, self.inner)]

    def tp_gather(self, blocks):
        return [blocks] + [
            [self.tp_shift(b, t) for b in blocks] for t in range(1, self.tp_count)
        ]


def behind(index, distance, count):
    return lax.rem(index - distance + count, count)


def untangled(blocks, index):
    bit = 1
    while bit < len(blocks):
        flag = (index & bit) > 0
        blocks = [jnp.where(flag, blocks[i ^ bit], b) for i, b in enumerate(blocks)]
        bit *= 2
    return blocks


def copy_all(pairs, sem):
    copies = [pltpu.make_async_copy(s, d, sem.at[n]) for n, (s, d) in enumerate(pairs)]
    for c in copies:
        c.start()
    return copies


def whole_vmem():
    return pl.BlockSpec(memory_space=pltpu.VMEM)


def turned(first, second, cosine, sine):
    return jnp.concatenate(
        [first * cosine - second * sine, first * sine + second * cosine], axis=-1
    ).astype(jnp.bfloat16)


def query_kernel(rank, normed_ref, w_ref, up_ref, cos_ref, sin_ref, out_ref, w, up, sem):
    heads, count, _ = out_ref.shape
    plain, half = PLAIN_QK_WIDTH, QK_ROPE // 2
    head = plain + QK_ROPE
    span = 2 * head
    pairs = heads // 2
    copies = copy_all(
        [
            (w_ref.at[:, p * span : (p + 1) * span], w.at[:, p * span : (p + 1) * span])
            for p in range(pairs)
        ]
        + [(up_ref, up)],
        sem,
    )
    cosine, sine = cos_ref[:count], sin_ref[:count]
    for p in range(pairs):
        copies[p].wait()
        query = jnp.dot(
            normed_ref[...], w[:, p * span : (p + 1) * span], preferred_element_type=jnp.float32
        ).astype(jnp.bfloat16)
        if p == 0:
            copies[pairs].wait()
        for i in range(2):
            h = 2 * p + i
            own = query[:, i * head : (i + 1) * head]
            out_ref[h, :, :rank] = lax.dot_general(
                own[:, :plain],
                up[:, h * plain : (h + 1) * plain],
                (((1,), (1,)), ((), ())),
                preferred_element_type=jnp.float32,
            ).astype(jnp.bfloat16)
            rope = own[:, plain:].astype(jnp.float32)
            out_ref[h, :, rank:] = turned(rope[:, :half], rope[:, half:], cosine, sine)


def latent_kernel(place, rank, share, *refs):
    outer, inner, tp = place.outer, place.inner, place.tp_count
    tables = tp if share else 1
    n_rows, n_w = outer, tables * inner
    row_refs, w_refs = refs[:n_rows], refs[n_rows : n_rows + n_w]
    gain_ref, cos_ref, sin_ref, out_ref, rows, weight = refs[n_rows + n_w :]
    zi, xi, ti = place.indices()
    piece = w_refs[0].shape[1]
    block = piece * tables
    count = row_refs[0].shape[0]
    for t in range(tables):
        owner = behind(ti, t, tp) if share else 0
        for k in range(inner):
            for j in range(outer):
                start = ((zi ^ j) * inner + (xi ^ k)) * block + owner * piece
                weight[pl.ds(pl.multiple_of(start, piece), piece)] = w_refs[t * inner + k][j]
    for j in range(outer):
        rows[j * count : (j + 1) * count] = row_refs[j][...]
    pre = jnp.dot(rows[...], weight[...], preferred_element_type=jnp.float32)
    plain = pre[:, :rank]
    scale = lax.rsqrt(jnp.mean(plain * plain, axis=-1, keepdims=True) + epsilon)
    out_ref[:, :rank] = (plain * scale * gain_ref[...]).astype(jnp.bfloat16)
    rope = pre[:, rank:]
    half = rope.shape[1] // 2
    total = outer * count
    cosine, sine = cos_ref[cos_ref.shape[0] - total :], sin_ref[sin_ref.shape[0] - total :]
    out_ref[:, rank:] = turned(rope[:, :half], rope[:, half:], cosine, sine)


def gated_kernel(place, *refs):
    outer, inner, tp = place.outer, place.inner, place.tp_count
    n_rows = tp * outer
    row_refs, w_refs = refs[:n_rows], refs[n_rows : n_rows + inner]
    outs = refs[n_rows + inner : n_rows + inner + outer]
    rows, weight = refs[n_rows + inner + outer :]
    zi, xi, ti = place.indices()
    block = w_refs[0].shape[1]
    count = row_refs[0].shape[0]
    for k in range(inner):
        for j in range(outer):
            start = ((zi ^ j) * inner + (xi ^ k)) * block
            weight[pl.ds(pl.multiple_of(start, block), block)] = w_refs[k][j]
    for t in range(tp):
        owner = behind(ti, t, tp)
        for j in range(outer):
            start = j * tp * count + owner * count
            rows[pl.ds(pl.multiple_of(start, count), count)] = row_refs[t * outer + j][...]
    chunk = tp * count
    width = outs[0].shape[1]
    pre = jnp.dot(rows[...], weight[...], preferred_element_type=jnp.float32)
    for j in range(outer):
        part = pre[j * chunk : (j + 1) * chunk]
        value, gate = part[:, :width], part[:, width:]
        outs[j][...] = (value * jax.nn.sigmoid(gate)).astype(jnp.bfloat16)


def attention_kernel(place, scale, rank, q_ref, up_ref, *refs):
    outer, inner, tp = place.outer, place.inner, place.tp_count
    n_k = tp * inner
    key_refs = refs[:n_k]
    out_ref, lse_ref, keys = refs[n_k:]
    zi, xi, ti = place.indices()
    heads, count, depth = q_ref.shape
    piece = key_refs[0].shape[0]
    share = piece // outer
    for n in range(n_k):
        keys[n * piece : (n + 1) * piece] = key_refs[n][...]
    lane = lax.broadcasted_iota(jnp.int32, (1, piece), 1)
    back = zi ^ lax.shift_right_logical(lane, share.bit_length() - 1)
    within = jnp.bitwise_and(lane, share - 1)
    parts = []
    for t in range(tp):
        owner = behind(ti, t, tp)
        for k in range(inner):
            parts.append((back * inner + (xi ^ k)) * count + owner * share + within)
    key_index = jnp.concatenate(parts, axis=1)
    first_row = (zi * inner + xi) * count
    together = math.gcd(heads, 4)
    size = together * count
    query_index = lax.broadcasted_iota(jnp.int32, (count, 1), 0) + first_row
    allowed = key_index <= jnp.concatenate([query_index] * together, axis=0)
    width = VALUE_HEAD_WIDTH
    sums = []
    for g in range(heads // together):
        queries = q_ref[g * together : (g + 1) * together].reshape(size, depth)
        scores = lax.dot_general(
            queries, keys[...], (((1,), (1,)), ((), ())), preferred_element_type=jnp.float32
        )
        scores = jnp.where(allowed, scores, masked_score)
        top = jnp.max(scores, axis=-1, keepdims=True)
        weights = jnp.exp2((scores - top) * (scale * math.log2(math.e)))
        total = jnp.sum(weights, axis=-1, keepdims=True)
        weighted = jnp.dot(
            weights.astype(jnp.bfloat16), keys[:, :rank], preferred_element_type=jnp.float32
        )
        latent_out = (weighted / total).astype(jnp.bfloat16)
        group_sums = top * scale + jnp.log(total)
        for i in range(together):
            h = g * together + i
            part = slice(i * count, (i + 1) * count)
            sums.append(group_sums[part])
            out_ref[:, h * width : (h + 1) * width] = jnp.dot(
                latent_out[part],
                up_ref[:, h * width : (h + 1) * width],
                preferred_element_type=jnp.float32,
            ).astype(jnp.bfloat16)
    spare = [jnp.zeros((count, 128 - heads), jnp.float32)]
    lse_ref[...] = jnp.concatenate(sums + spare, axis=1).T[:heads]


def local(
    tokens,
    norm_gain,
    w_value,
    w_gate,
    conv_taps,
    conv_gain,
    w_query,
    latent_down_weight,
    latent_norm_gain,
    w_rope_key,
    key_up_weight,
    value_up_weight,
    w_merge_conv,
    w_merge_attn,
):
    place = Place()
    outer, inner, tp_count = place.outer, place.inner, place.tp_count
    zi, xi, ti = place.indices()
    row_count = tokens.shape[0]
    share = row_count // tp_count
    depth = latent_down_weight.shape[0]
    rank = latent_down_weight.shape[1]

    width = w_value.shape[1] // outer
    columns = []
    for j in range(outer):
        start = (zi ^ j) * width
        block = jnp.concatenate(
            [
                lax.dynamic_slice_in_dim(w_value, start, width, 1),
                lax.dynamic_slice_in_dim(w_gate, start, width, 1),
            ],
            axis=1,
        )
        columns.append(block if j == 0 else place.outer_swap(block, j))

    split_rows = depth % (16 * tp_count) == 0
    own_table = jnp.concatenate([latent_down_weight, w_rope_key], axis=1)
    if split_rows:
        piece = depth // tp_count
        own_table = lax.dynamic_slice_in_dim(own_table, ti * piece, piece, 0)
    table_parts = place.outer_gather(own_table)

    weight_blocks = place.inner_gather(jnp.stack(columns))
    tables = place.inner_gather(jnp.stack(table_parts))

    gathered = lax.all_gather(tokens, "tp", axis=1, tiled=True)
    features = gathered.astype(jnp.float32)
    normed = (
        features
        * lax.rsqrt(jnp.mean(features * features, axis=-1, keepdims=True) + epsilon)
        * norm_gain
    ).astype(jnp.bfloat16)

    own_rows = lax.dynamic_slice_in_dim(normed, ti * share, share, 0)
    rows = place.outer_forward(own_rows)

    bf16 = jnp.bfloat16
    model = normed.shape[1]
    head_count = key_up_weight.shape[1] // PLAIN_QK_WIDTH
    query_index = lax.axis_index("sp") * row_count + jnp.arange(row_count, dtype=jnp.int32)
    back = zi ^ jnp.arange(outer, dtype=jnp.int32)
    key_index = (
        ((back * inner + xi) * row_count + ti * share)[:, None]
        + jnp.arange(share, dtype=jnp.int32)[None, :]
    ).reshape(-1)
    angles = angles_at(
        jnp.concatenate([query_index, key_index]).astype(jnp.float32), QK_ROPE
    )
    cosine, sine = jnp.cos(angles), jnp.sin(angles)

    query_width = w_query.shape[1]
    queries = pl.pallas_call(
        functools.partial(query_kernel, rank),
        out_shape=jax.ShapeDtypeStruct((head_count, row_count, rank + QK_ROPE), bf16),
        in_specs=[whole_vmem()] + [pl.BlockSpec(memory_space=pltpu.HBM)] * 2 + [whole_vmem()] * 2,
        out_specs=whole_vmem(),
        scratch_shapes=[
            pltpu.VMEM((model, query_width), bf16),
            pltpu.VMEM(key_up_weight.shape, bf16),
            pltpu.SemaphoreType.DMA((head_count // 2 + 1,)),
        ],
        compiler_params=pltpu.CompilerParams(vmem_limit_bytes=52 << 20),
        cost_estimate=pl.CostEstimate(
            flops=2 * row_count * model * query_width,
            bytes_accessed=2 * model * query_width,
            transcendentals=0,
        ),
        name="queries",
    )(normed, w_query, key_up_weight, cosine, sine)

    rows, _ = lax.optimization_barrier((rows, queries))
    all_rows = sum(place.tp_gather(rows), [])
    gated = pl.pallas_call(
        functools.partial(gated_kernel, place),
        out_shape=[jax.ShapeDtypeStruct((row_count, width), bf16)] * outer,
        in_specs=[whole_vmem()] * (len(all_rows) + inner),
        out_specs=[whole_vmem()] * outer,
        scratch_shapes=[
            pltpu.VMEM((outer * row_count, model), bf16),
            pltpu.VMEM((model, 2 * width), bf16),
        ],
        compiler_params=pltpu.CompilerParams(vmem_limit_bytes=24 << 20),
        cost_estimate=pl.CostEstimate(
            flops=4 * outer * row_count * model * width,
            bytes_accessed=2 * model * (2 * width + outer * row_count),
            transcendentals=outer * row_count * width,
        ),
        name="gated",
    )(*all_rows, *weight_blocks)
    home = [gated[0]] + [place.outer_swap(gated[j], j) for j in range(1, outer)]
    if split_rows:
        tables = sum(place.tp_gather(tables), [])

    latent = pl.pallas_call(
        functools.partial(latent_kernel, place, rank, split_rows),
        out_shape=jax.ShapeDtypeStruct((outer * share, rank + QK_ROPE), bf16),
        in_specs=[whole_vmem()] * (outer + len(tables) + 3),
        out_specs=whole_vmem(),
        scratch_shapes=[
            pltpu.VMEM((outer * share, model), bf16),
            pltpu.VMEM((model, rank + QK_ROPE), bf16),
        ],
        compiler_params=pltpu.CompilerParams(vmem_limit_bytes=16 << 20),
        cost_estimate=pl.CostEstimate(
            flops=2 * outer * share * model * (rank + QK_ROPE),
            bytes_accessed=2 * model * (rank + QK_ROPE + outer * share),
            transcendentals=0,
        ),
        name="latents",
    )(*rows, *tables, latent_norm_gain[None, :], cosine, sine)
    latents = place.inner_gather(latent)
    home, _ = lax.optimization_barrier((home, latent))
    gated_rows = jnp.concatenate(untangled(home, zi), axis=1)
    conv_reach = conv_taps.shape[0] - 1
    prior_rows = lax.ppermute(
        gated_rows[row_count - conv_reach :],
        "sp",
        [(i, i + 1) for i in range(place.sp_count - 1)],
    )
    padded = jnp.concatenate([prior_rows, gated_rows], axis=0).astype(jnp.float32)
    mixed = jnp.zeros(gated_rows.shape, jnp.float32)
    for tap_index in range(conv_taps.shape[0]):
        mixed = (
            mixed
            + conv_taps[tap_index].astype(jnp.float32) * padded[tap_index : tap_index + row_count]
        )
    channel_total = mixed.shape[1] * tp_count
    stats = jnp.stack([jnp.sum(mixed, axis=1), jnp.sum(mixed * mixed, axis=1)])
    stat_sum, stat_squares = sum(
        [place.tp_shift(stats, t) for t in range(1, tp_count)], start=stats
    )
    channel_mean = stat_sum / channel_total
    channel_var = stat_squares / channel_total - channel_mean * channel_mean
    conv_out = jax.nn.silu(
        (mixed - channel_mean[:, None]) * lax.rsqrt(channel_var + epsilon)[:, None] * conv_gain
    ).astype(bf16)

    conv_part = jnp.dot(conv_out, w_merge_conv, preferred_element_type=jnp.float32)
    latents, queries, _ = lax.optimization_barrier((latents, queries, conv_part))
    latents = sum(place.tp_gather(latents), [])

    score_scale = (PLAIN_QK_WIDTH + QK_ROPE) ** (-0.5)
    key_total = place.sp_count * row_count
    attention, log_sums = pl.pallas_call(
        functools.partial(attention_kernel, place, score_scale, rank),
        out_shape=[
            jax.ShapeDtypeStruct((row_count, head_count * VALUE_HEAD_WIDTH), bf16),
            jax.ShapeDtypeStruct((head_count, row_count), jnp.float32),
        ],
        in_specs=[whole_vmem()] * (2 + len(latents)),
        out_specs=[whole_vmem()] * 2,
        scratch_shapes=[
            pltpu.VMEM((key_total, rank + QK_ROPE), bf16),
        ],
        compiler_params=pltpu.CompilerParams(vmem_limit_bytes=32 << 20),
        cost_estimate=pl.CostEstimate(
            flops=2 * row_count * head_count * key_total * (2 * rank + QK_ROPE),
            bytes_accessed=2 * key_total * (rank + QK_ROPE),
            transcendentals=row_count * head_count * key_total,
        ),
        name="attention",
    )(queries, value_up_weight, *latents)

    partial = (
        conv_part + jnp.dot(attention, w_merge_attn, preferred_element_type=jnp.float32)
    ).astype(bf16)
    merged = lax.dynamic_slice_in_dim(partial, ti * share, share, 0).astype(jnp.float32)
    for t in range(1, tp_count):
        away = lax.dynamic_slice_in_dim(partial, lax.rem(ti + t, tp_count) * share, share, 0)
        merged = merged + place.tp_shift(away, t).astype(jnp.float32)
    return (merged.astype(bf16), log_sums.T)


def solution(mesh):
    return jax.shard_map(
        local,
        mesh=mesh,
        in_specs=(
            P("sp", "tp"),
            P(),
            P("sp", "tp"),
            P("sp", "tp"),
            P(None, "tp"),
            P("tp"),
            P(None, "tp"),
            P("sp", None),
            P(),
            P("sp", None),
            P(None, "tp"),
            P(None, "tp"),
            P("tp", None),
            P("tp", None),
        ),
        out_specs=(P(("sp", "tp"), None), P("sp", "tp")),
        check_vma=False,
    )
```

```python
import functools
import math

import jax
import jax.numpy as jnp
from jax import lax
from jax.experimental import pallas as pl
from jax.experimental.pallas import tpu as pltpu
from jax.sharding import PartitionSpec as P


PLAIN_QK_WIDTH = 128
QK_ROPE = 64
VALUE_HEAD_WIDTH = 128


epsilon = 1e-06
rope_base = 10000.0
masked_score = -1e30


def angles_at(positions, width):
    inverse = rope_base ** (-2.0 * jnp.arange(width // 2, dtype=jnp.float32) / width)
    return positions[:, None] * inverse[None, :]


class Place:
    def __init__(self):
        self.sp_count = lax.axis_size("sp")
        self.tp_count = lax.axis_size("tp")
        self.inner = math.gcd(self.sp_count, 4)
        self.outer = self.sp_count // self.inner

    def indices(self):
        index = lax.axis_index("sp")
        return index // self.inner, index % self.inner, lax.axis_index("tp")

    def outer_swap(self, block, mask):
        mask = mask * self.inner
        return lax.ppermute(block, "sp", [(i, i ^ mask) for i in range(self.sp_count)])

    def inner_swap(self, block, mask):
        return lax.ppermute(block, "sp", [(i, i ^ mask) for i in range(self.sp_count)])

    def tp_shift(self, block, distance):
        route = [(i, (i + distance) % self.tp_count) for i in range(self.tp_count)]
        return lax.ppermute(block, "tp", route)

    def outer_gather(self, block):
        return [block] + [self.outer_swap(block, j) for j in range(1, self.outer)]

    def outer_forward(self, block):
        blocks = [block]
        for j in range(1, self.outer):
            near = j & -j
            blocks.append(self.outer_swap(blocks[j ^ near], near))
        return blocks

    def inner_gather(self, block):
        return [block] + [self.inner_swap(block, k) for k in range(1, self.inner)]

    def tp_gather(self, blocks):
        return [blocks] + [
            [self.tp_shift(b, t) for b in blocks] for t in range(1, self.tp_count)
        ]


def behind(index, distance, count):
    return lax.rem(index - distance + count, count)


def untangled(blocks, index):
    bit = 1
    while bit < len(blocks):
        flag = (index & bit) > 0
        blocks = [jnp.where(flag, blocks[i ^ bit], b) for i, b in enumerate(blocks)]
        bit *= 2
    return blocks


def copy_all(pairs, sem):
    copies = [pltpu.make_async_copy(s, d, sem.at[n]) for n, (s, d) in enumerate(pairs)]
    for c in copies:
        c.start()
    return copies


def whole_vmem():
    return pl.BlockSpec(memory_space=pltpu.VMEM)


def turned(first, second, cosine, sine):
    return jnp.concatenate(
        [first * cosine - second * sine, first * sine + second * cosine], axis=-1
    ).astype(jnp.bfloat16)


def query_kernel(rank, normed_ref, w_ref, up_ref, cos_ref, sin_ref, out_ref, w, up, sem):
    heads, count, _ = out_ref.shape
    plain, half = PLAIN_QK_WIDTH, QK_ROPE // 2
    head = plain + QK_ROPE
    span = 2 * head
    pairs = heads // 2
    copies = copy_all(
        [
            (w_ref.at[:, p * span : (p + 1) * span], w.at[:, p * span : (p + 1) * span])
            for p in range(pairs)
        ]
        + [(up_ref, up)],
        sem,
    )
    cosine, sine = cos_ref[:count], sin_ref[:count]
    for p in range(pairs):
        copies[p].wait()
        query = jnp.dot(
            normed_ref[...], w[:, p * span : (p + 1) * span], preferred_element_type=jnp.float32
        ).astype(jnp.bfloat16)
        if p == 0:
            copies[pairs].wait()
        for i in range(2):
            h = 2 * p + i
            own = query[:, i * head : (i + 1) * head]
            out_ref[h, :, :rank] = lax.dot_general(
                own[:, :plain],
                up[:, h * plain : (h + 1) * plain],
                (((1,), (1,)), ((), ())),
                preferred_element_type=jnp.float32,
            ).astype(jnp.bfloat16)
            rope = own[:, plain:].astype(jnp.float32)
            out_ref[h, :, rank:] = turned(rope[:, :half], rope[:, half:], cosine, sine)


def latent_kernel(place, rank, share, *refs):
    outer, inner, tp = place.outer, place.inner, place.tp_count
    tables = tp if share else 1
    n_rows, n_w = outer, tables * inner
    row_refs, w_refs = refs[:n_rows], refs[n_rows : n_rows + n_w]
    gain_ref, cos_ref, sin_ref, out_ref, rows, weight = refs[n_rows + n_w :]
    zi, xi, ti = place.indices()
    piece = w_refs[0].shape[1]
    block = piece * tables
    count = row_refs[0].shape[0]
    for t in range(tables):
        owner = behind(ti, t, tp) if share else 0
        for k in range(inner):
            for j in range(outer):
                start = ((zi ^ j) * inner + (xi ^ k)) * block + owner * piece
                weight[pl.ds(pl.multiple_of(start, piece), piece)] = w_refs[t * inner + k][j]
    for j in range(outer):
        rows[j * count : (j + 1) * count] = row_refs[j][...]
    pre = jnp.dot(rows[...], weight[...], preferred_element_type=jnp.float32)
    plain = pre[:, :rank]
    scale = lax.rsqrt(jnp.mean(plain * plain, axis=-1, keepdims=True) + epsilon)
    out_ref[:, :rank] = (plain * scale * gain_ref[...]).astype(jnp.bfloat16)
    rope = pre[:, rank:]
    half = rope.shape[1] // 2
    total = outer * count
    cosine, sine = cos_ref[cos_ref.shape[0] - total :], sin_ref[sin_ref.shape[0] - total :]
    out_ref[:, rank:] = turned(rope[:, :half], rope[:, half:], cosine, sine)


def gated_kernel(place, *refs):
    outer, inner, tp = place.outer, place.inner, place.tp_count
    n_rows = tp * outer
    row_refs, w_refs = refs[:n_rows], refs[n_rows : n_rows + inner]
    outs = refs[n_rows + inner : n_rows + inner + outer]
    rows, weight = refs[n_rows + inner + outer :]
    zi, xi, ti = place.indices()
    block = w_refs[0].shape[1]
    count = row_refs[0].shape[0]
    for k in range(inner):
        for j in range(outer):
            start = ((zi ^ j) * inner + (xi ^ k)) * block
            weight[pl.ds(pl.multiple_of(start, block), block)] = w_refs[k][j]
    for t in range(tp):
        owner = behind(ti, t, tp)
        for j in range(outer):
            start = j * tp * count + owner * count
            rows[pl.ds(pl.multiple_of(start, count), count)] = row_refs[t * outer + j][...]
    chunk = tp * count
    width = outs[0].shape[1]
    pre = jnp.dot(rows[...], weight[...], preferred_element_type=jnp.float32)
    for j in range(outer):
        part = pre[j * chunk : (j + 1) * chunk]
        value, gate = part[:, :width], part[:, width:]
        outs[j][...] = (value * jax.nn.sigmoid(gate)).astype(jnp.bfloat16)


def attention_kernel(place, scale, rank, q_ref, up_ref, *refs):
    outer, inner, tp = place.outer, place.inner, place.tp_count
    n_k = tp * inner
    key_refs = refs[:n_k]
    out_ref, lse_ref, keys = refs[n_k:]
    zi, xi, ti = place.indices()
    heads, count, depth = q_ref.shape
    piece = key_refs[0].shape[0]
    share = piece // outer
    for n in range(n_k):
        keys[n * piece : (n + 1) * piece] = key_refs[n][...]
    lane = lax.broadcasted_iota(jnp.int32, (1, piece), 1)
    back = zi ^ lax.shift_right_logical(lane, share.bit_length() - 1)
    within = jnp.bitwise_and(lane, share - 1)
    parts = []
    for t in range(tp):
        owner = behind(ti, t, tp)
        for k in range(inner):
            parts.append((back * inner + (xi ^ k)) * count + owner * share + within)
    key_index = jnp.concatenate(parts, axis=1)
    first_row = (zi * inner + xi) * count
    together = math.gcd(heads, 4)
    size = together * count
    query_index = lax.broadcasted_iota(jnp.int32, (count, 1), 0) + first_row
    allowed = key_index <= jnp.concatenate([query_index] * together, axis=0)
    width = VALUE_HEAD_WIDTH
    sums = []
    for g in range(heads // together):
        queries = q_ref[g * together : (g + 1) * together].reshape(size, depth)
        scores = lax.dot_general(
            queries, keys[...], (((1,), (1,)), ((), ())), preferred_element_type=jnp.float32
        )
        scores = jnp.where(allowed, scores, masked_score)
        top = jnp.max(scores, axis=-1, keepdims=True)
        weights = jnp.exp2((scores - top) * (scale * math.log2(math.e)))
        total = jnp.sum(weights, axis=-1, keepdims=True)
        weighted = jnp.dot(
            weights.astype(jnp.bfloat16), keys[:, :rank], preferred_element_type=jnp.float32
        )
        latent_out = (weighted / total).astype(jnp.bfloat16)
        group_sums = top * scale + jnp.log(total)
        for i in range(together):
            h = g * together + i
            part = slice(i * count, (i + 1) * count)
            sums.append(group_sums[part])
            out_ref[:, h * width : (h + 1) * width] = jnp.dot(
                latent_out[part],
                up_ref[:, h * width : (h + 1) * width],
                preferred_element_type=jnp.float32,
            ).astype(jnp.bfloat16)
    spare = [jnp.zeros((count, 128 - heads), jnp.float32)]
    lse_ref[...] = jnp.concatenate(sums + spare, axis=1).T[:heads]


def local(
    tokens,
    norm_gain,
    w_value,
    w_gate,
    conv_taps,
    conv_gain,
    w_query,
    latent_down_weight,
    latent_norm_gain,
    w_rope_key,
    key_up_weight,
    value_up_weight,
    w_merge_conv,
    w_merge_attn,
):
    place = Place()
    outer, inner, tp_count = place.outer, place.inner, place.tp_count
    zi, xi, ti = place.indices()
    row_count = tokens.shape[0]
    share = row_count // tp_count
    depth = latent_down_weight.shape[0]
    rank = latent_down_weight.shape[1]

    split_rows = depth % (16 * tp_count) == 0
    own_table = jnp.concatenate([latent_down_weight, w_rope_key], axis=1)
    if split_rows:
        piece = depth // tp_count
        own_table = lax.dynamic_slice_in_dim(own_table, ti * piece, piece, 0)
    own_table, w_value, w_gate = lax.optimization_barrier((own_table, w_value, w_gate))
    table_parts = place.outer_gather(own_table)

    width = w_value.shape[1] // outer
    columns = []
    for j in range(outer):
        start = (zi ^ j) * width
        block = jnp.concatenate(
            [
                lax.dynamic_slice_in_dim(w_value, start, width, 1),
                lax.dynamic_slice_in_dim(w_gate, start, width, 1),
            ],
            axis=1,
        )
        columns.append(block if j == 0 else place.outer_swap(block, j))

    table = jnp.stack(table_parts)
    table, tokens = lax.optimization_barrier((table, tokens))
    tables = place.inner_gather(table)

    gathered = lax.all_gather(tokens, "tp", axis=1, tiled=True)
    features = gathered.astype(jnp.float32)
    normed = (
        features
        * lax.rsqrt(jnp.mean(features * features, axis=-1, keepdims=True) + epsilon)
        * norm_gain
    ).astype(jnp.bfloat16)

    own_rows = lax.dynamic_slice_in_dim(normed, ti * share, share, 0)
    rows = place.outer_forward(own_rows)
    weight_block = jnp.stack(columns)
    weight_block, query_rows = lax.optimization_barrier((weight_block, normed))
    weight_blocks = place.inner_gather(weight_block)

    bf16 = jnp.bfloat16
    model = normed.shape[1]
    head_count = key_up_weight.shape[1] // PLAIN_QK_WIDTH
    query_index = lax.axis_index("sp") * row_count + jnp.arange(row_count, dtype=jnp.int32)
    back = zi ^ jnp.arange(outer, dtype=jnp.int32)
    key_index = (
        ((back * inner + xi) * row_count + ti * share)[:, None]
        + jnp.arange(share, dtype=jnp.int32)[None, :]
    ).reshape(-1)
    angles = angles_at(
        jnp.concatenate([query_index, key_index]).astype(jnp.float32), QK_ROPE
    )
    cosine, sine = jnp.cos(angles), jnp.sin(angles)

    query_width = w_query.shape[1]
    queries = pl.pallas_call(
        functools.partial(query_kernel, rank),
        out_shape=jax.ShapeDtypeStruct((head_count, row_count, rank + QK_ROPE), bf16),
        in_specs=[whole_vmem()] + [pl.BlockSpec(memory_space=pltpu.HBM)] * 2 + [whole_vmem()] * 2,
        out_specs=whole_vmem(),
        scratch_shapes=[
            pltpu.VMEM((model, query_width), bf16),
            pltpu.VMEM(key_up_weight.shape, bf16),
            pltpu.SemaphoreType.DMA((head_count // 2 + 1,)),
        ],
        compiler_params=pltpu.CompilerParams(vmem_limit_bytes=52 << 20),
        cost_estimate=pl.CostEstimate(
            flops=2 * row_count * model * query_width,
            bytes_accessed=2 * model * query_width,
            transcendentals=0,
        ),
        name="queries",
    )(query_rows, w_query, key_up_weight, cosine, sine)

    rows, tables, _ = lax.optimization_barrier((rows, tables, queries))
    if split_rows:
        tables = sum(place.tp_gather(tables), [])

    latent = pl.pallas_call(
        functools.partial(latent_kernel, place, rank, split_rows),
        out_shape=jax.ShapeDtypeStruct((outer * share, rank + QK_ROPE), bf16),
        in_specs=[whole_vmem()] * (outer + len(tables) + 3),
        out_specs=whole_vmem(),
        scratch_shapes=[
            pltpu.VMEM((outer * share, model), bf16),
            pltpu.VMEM((model, rank + QK_ROPE), bf16),
        ],
        compiler_params=pltpu.CompilerParams(vmem_limit_bytes=16 << 20),
        cost_estimate=pl.CostEstimate(
            flops=2 * outer * share * model * (rank + QK_ROPE),
            bytes_accessed=2 * model * (rank + QK_ROPE + outer * share),
            transcendentals=0,
        ),
        name="latents",
    )(*rows, *tables, latent_norm_gain[None, :], cosine, sine)
    _, *weight_blocks = lax.optimization_barrier((latent, *weight_blocks))
    latents = place.inner_gather(latent)
    latents = sum(place.tp_gather(latents), [])

    all_rows = sum(place.tp_gather(rows), [])
    gated = pl.pallas_call(
        functools.partial(gated_kernel, place),
        out_shape=[jax.ShapeDtypeStruct((row_count, width), bf16)] * outer,
        in_specs=[whole_vmem()] * (len(all_rows) + inner),
        out_specs=[whole_vmem()] * outer,
        scratch_shapes=[
            pltpu.VMEM((outer * row_count, model), bf16),
            pltpu.VMEM((model, 2 * width), bf16),
        ],
        compiler_params=pltpu.CompilerParams(vmem_limit_bytes=24 << 20),
        cost_estimate=pl.CostEstimate(
            flops=4 * outer * row_count * model * width,
            bytes_accessed=2 * model * (2 * width + outer * row_count),
            transcendentals=outer * row_count * width,
        ),
        name="gated",
    )(*all_rows, *weight_blocks)
    home = [gated[0]] + [place.outer_swap(gated[j], j) for j in range(1, outer)]
    gated_rows = jnp.concatenate(untangled(home, zi), axis=1)

    conv_reach = conv_taps.shape[0] - 1
    prior_rows = lax.ppermute(
        gated_rows[row_count - conv_reach :],
        "sp",
        [(i, i + 1) for i in range(place.sp_count - 1)],
    )
    score_scale = (PLAIN_QK_WIDTH + QK_ROPE) ** (-0.5)
    key_total = place.sp_count * row_count
    attention, log_sums = pl.pallas_call(
        functools.partial(attention_kernel, place, score_scale, rank),
        out_shape=[
            jax.ShapeDtypeStruct((row_count, head_count * VALUE_HEAD_WIDTH), bf16),
            jax.ShapeDtypeStruct((head_count, row_count), jnp.float32),
        ],
        in_specs=[whole_vmem()] * (2 + len(latents)),
        out_specs=[whole_vmem()] * 2,
        scratch_shapes=[
            pltpu.VMEM((key_total, rank + QK_ROPE), bf16),
        ],
        compiler_params=pltpu.CompilerParams(vmem_limit_bytes=32 << 20),
        cost_estimate=pl.CostEstimate(
            flops=2 * row_count * head_count * key_total * (2 * rank + QK_ROPE),
            bytes_accessed=2 * key_total * (rank + QK_ROPE),
            transcendentals=row_count * head_count * key_total,
        ),
        name="attention",
    )(queries, value_up_weight, *latents)

    attn_part = jnp.dot(attention, w_merge_attn, preferred_element_type=jnp.float32)
    prior_rows, gated_rows, _ = lax.optimization_barrier((prior_rows, gated_rows, attn_part))
    padded = jnp.concatenate([prior_rows, gated_rows], axis=0).astype(jnp.float32)
    mixed = jnp.zeros(gated_rows.shape, jnp.float32)
    for tap_index in range(conv_taps.shape[0]):
        mixed = (
            mixed
            + conv_taps[tap_index].astype(jnp.float32) * padded[tap_index : tap_index + row_count]
        )
    channel_total = mixed.shape[1] * tp_count
    stats = jnp.stack([jnp.sum(mixed, axis=1), jnp.sum(mixed * mixed, axis=1)])
    stat_sum, stat_squares = sum(
        [place.tp_shift(stats, t) for t in range(1, tp_count)], start=stats
    )
    channel_mean = stat_sum / channel_total
    channel_var = stat_squares / channel_total - channel_mean * channel_mean
    conv_out = jax.nn.silu(
        (mixed - channel_mean[:, None]) * lax.rsqrt(channel_var + epsilon)[:, None] * conv_gain
    ).astype(bf16)

    partial = (
        attn_part + jnp.dot(conv_out, w_merge_conv, preferred_element_type=jnp.float32)
    ).astype(bf16)
    merged = lax.dynamic_slice_in_dim(partial, ti * share, share, 0).astype(jnp.float32)
    for t in range(1, tp_count):
        away = lax.dynamic_slice_in_dim(partial, lax.rem(ti + t, tp_count) * share, share, 0)
        merged = merged + place.tp_shift(away, t).astype(jnp.float32)
    return (merged.astype(bf16), log_sums.T)


def solution(mesh):
    return jax.shard_map(
        local,
        mesh=mesh,
        in_specs=(
            P("sp", "tp"),
            P(),
            P("sp", "tp"),
            P("sp", "tp"),
            P(None, "tp"),
            P("tp"),
            P(None, "tp"),
            P("sp", None),
            P(),
            P("sp", None),
            P(None, "tp"),
            P(None, "tp"),
            P("tp", None),
            P("tp", None),
        ),
        out_specs=(P(("sp", "tp"), None), P("sp", "tp")),
        check_vma=False,
    )
```

```python
import functools
import math

import jax
import jax.numpy as jnp
from jax import lax
from jax.experimental import pallas as pl
from jax.experimental.pallas import tpu as pltpu
from jax.sharding import PartitionSpec as P


PLAIN_QK_WIDTH = 128
QK_ROPE = 64
VALUE_HEAD_WIDTH = 128


epsilon = 1e-06
rope_base = 10000.0
masked_score = -1e30


def angles_at(positions, width):
    inverse = rope_base ** (-2.0 * jnp.arange(width // 2, dtype=jnp.float32) / width)
    return positions[:, None] * inverse[None, :]


class Place:
    def __init__(self):
        self.sp_count = lax.axis_size("sp")
        self.tp_count = lax.axis_size("tp")
        self.inner = math.gcd(self.sp_count, 4)
        self.outer = self.sp_count // self.inner

    def indices(self):
        index = lax.axis_index("sp")
        return index // self.inner, index % self.inner, lax.axis_index("tp")

    def outer_swap(self, block, mask):
        mask = mask * self.inner
        return lax.ppermute(block, "sp", [(i, i ^ mask) for i in range(self.sp_count)])

    def inner_swap(self, block, mask):
        return lax.ppermute(block, "sp", [(i, i ^ mask) for i in range(self.sp_count)])

    def tp_shift(self, block, distance):
        route = [(i, (i + distance) % self.tp_count) for i in range(self.tp_count)]
        return lax.ppermute(block, "tp", route)

    def outer_gather(self, block):
        return [block] + [self.outer_swap(block, j) for j in range(1, self.outer)]

    def outer_forward(self, block):
        blocks = [block]
        for j in range(1, self.outer):
            near = j & -j
            blocks.append(self.outer_swap(blocks[j ^ near], near))
        return blocks

    def inner_gather(self, block):
        return [block] + [self.inner_swap(block, k) for k in range(1, self.inner)]

    def tp_gather(self, blocks):
        return [blocks] + [
            [self.tp_shift(b, t) for b in blocks] for t in range(1, self.tp_count)
        ]


def behind(index, distance, count):
    return lax.rem(index - distance + count, count)


def untangled(blocks, index):
    bit = 1
    while bit < len(blocks):
        flag = (index & bit) > 0
        blocks = [jnp.where(flag, blocks[i ^ bit], b) for i, b in enumerate(blocks)]
        bit *= 2
    return blocks


def copy_all(pairs, sem):
    copies = [pltpu.make_async_copy(s, d, sem.at[n]) for n, (s, d) in enumerate(pairs)]
    for c in copies:
        c.start()
    return copies


def whole_vmem():
    return pl.BlockSpec(memory_space=pltpu.VMEM)


def turned(first, second, cosine, sine):
    return jnp.concatenate(
        [first * cosine - second * sine, first * sine + second * cosine], axis=-1
    ).astype(jnp.bfloat16)


def query_kernel(rank, normed_ref, w_ref, up_ref, cos_ref, sin_ref, out_ref, w, up, sem):
    heads, count, _ = out_ref.shape
    plain, half = PLAIN_QK_WIDTH, QK_ROPE // 2
    head = plain + QK_ROPE
    span = 2 * head
    pairs = heads // 2
    copies = copy_all(
        [
            (w_ref.at[:, p * span : (p + 1) * span], w.at[:, p * span : (p + 1) * span])
            for p in range(pairs)
        ]
        + [(up_ref, up)],
        sem,
    )
    cosine, sine = cos_ref[:count], sin_ref[:count]
    for p in range(pairs):
        copies[p].wait()
        query = jnp.dot(
            normed_ref[...], w[:, p * span : (p + 1) * span], preferred_element_type=jnp.float32
        ).astype(jnp.bfloat16)
        if p == 0:
            copies[pairs].wait()
        for i in range(2):
            h = 2 * p + i
            own = query[:, i * head : (i + 1) * head]
            out_ref[h, :, :rank] = lax.dot_general(
                own[:, :plain],
                up[:, h * plain : (h + 1) * plain],
                (((1,), (1,)), ((), ())),
                preferred_element_type=jnp.float32,
            ).astype(jnp.bfloat16)
            rope = own[:, plain:].astype(jnp.float32)
            out_ref[h, :, rank:] = turned(rope[:, :half], rope[:, half:], cosine, sine)


def latent_kernel(place, rank, share, *refs):
    outer, inner, tp = place.outer, place.inner, place.tp_count
    tables = tp if share else 1
    n_rows, n_w = outer, tables * inner
    row_refs, w_refs = refs[:n_rows], refs[n_rows : n_rows + n_w]
    gain_ref, cos_ref, sin_ref, out_ref, rows, weight = refs[n_rows + n_w :]
    zi, xi, ti = place.indices()
    piece = w_refs[0].shape[1]
    block = piece * tables
    count = row_refs[0].shape[0]
    for t in range(tables):
        owner = behind(ti, t, tp) if share else 0
        for k in range(inner):
            for j in range(outer):
                start = ((zi ^ j) * inner + (xi ^ k)) * block + owner * piece
                weight[pl.ds(pl.multiple_of(start, piece), piece)] = w_refs[t * inner + k][j]
    for j in range(outer):
        rows[j * count : (j + 1) * count] = row_refs[j][...]
    pre = jnp.dot(rows[...], weight[...], preferred_element_type=jnp.float32)
    plain = pre[:, :rank]
    scale = lax.rsqrt(jnp.mean(plain * plain, axis=-1, keepdims=True) + epsilon)
    out_ref[:, :rank] = (plain * scale * gain_ref[...]).astype(jnp.bfloat16)
    rope = pre[:, rank:]
    half = rope.shape[1] // 2
    total = outer * count
    cosine, sine = cos_ref[cos_ref.shape[0] - total :], sin_ref[sin_ref.shape[0] - total :]
    out_ref[:, rank:] = turned(rope[:, :half], rope[:, half:], cosine, sine)


def gated_kernel(place, *refs):
    outer, inner, tp = place.outer, place.inner, place.tp_count
    n_rows = tp * outer
    row_refs, w_refs = refs[:n_rows], refs[n_rows : n_rows + inner]
    outs = refs[n_rows + inner : n_rows + inner + outer]
    rows, weight = refs[n_rows + inner + outer :]
    zi, xi, ti = place.indices()
    block = w_refs[0].shape[1]
    count = row_refs[0].shape[0]
    for k in range(inner):
        for j in range(outer):
            start = ((zi ^ j) * inner + (xi ^ k)) * block
            weight[pl.ds(pl.multiple_of(start, block), block)] = w_refs[k][j]
    for t in range(tp):
        owner = behind(ti, t, tp)
        for j in range(outer):
            start = j * tp * count + owner * count
            rows[pl.ds(pl.multiple_of(start, count), count)] = row_refs[t * outer + j][...]
    chunk = tp * count
    width = outs[0].shape[1]
    pre = jnp.dot(rows[...], weight[...], preferred_element_type=jnp.float32)
    for j in range(outer):
        part = pre[j * chunk : (j + 1) * chunk]
        value, gate = part[:, :width], part[:, width:]
        outs[j][...] = (value * jax.nn.sigmoid(gate)).astype(jnp.bfloat16)


def attention_kernel(place, scale, rank, q_ref, up_ref, *refs):
    outer, inner, tp = place.outer, place.inner, place.tp_count
    n_k = tp * inner
    key_refs = refs[:n_k]
    out_ref, lse_ref, keys = refs[n_k:]
    zi, xi, ti = place.indices()
    heads, count, depth = q_ref.shape
    piece = key_refs[0].shape[0]
    share = piece // outer
    for n in range(n_k):
        keys[n * piece : (n + 1) * piece] = key_refs[n][...]
    lane = lax.broadcasted_iota(jnp.int32, (1, piece), 1)
    back = zi ^ lax.shift_right_logical(lane, share.bit_length() - 1)
    within = jnp.bitwise_and(lane, share - 1)
    parts = []
    for t in range(tp):
        owner = behind(ti, t, tp)
        for k in range(inner):
            parts.append((back * inner + (xi ^ k)) * count + owner * share + within)
    key_index = jnp.concatenate(parts, axis=1)
    first_row = (zi * inner + xi) * count
    together = math.gcd(heads, 4)
    size = together * count
    query_index = lax.broadcasted_iota(jnp.int32, (count, 1), 0) + first_row
    allowed = key_index <= jnp.concatenate([query_index] * together, axis=0)
    width = VALUE_HEAD_WIDTH
    sums = []
    for g in range(heads // together):
        queries = q_ref[g * together : (g + 1) * together].reshape(size, depth)
        scores = lax.dot_general(
            queries, keys[...], (((1,), (1,)), ((), ())), preferred_element_type=jnp.float32
        )
        scores = jnp.where(allowed, scores, masked_score)
        top = jnp.max(scores, axis=-1, keepdims=True)
        weights = jnp.exp2((scores - top) * (scale * math.log2(math.e)))
        total = jnp.sum(weights, axis=-1, keepdims=True)
        weighted = jnp.dot(
            weights.astype(jnp.bfloat16), keys[:, :rank], preferred_element_type=jnp.float32
        )
        latent_out = (weighted / total).astype(jnp.bfloat16)
        group_sums = top * scale + jnp.log(total)
        for i in range(together):
            h = g * together + i
            part = slice(i * count, (i + 1) * count)
            sums.append(group_sums[part])
            out_ref[:, h * width : (h + 1) * width] = jnp.dot(
                latent_out[part],
                up_ref[:, h * width : (h + 1) * width],
                preferred_element_type=jnp.float32,
            ).astype(jnp.bfloat16)
    spare = [jnp.zeros((count, 128 - heads), jnp.float32)]
    lse_ref[...] = jnp.concatenate(sums + spare, axis=1).T[:heads]


def local(
    tokens,
    norm_gain,
    w_value,
    w_gate,
    conv_taps,
    conv_gain,
    w_query,
    latent_down_weight,
    latent_norm_gain,
    w_rope_key,
    key_up_weight,
    value_up_weight,
    w_merge_conv,
    w_merge_attn,
):
    place = Place()
    outer, inner, tp_count = place.outer, place.inner, place.tp_count
    zi, xi, ti = place.indices()
    row_count = tokens.shape[0]
    share = row_count // tp_count
    depth = latent_down_weight.shape[0]
    rank = latent_down_weight.shape[1]

    split_rows = depth % (16 * tp_count) == 0
    own_table = jnp.concatenate([latent_down_weight, w_rope_key], axis=1)
    if split_rows:
        piece = depth // tp_count
        own_table = lax.dynamic_slice_in_dim(own_table, ti * piece, piece, 0)
    own_table, w_value, w_gate = lax.optimization_barrier((own_table, w_value, w_gate))
    table_parts = place.outer_gather(own_table)

    width = w_value.shape[1] // outer
    columns = []
    for j in range(outer):
        start = (zi ^ j) * width
        block = jnp.concatenate(
            [
                lax.dynamic_slice_in_dim(w_value, start, width, 1),
                lax.dynamic_slice_in_dim(w_gate, start, width, 1),
            ],
            axis=1,
        )
        columns.append(block if j == 0 else place.outer_swap(block, j))

    table = jnp.stack(table_parts)
    tables = place.inner_gather(table)

    gathered = lax.all_gather(tokens, "tp", axis=1, tiled=True)
    features = gathered.astype(jnp.float32)
    normed = (
        features
        * lax.rsqrt(jnp.mean(features * features, axis=-1, keepdims=True) + epsilon)
        * norm_gain
    ).astype(jnp.bfloat16)

    own_rows = lax.dynamic_slice_in_dim(normed, ti * share, share, 0)
    rows = place.outer_forward(own_rows)
    weight_block = jnp.stack(columns)
    taps = conv_taps.astype(jnp.float32)
    weight_block, query_rows, taps = lax.optimization_barrier((weight_block, normed, taps))
    weight_blocks = place.inner_gather(weight_block)

    bf16 = jnp.bfloat16
    model = normed.shape[1]
    head_count = key_up_weight.shape[1] // PLAIN_QK_WIDTH
    query_index = lax.axis_index("sp") * row_count + jnp.arange(row_count, dtype=jnp.int32)
    back = zi ^ jnp.arange(outer, dtype=jnp.int32)
    key_index = (
        ((back * inner + xi) * row_count + ti * share)[:, None]
        + jnp.arange(share, dtype=jnp.int32)[None, :]
    ).reshape(-1)
    angles = angles_at(
        jnp.concatenate([query_index, key_index]).astype(jnp.float32), QK_ROPE
    )
    cosine, sine = jnp.cos(angles), jnp.sin(angles)

    query_width = w_query.shape[1]
    queries = pl.pallas_call(
        functools.partial(query_kernel, rank),
        out_shape=jax.ShapeDtypeStruct((head_count, row_count, rank + QK_ROPE), bf16),
        in_specs=[whole_vmem()] + [pl.BlockSpec(memory_space=pltpu.HBM)] * 2 + [whole_vmem()] * 2,
        out_specs=whole_vmem(),
        scratch_shapes=[
            pltpu.VMEM((model, query_width), bf16),
            pltpu.VMEM(key_up_weight.shape, bf16),
            pltpu.SemaphoreType.DMA((head_count // 2 + 1,)),
        ],
        compiler_params=pltpu.CompilerParams(vmem_limit_bytes=52 << 20),
        cost_estimate=pl.CostEstimate(
            flops=2 * row_count * model * query_width,
            bytes_accessed=2 * model * query_width,
            transcendentals=0,
        ),
        name="queries",
    )(query_rows, w_query, key_up_weight, cosine, sine)

    tables, _ = lax.optimization_barrier((tables, queries))
    rows, _ = lax.optimization_barrier((rows, queries))
    if split_rows:
        tables = sum(place.tp_gather(tables), [])

    latent = pl.pallas_call(
        functools.partial(latent_kernel, place, rank, split_rows),
        out_shape=jax.ShapeDtypeStruct((outer * share, rank + QK_ROPE), bf16),
        in_specs=[whole_vmem()] * (outer + len(tables) + 3),
        out_specs=whole_vmem(),
        scratch_shapes=[
            pltpu.VMEM((outer * share, model), bf16),
            pltpu.VMEM((model, rank + QK_ROPE), bf16),
        ],
        compiler_params=pltpu.CompilerParams(vmem_limit_bytes=16 << 20),
        cost_estimate=pl.CostEstimate(
            flops=2 * outer * share * model * (rank + QK_ROPE),
            bytes_accessed=2 * model * (rank + QK_ROPE + outer * share),
            transcendentals=0,
        ),
        name="latents",
    )(*rows, *tables, latent_norm_gain[None, :], cosine, sine)
    _, *weight_blocks = lax.optimization_barrier((latent, *weight_blocks))
    latents = place.inner_gather(latent)
    latents = sum(place.tp_gather(latents), [])

    all_rows = sum(place.tp_gather(rows), [])
    gated = pl.pallas_call(
        functools.partial(gated_kernel, place),
        out_shape=[jax.ShapeDtypeStruct((row_count, width), bf16)] * outer,
        in_specs=[whole_vmem()] * (len(all_rows) + inner),
        out_specs=[whole_vmem()] * outer,
        scratch_shapes=[
            pltpu.VMEM((outer * row_count, model), bf16),
            pltpu.VMEM((model, 2 * width), bf16),
        ],
        compiler_params=pltpu.CompilerParams(vmem_limit_bytes=24 << 20),
        cost_estimate=pl.CostEstimate(
            flops=4 * outer * row_count * model * width,
            bytes_accessed=2 * model * (2 * width + outer * row_count),
            transcendentals=outer * row_count * width,
        ),
        name="gated",
    )(*all_rows, *weight_blocks)
    home = [gated[0]] + [place.outer_swap(gated[j], j) for j in range(1, outer)]
    gated_rows = jnp.concatenate(untangled(home, zi), axis=1)

    conv_reach = conv_taps.shape[0] - 1
    prior_rows = lax.ppermute(
        gated_rows[row_count - conv_reach :],
        "sp",
        [(i, i + 1) for i in range(place.sp_count - 1)],
    )
    score_scale = (PLAIN_QK_WIDTH + QK_ROPE) ** (-0.5)
    key_total = place.sp_count * row_count
    attention, log_sums = pl.pallas_call(
        functools.partial(attention_kernel, place, score_scale, rank),
        out_shape=[
            jax.ShapeDtypeStruct((row_count, head_count * VALUE_HEAD_WIDTH), bf16),
            jax.ShapeDtypeStruct((head_count, row_count), jnp.float32),
        ],
        in_specs=[whole_vmem()] * (2 + len(latents)),
        out_specs=[whole_vmem()] * 2,
        scratch_shapes=[
            pltpu.VMEM((key_total, rank + QK_ROPE), bf16),
        ],
        compiler_params=pltpu.CompilerParams(vmem_limit_bytes=32 << 20),
        cost_estimate=pl.CostEstimate(
            flops=2 * row_count * head_count * key_total * (2 * rank + QK_ROPE),
            bytes_accessed=2 * key_total * (rank + QK_ROPE),
            transcendentals=row_count * head_count * key_total,
        ),
        name="attention",
    )(queries, value_up_weight, *latents)

    attn_part = jnp.dot(attention, w_merge_attn, preferred_element_type=jnp.float32)
    prior_rows, gated_rows, _ = lax.optimization_barrier((prior_rows, gated_rows, attn_part))
    padded = jnp.concatenate([prior_rows, gated_rows], axis=0).astype(jnp.float32)
    mixed = jnp.zeros(gated_rows.shape, jnp.float32)
    for tap_index in range(conv_taps.shape[0]):
        mixed = (
            mixed
            + taps[tap_index] * padded[tap_index : tap_index + row_count]
        )
    channel_total = mixed.shape[1] * tp_count
    stats = jnp.stack([jnp.sum(mixed, axis=1), jnp.sum(mixed * mixed, axis=1)])
    stat_sum, stat_squares = sum(
        [place.tp_shift(stats, t) for t in range(1, tp_count)], start=stats
    )
    channel_mean = stat_sum / channel_total
    channel_var = stat_squares / channel_total - channel_mean * channel_mean
    conv_out = jax.nn.silu(
        (mixed - channel_mean[:, None]) * lax.rsqrt(channel_var + epsilon)[:, None] * conv_gain
    ).astype(bf16)

    conv_part = jnp.dot(conv_out, w_merge_conv, preferred_element_type=jnp.float32)
    conv_part = lax.optimization_barrier(conv_part)
    partial = (conv_part + attn_part).astype(bf16)
    merged = lax.dynamic_slice_in_dim(partial, ti * share, share, 0).astype(jnp.float32)
    for t in range(1, tp_count):
        away = lax.dynamic_slice_in_dim(partial, lax.rem(ti + t, tp_count) * share, share, 0)
        merged = merged + place.tp_shift(away, t).astype(jnp.float32)
    return (merged.astype(bf16), log_sums.T)


def solution(mesh):
    return jax.shard_map(
        local,
        mesh=mesh,
        in_specs=(
            P("sp", "tp"),
            P(),
            P("sp", "tp"),
            P("sp", "tp"),
            P(None, "tp"),
            P("tp"),
            P(None, "tp"),
            P("sp", None),
            P(),
            P("sp", None),
            P(None, "tp"),
            P(None, "tp"),
            P("tp", None),
            P("tp", None),
        ),
        out_specs=(P(("sp", "tp"), None), P("sp", "tp")),
        check_vma=False,
    )
```

```python
import functools
import math

import jax
import jax.numpy as jnp
from jax import lax
from jax.experimental import pallas as pl
from jax.experimental.pallas import tpu as pltpu
from jax.sharding import PartitionSpec as P


PLAIN_QK_WIDTH = 128
QK_ROPE = 64
VALUE_HEAD_WIDTH = 128


epsilon = 1e-06
rope_base = 10000.0
masked_score = -1e30


def angles_at(positions, width):
    inverse = rope_base ** (-2.0 * jnp.arange(width // 2, dtype=jnp.float32) / width)
    return positions[:, None] * inverse[None, :]


class Place:
    def __init__(self):
        self.sp_count = lax.axis_size("sp")
        self.tp_count = lax.axis_size("tp")
        self.inner = math.gcd(self.sp_count, 4)
        self.outer = self.sp_count // self.inner

    def indices(self):
        index = lax.axis_index("sp")
        return index // self.inner, index % self.inner, lax.axis_index("tp")

    def outer_swap(self, block, mask):
        mask = mask * self.inner
        return lax.ppermute(block, "sp", [(i, i ^ mask) for i in range(self.sp_count)])

    def inner_swap(self, block, mask):
        return lax.ppermute(block, "sp", [(i, i ^ mask) for i in range(self.sp_count)])

    def inner_forward(self, block):
        half = block.shape[0] // 2
        if self.inner != 4 or half == 0:
            return [(k, 0) for k in range(self.inner)], self.inner_gather(block)
        one, two = self.inner_swap(block, 1), self.inner_swap(block, 2)
        low, high = self.inner_swap(two[:half], 1), self.inner_swap(one[half:], 2)
        return [(0, 0), (1, 0), (2, 0), (3, 0), (3, half)], [block, one, two, low, high]

    def tp_shift(self, block, distance):
        route = [(i, (i + distance) % self.tp_count) for i in range(self.tp_count)]
        return lax.ppermute(block, "tp", route)

    def outer_gather(self, block):
        return [block] + [self.outer_swap(block, j) for j in range(1, self.outer)]

    def outer_forward(self, block):
        blocks = [block]
        for j in range(1, self.outer):
            near = j & -j
            blocks.append(self.outer_swap(blocks[j ^ near], near))
        return blocks

    def inner_gather(self, block):
        return [block] + [self.inner_swap(block, k) for k in range(1, self.inner)]

    def tp_gather(self, blocks):
        return [blocks] + [
            [self.tp_shift(b, t) for b in blocks] for t in range(1, self.tp_count)
        ]


def behind(index, distance, count):
    return lax.rem(index - distance + count, count)


def untangled(blocks, index):
    bit = 1
    while bit < len(blocks):
        flag = (index & bit) > 0
        blocks = [jnp.where(flag, blocks[i ^ bit], b) for i, b in enumerate(blocks)]
        bit *= 2
    return blocks


def copy_all(pairs, sem):
    copies = [pltpu.make_async_copy(s, d, sem.at[n]) for n, (s, d) in enumerate(pairs)]
    for c in copies:
        c.start()
    return copies


def whole_vmem():
    return pl.BlockSpec(memory_space=pltpu.VMEM)


def turned(first, second, cosine, sine):
    return jnp.concatenate(
        [first * cosine - second * sine, first * sine + second * cosine], axis=-1
    ).astype(jnp.bfloat16)


def query_kernel(rank, normed_ref, w_ref, up_ref, cos_ref, sin_ref, out_ref, w, up, sem):
    heads, count, _ = out_ref.shape
    plain, half = PLAIN_QK_WIDTH, QK_ROPE // 2
    head = plain + QK_ROPE
    span = 2 * head
    pairs = heads // 2
    copies = copy_all(
        [
            (w_ref.at[:, p * span : (p + 1) * span], w.at[:, p * span : (p + 1) * span])
            for p in range(pairs)
        ]
        + [(up_ref, up)],
        sem,
    )
    cosine, sine = cos_ref[:count], sin_ref[:count]
    for p in range(pairs):
        copies[p].wait()
        query = jnp.dot(
            normed_ref[...], w[:, p * span : (p + 1) * span], preferred_element_type=jnp.float32
        ).astype(jnp.bfloat16)
        if p == 0:
            copies[pairs].wait()
        for i in range(2):
            h = 2 * p + i
            own = query[:, i * head : (i + 1) * head]
            out_ref[h, :, :rank] = lax.dot_general(
                own[:, :plain],
                up[:, h * plain : (h + 1) * plain],
                (((1,), (1,)), ((), ())),
                preferred_element_type=jnp.float32,
            ).astype(jnp.bfloat16)
            rope = own[:, plain:].astype(jnp.float32)
            out_ref[h, :, rank:] = turned(rope[:, :half], rope[:, half:], cosine, sine)


def latent_kernel(place, rank, share, parts, *refs):
    outer, inner, tp = place.outer, place.inner, place.tp_count
    tables = tp if share else 1
    n_rows, n_w = outer, tables * len(parts)
    row_refs, w_refs = refs[:n_rows], refs[n_rows : n_rows + n_w]
    gain_ref, cos_ref, sin_ref, out_ref, rows, weight = refs[n_rows + n_w :]
    zi, xi, ti = place.indices()
    piece = w_refs[0].shape[1]
    block = piece * tables
    count = row_refs[0].shape[0]
    for t in range(tables):
        owner = behind(ti, t, tp) if share else 0
        for (k, first), ref in zip(parts, w_refs[t * len(parts) :]):
            for j in range(ref.shape[0]):
                start = ((zi ^ (first + j)) * inner + (xi ^ k)) * block + owner * piece
                weight[pl.ds(pl.multiple_of(start, piece), piece)] = ref[j]
    for j in range(outer):
        rows[j * count : (j + 1) * count] = row_refs[j][...]
    pre = jnp.dot(rows[...], weight[...], preferred_element_type=jnp.float32)
    plain = pre[:, :rank]
    scale = lax.rsqrt(jnp.mean(plain * plain, axis=-1, keepdims=True) + epsilon)
    out_ref[:, :rank] = (plain * scale * gain_ref[...]).astype(jnp.bfloat16)
    rope = pre[:, rank:]
    half = rope.shape[1] // 2
    total = outer * count
    cosine, sine = cos_ref[cos_ref.shape[0] - total :], sin_ref[sin_ref.shape[0] - total :]
    out_ref[:, rank:] = turned(rope[:, :half], rope[:, half:], cosine, sine)


def gated_kernel(place, parts, *refs):
    outer, inner, tp = place.outer, place.inner, place.tp_count
    n_rows = tp * outer
    n_w = len(parts)
    row_refs, w_refs = refs[:n_rows], refs[n_rows : n_rows + n_w]
    outs = refs[n_rows + n_w : n_rows + n_w + outer]
    rows, weight = refs[n_rows + n_w + outer :]
    zi, xi, ti = place.indices()
    block = w_refs[0].shape[1]
    count = row_refs[0].shape[0]
    for (k, first), ref in zip(parts, w_refs):
        for j in range(ref.shape[0]):
            start = ((zi ^ (first + j)) * inner + (xi ^ k)) * block
            weight[pl.ds(pl.multiple_of(start, block), block)] = ref[j]
    for t in range(tp):
        owner = behind(ti, t, tp)
        for j in range(outer):
            start = j * tp * count + owner * count
            rows[pl.ds(pl.multiple_of(start, count), count)] = row_refs[t * outer + j][...]
    chunk = tp * count
    width = outs[0].shape[1]
    pre = jnp.dot(rows[...], weight[...], preferred_element_type=jnp.float32)
    for j in range(outer):
        part = pre[j * chunk : (j + 1) * chunk]
        value, gate = part[:, :width], part[:, width:]
        outs[j][...] = (value * jax.nn.sigmoid(gate)).astype(jnp.bfloat16)


def attention_kernel(place, scale, rank, q_ref, up_ref, *refs):
    outer, inner, tp = place.outer, place.inner, place.tp_count
    n_k = tp * inner
    key_refs = refs[:n_k]
    out_ref, lse_ref, keys = refs[n_k:]
    zi, xi, ti = place.indices()
    heads, count, depth = q_ref.shape
    piece = key_refs[0].shape[0]
    share = piece // outer
    for n in range(n_k):
        keys[n * piece : (n + 1) * piece] = key_refs[n][...]
    lane = lax.broadcasted_iota(jnp.int32, (1, piece), 1)
    back = zi ^ lax.shift_right_logical(lane, share.bit_length() - 1)
    within = jnp.bitwise_and(lane, share - 1)
    parts = []
    for t in range(tp):
        owner = behind(ti, t, tp)
        for k in range(inner):
            parts.append((back * inner + (xi ^ k)) * count + owner * share + within)
    key_index = jnp.concatenate(parts, axis=1)
    first_row = (zi * inner + xi) * count
    together = math.gcd(heads, 4)
    size = together * count
    query_index = lax.broadcasted_iota(jnp.int32, (count, 1), 0) + first_row
    allowed = key_index <= jnp.concatenate([query_index] * together, axis=0)
    width = VALUE_HEAD_WIDTH
    sums = []
    for g in range(heads // together):
        queries = q_ref[g * together : (g + 1) * together].reshape(size, depth)
        scores = lax.dot_general(
            queries, keys[...], (((1,), (1,)), ((), ())), preferred_element_type=jnp.float32
        )
        scores = jnp.where(allowed, scores, masked_score)
        top = jnp.max(scores, axis=-1, keepdims=True)
        weights = jnp.exp2((scores - top) * (scale * math.log2(math.e)))
        total = jnp.sum(weights, axis=-1, keepdims=True)
        weighted = jnp.dot(
            weights.astype(jnp.bfloat16), keys[:, :rank], preferred_element_type=jnp.float32
        )
        latent_out = (weighted / total).astype(jnp.bfloat16)
        group_sums = top * scale + jnp.log(total)
        for i in range(together):
            h = g * together + i
            part = slice(i * count, (i + 1) * count)
            sums.append(group_sums[part])
            out_ref[:, h * width : (h + 1) * width] = jnp.dot(
                latent_out[part],
                up_ref[:, h * width : (h + 1) * width],
                preferred_element_type=jnp.float32,
            ).astype(jnp.bfloat16)
    spare = [jnp.zeros((count, 128 - heads), jnp.float32)]
    lse_ref[...] = jnp.concatenate(sums + spare, axis=1).T[:heads]


def local(
    tokens,
    norm_gain,
    w_value,
    w_gate,
    conv_taps,
    conv_gain,
    w_query,
    latent_down_weight,
    latent_norm_gain,
    w_rope_key,
    key_up_weight,
    value_up_weight,
    w_merge_conv,
    w_merge_attn,
):
    place = Place()
    outer, inner, tp_count = place.outer, place.inner, place.tp_count
    zi, xi, ti = place.indices()
    row_count = tokens.shape[0]
    share = row_count // tp_count
    depth = latent_down_weight.shape[0]
    rank = latent_down_weight.shape[1]

    split_rows = depth % (16 * tp_count) == 0
    own_table = jnp.concatenate([latent_down_weight, w_rope_key], axis=1)
    if split_rows:
        piece = depth // tp_count
        own_table = lax.dynamic_slice_in_dim(own_table, ti * piece, piece, 0)
    own_table, w_value, w_gate = lax.optimization_barrier((own_table, w_value, w_gate))
    table_parts = place.outer_gather(own_table)

    width = w_value.shape[1] // outer
    columns = []
    for j in range(outer):
        start = (zi ^ j) * width
        block = jnp.concatenate(
            [
                lax.dynamic_slice_in_dim(w_value, start, width, 1),
                lax.dynamic_slice_in_dim(w_gate, start, width, 1),
            ],
            axis=1,
        )
        columns.append(block if j == 0 else place.outer_swap(block, j))

    table = jnp.stack(table_parts)
    table_map, tables = place.inner_forward(table)

    gathered = lax.all_gather(tokens, "tp", axis=1, tiled=True)
    features = gathered.astype(jnp.float32)
    normed = (
        features
        * lax.rsqrt(jnp.mean(features * features, axis=-1, keepdims=True) + epsilon)
        * norm_gain
    ).astype(jnp.bfloat16)

    own_rows = lax.dynamic_slice_in_dim(normed, ti * share, share, 0)
    rows = place.outer_forward(own_rows)
    weight_block = jnp.stack(columns)
    weight_block, query_rows = lax.optimization_barrier((weight_block, normed))
    weight_map, weight_blocks = place.inner_forward(weight_block)

    bf16 = jnp.bfloat16
    model = normed.shape[1]
    head_count = key_up_weight.shape[1] // PLAIN_QK_WIDTH
    query_index = lax.axis_index("sp") * row_count + jnp.arange(row_count, dtype=jnp.int32)
    back = zi ^ jnp.arange(outer, dtype=jnp.int32)
    key_index = (
        ((back * inner + xi) * row_count + ti * share)[:, None]
        + jnp.arange(share, dtype=jnp.int32)[None, :]
    ).reshape(-1)
    angles = angles_at(
        jnp.concatenate([query_index, key_index]).astype(jnp.float32), QK_ROPE
    )
    cosine, sine = jnp.cos(angles), jnp.sin(angles)

    query_width = w_query.shape[1]
    queries = pl.pallas_call(
        functools.partial(query_kernel, rank),
        out_shape=jax.ShapeDtypeStruct((head_count, row_count, rank + QK_ROPE), bf16),
        in_specs=[whole_vmem()] + [pl.BlockSpec(memory_space=pltpu.HBM)] * 2 + [whole_vmem()] * 2,
        out_specs=whole_vmem(),
        scratch_shapes=[
            pltpu.VMEM((model, query_width), bf16),
            pltpu.VMEM(key_up_weight.shape, bf16),
            pltpu.SemaphoreType.DMA((head_count // 2 + 1,)),
        ],
        compiler_params=pltpu.CompilerParams(vmem_limit_bytes=52 << 20),
        cost_estimate=pl.CostEstimate(
            flops=2 * row_count * model * query_width,
            bytes_accessed=2 * model * query_width,
            transcendentals=0,
        ),
        name="queries",
    )(query_rows, w_query, key_up_weight, cosine, sine)

    tables, _ = lax.optimization_barrier((tables, queries))
    tap_rows = [conv_taps[n].astype(jnp.float32) for n in range(conv_taps.shape[0])]
    rows, tap_rows, _ = lax.optimization_barrier((rows, tap_rows, queries))
    if split_rows:
        tables = sum(place.tp_gather(tables), [])

    latent = pl.pallas_call(
        functools.partial(latent_kernel, place, rank, split_rows, table_map),
        out_shape=jax.ShapeDtypeStruct((outer * share, rank + QK_ROPE), bf16),
        in_specs=[whole_vmem()] * (outer + len(tables) + 3),
        out_specs=whole_vmem(),
        scratch_shapes=[
            pltpu.VMEM((outer * share, model), bf16),
            pltpu.VMEM((model, rank + QK_ROPE), bf16),
        ],
        compiler_params=pltpu.CompilerParams(vmem_limit_bytes=16 << 20),
        cost_estimate=pl.CostEstimate(
            flops=2 * outer * share * model * (rank + QK_ROPE),
            bytes_accessed=2 * model * (rank + QK_ROPE + outer * share),
            transcendentals=0,
        ),
        name="latents",
    )(*rows, *tables, latent_norm_gain[None, :], cosine, sine)
    _, *weight_blocks = lax.optimization_barrier((latent, *weight_blocks))
    latents = place.inner_gather(latent)
    latents = sum(place.tp_gather(latents), [])

    all_rows = sum(place.tp_gather(rows), [])
    gated = pl.pallas_call(
        functools.partial(gated_kernel, place, weight_map),
        out_shape=[jax.ShapeDtypeStruct((row_count, width), bf16)] * outer,
        in_specs=[whole_vmem()] * (len(all_rows) + len(weight_blocks)),
        out_specs=[whole_vmem()] * outer,
        scratch_shapes=[
            pltpu.VMEM((outer * row_count, model), bf16),
            pltpu.VMEM((model, 2 * width), bf16),
        ],
        compiler_params=pltpu.CompilerParams(vmem_limit_bytes=24 << 20),
        cost_estimate=pl.CostEstimate(
            flops=4 * outer * row_count * model * width,
            bytes_accessed=2 * model * (2 * width + outer * row_count),
            transcendentals=outer * row_count * width,
        ),
        name="gated",
    )(*all_rows, *weight_blocks)
    home = [gated[0]] + [place.outer_swap(gated[j], j) for j in range(1, outer)]
    gated_rows = jnp.concatenate(untangled(home, zi), axis=1)

    conv_reach = conv_taps.shape[0] - 1
    prior_rows = lax.ppermute(
        gated_rows[row_count - conv_reach :],
        "sp",
        [(i, i + 1) for i in range(place.sp_count - 1)],
    )
    score_scale = (PLAIN_QK_WIDTH + QK_ROPE) ** (-0.5)
    key_total = place.sp_count * row_count
    attention, log_sums = pl.pallas_call(
        functools.partial(attention_kernel, place, score_scale, rank),
        out_shape=[
            jax.ShapeDtypeStruct((row_count, head_count * VALUE_HEAD_WIDTH), bf16),
            jax.ShapeDtypeStruct((head_count, row_count), jnp.float32),
        ],
        in_specs=[whole_vmem()] * (2 + len(latents)),
        out_specs=[whole_vmem()] * 2,
        scratch_shapes=[
            pltpu.VMEM((key_total, rank + QK_ROPE), bf16),
        ],
        compiler_params=pltpu.CompilerParams(vmem_limit_bytes=32 << 20),
        cost_estimate=pl.CostEstimate(
            flops=2 * row_count * head_count * key_total * (2 * rank + QK_ROPE),
            bytes_accessed=2 * key_total * (rank + QK_ROPE),
            transcendentals=row_count * head_count * key_total,
        ),
        name="attention",
    )(queries, value_up_weight, *latents)

    attn_part = jnp.dot(attention, w_merge_attn, preferred_element_type=jnp.float32)
    prior_rows, gated_rows, _ = lax.optimization_barrier((prior_rows, gated_rows, attn_part))
    padded = jnp.concatenate([prior_rows, gated_rows], axis=0).astype(jnp.float32)
    mixed = jnp.zeros(gated_rows.shape, jnp.float32)
    for tap_index in range(conv_taps.shape[0]):
        mixed = (
            mixed
            + tap_rows[tap_index] * padded[tap_index : tap_index + row_count]
        )
    channel_total = mixed.shape[1] * tp_count
    stats = jnp.stack([jnp.sum(mixed, axis=1), jnp.sum(mixed * mixed, axis=1)])
    stat_sum, stat_squares = sum(
        [place.tp_shift(stats, t) for t in range(1, tp_count)], start=stats
    )
    channel_mean = stat_sum / channel_total
    channel_var = stat_squares / channel_total - channel_mean * channel_mean
    conv_out = jax.nn.silu(
        (mixed - channel_mean[:, None]) * lax.rsqrt(channel_var + epsilon)[:, None] * conv_gain
    ).astype(bf16)

    partial = (
        attn_part + jnp.dot(conv_out, w_merge_conv, preferred_element_type=jnp.float32)
    ).astype(bf16)
    merged = lax.dynamic_slice_in_dim(partial, ti * share, share, 0).astype(jnp.float32)
    for t in range(1, tp_count):
        away = lax.dynamic_slice_in_dim(partial, lax.rem(ti + t, tp_count) * share, share, 0)
        merged = merged + place.tp_shift(away, t).astype(jnp.float32)
    return (merged.astype(bf16), log_sums.T)


def solution(mesh):
    return jax.shard_map(
        local,
        mesh=mesh,
        in_specs=(
            P("sp", "tp"),
            P(),
            P("sp", "tp"),
            P("sp", "tp"),
            P(None, "tp"),
            P("tp"),
            P(None, "tp"),
            P("sp", None),
            P(),
            P("sp", None),
            P(None, "tp"),
            P(None, "tp"),
            P("tp", None),
            P("tp", None),
        ),
        out_specs=(P(("sp", "tp"), None), P("sp", "tp")),
        check_vma=False,
    )
```

```python
import functools
import math

import jax
import jax.numpy as jnp
from jax import lax
from jax.experimental import pallas as pl
from jax.experimental.pallas import tpu as pltpu
from jax.sharding import PartitionSpec as P


PLAIN_QK_WIDTH = 128
QK_ROPE = 64
VALUE_HEAD_WIDTH = 128


epsilon = 1e-06
rope_base = 10000.0
masked_score = -1e30


def angles_at(positions, width):
    inverse = rope_base ** (-2.0 * jnp.arange(width // 2, dtype=jnp.float32) / width)
    return positions[:, None] * inverse[None, :]


class Place:
    def __init__(self):
        self.sp_count = lax.axis_size("sp")
        self.tp_count = lax.axis_size("tp")
        self.inner = math.gcd(self.sp_count, 4)
        self.outer = self.sp_count // self.inner

    def indices(self):
        index = lax.axis_index("sp")
        return index // self.inner, index % self.inner, lax.axis_index("tp")

    def outer_swap(self, block, mask):
        mask = mask * self.inner
        return lax.ppermute(block, "sp", [(i, i ^ mask) for i in range(self.sp_count)])

    def inner_swap(self, block, mask):
        return lax.ppermute(block, "sp", [(i, i ^ mask) for i in range(self.sp_count)])

    def tp_shift(self, block, distance):
        route = [(i, (i + distance) % self.tp_count) for i in range(self.tp_count)]
        return lax.ppermute(block, "tp", route)

    def outer_gather(self, block):
        return [block] + [self.outer_swap(block, j) for j in range(1, self.outer)]

    def outer_forward(self, block):
        blocks = [block]
        for j in range(1, self.outer):
            near = j & -j
            blocks.append(self.outer_swap(blocks[j ^ near], near))
        return blocks

    def inner_gather(self, block):
        return [block] + [self.inner_swap(block, k) for k in range(1, self.inner)]

    def tp_gather(self, blocks):
        return [blocks] + [
            [self.tp_shift(b, t) for b in blocks] for t in range(1, self.tp_count)
        ]


def behind(index, distance, count):
    return lax.rem(index - distance + count, count)


def copy_all(pairs, sem):
    copies = [pltpu.make_async_copy(s, d, sem.at[n]) for n, (s, d) in enumerate(pairs)]
    for c in copies:
        c.start()
    return copies


def whole_vmem():
    return pl.BlockSpec(memory_space=pltpu.VMEM)


def turned(first, second, cosine, sine):
    return jnp.concatenate(
        [first * cosine - second * sine, first * sine + second * cosine], axis=-1
    ).astype(jnp.bfloat16)


def query_kernel(rank, normed_ref, w_ref, up_ref, cos_ref, sin_ref, out_ref, w, up, sem):
    heads, count, _ = out_ref.shape
    plain, half = PLAIN_QK_WIDTH, QK_ROPE // 2
    head = plain + QK_ROPE
    span = 2 * head
    pairs = heads // 2
    copies = copy_all(
        [
            (w_ref.at[:, p * span : (p + 1) * span], w.at[:, p * span : (p + 1) * span])
            for p in range(pairs)
        ]
        + [(up_ref, up)],
        sem,
    )
    cosine, sine = cos_ref[:count], sin_ref[:count]
    for p in range(pairs):
        copies[p].wait()
        query = jnp.dot(
            normed_ref[...], w[:, p * span : (p + 1) * span], preferred_element_type=jnp.float32
        ).astype(jnp.bfloat16)
        if p == 0:
            copies[pairs].wait()
        for i in range(2):
            h = 2 * p + i
            own = query[:, i * head : (i + 1) * head]
            out_ref[h, :, :rank] = lax.dot_general(
                own[:, :plain],
                up[:, h * plain : (h + 1) * plain],
                (((1,), (1,)), ((), ())),
                preferred_element_type=jnp.float32,
            ).astype(jnp.bfloat16)
            rope = own[:, plain:].astype(jnp.float32)
            out_ref[h, :, rank:] = turned(rope[:, :half], rope[:, half:], cosine, sine)


def latent_kernel(place, rank, share, *refs):
    outer, inner, tp = place.outer, place.inner, place.tp_count
    tables = tp if share else 1
    n_rows, n_w = outer, tables * inner
    row_refs, w_refs = refs[:n_rows], refs[n_rows : n_rows + n_w]
    gain_ref, cos_ref, sin_ref, out_ref, rows, weight = refs[n_rows + n_w :]
    zi, xi, ti = place.indices()
    piece = w_refs[0].shape[1]
    block = piece * tables
    count = row_refs[0].shape[0]
    for t in range(tables):
        owner = behind(ti, t, tp) if share else 0
        for k in range(inner):
            for j in range(outer):
                start = ((zi ^ j) * inner + (xi ^ k)) * block + owner * piece
                weight[pl.ds(pl.multiple_of(start, piece), piece)] = w_refs[t * inner + k][j]
    for j in range(outer):
        rows[j * count : (j + 1) * count] = row_refs[j][...]
    pre = jnp.dot(rows[...], weight[...], preferred_element_type=jnp.float32)
    plain = pre[:, :rank]
    scale = lax.rsqrt(jnp.mean(plain * plain, axis=-1, keepdims=True) + epsilon)
    out_ref[:, :rank] = (plain * scale * gain_ref[...]).astype(jnp.bfloat16)
    rope = pre[:, rank:]
    half = rope.shape[1] // 2
    total = outer * count
    cosine, sine = cos_ref[cos_ref.shape[0] - total :], sin_ref[sin_ref.shape[0] - total :]
    out_ref[:, rank:] = turned(rope[:, :half], rope[:, half:], cosine, sine)


def gated_kernel(place, *refs):
    outer, inner, tp = place.outer, place.inner, place.tp_count
    n_rows = tp * outer
    row_refs, w_refs = refs[:n_rows], refs[n_rows : n_rows + inner]
    outs = refs[n_rows + inner : n_rows + inner + outer]
    rows, weight = refs[n_rows + inner + outer :]
    zi, xi, ti = place.indices()
    block = w_refs[0].shape[1]
    count = row_refs[0].shape[0]
    for k in range(inner):
        for j in range(outer):
            start = ((zi ^ j) * inner + (xi ^ k)) * block
            weight[pl.ds(pl.multiple_of(start, block), block)] = w_refs[k][j]
    for t in range(tp):
        owner = behind(ti, t, tp)
        for j in range(outer):
            start = j * tp * count + owner * count
            rows[pl.ds(pl.multiple_of(start, count), count)] = row_refs[t * outer + j][...]
    chunk = tp * count
    width = outs[0].shape[1]
    pre = jnp.dot(rows[...], weight[...], preferred_element_type=jnp.float32)
    for j in range(outer):
        part = pre[j * chunk : (j + 1) * chunk]
        value, gate = part[:, :width], part[:, width:]
        outs[j][...] = (value * jax.nn.sigmoid(gate)).astype(jnp.bfloat16)


def attention_kernel(place, scale, rank, q_ref, up_ref, *refs):
    outer, inner, tp = place.outer, place.inner, place.tp_count
    n_k = tp * inner
    key_refs = refs[:n_k]
    out_ref, lse_ref, keys = refs[n_k:]
    zi, xi, ti = place.indices()
    heads, count, depth = q_ref.shape
    piece = key_refs[0].shape[0]
    share = piece // outer
    for n in range(n_k):
        keys[n * piece : (n + 1) * piece] = key_refs[n][...]
    lane = lax.broadcasted_iota(jnp.int32, (1, piece), 1)
    back = zi ^ lax.shift_right_logical(lane, share.bit_length() - 1)
    within = jnp.bitwise_and(lane, share - 1)
    parts = []
    for t in range(tp):
        owner = behind(ti, t, tp)
        for k in range(inner):
            parts.append((back * inner + (xi ^ k)) * count + owner * share + within)
    key_index = jnp.concatenate(parts, axis=1)
    first_row = (zi * inner + xi) * count
    together = math.gcd(heads, 4)
    size = together * count
    query_index = lax.broadcasted_iota(jnp.int32, (count, 1), 0) + first_row
    allowed = key_index <= jnp.concatenate([query_index] * together, axis=0)
    width = VALUE_HEAD_WIDTH
    sums = []
    for g in range(heads // together):
        queries = q_ref[g * together : (g + 1) * together].reshape(size, depth)
        scores = lax.dot_general(
            queries, keys[...], (((1,), (1,)), ((), ())), preferred_element_type=jnp.float32
        )
        scores = jnp.where(allowed, scores, masked_score)
        top = jnp.max(scores, axis=-1, keepdims=True)
        weights = jnp.exp2((scores - top) * (scale * math.log2(math.e)))
        total = jnp.sum(weights, axis=-1, keepdims=True)
        weighted = jnp.dot(
            weights.astype(jnp.bfloat16), keys[:, :rank], preferred_element_type=jnp.float32
        )
        latent_out = (weighted / total).astype(jnp.bfloat16)
        group_sums = top * scale + jnp.log(total)
        for i in range(together):
            h = g * together + i
            part = slice(i * count, (i + 1) * count)
            sums.append(group_sums[part])
            out_ref[:, h * width : (h + 1) * width] = jnp.dot(
                latent_out[part],
                up_ref[:, h * width : (h + 1) * width],
                preferred_element_type=jnp.float32,
            ).astype(jnp.bfloat16)
    spare = [jnp.zeros((count, 128 - heads), jnp.float32)]
    lse_ref[...] = jnp.concatenate(sums + spare, axis=1).T[:heads]


def local(
    tokens,
    norm_gain,
    w_value,
    w_gate,
    conv_taps,
    conv_gain,
    w_query,
    latent_down_weight,
    latent_norm_gain,
    w_rope_key,
    key_up_weight,
    value_up_weight,
    w_merge_conv,
    w_merge_attn,
):
    place = Place()
    outer, inner, tp_count = place.outer, place.inner, place.tp_count
    zi, xi, ti = place.indices()
    row_count = tokens.shape[0]
    share = row_count // tp_count
    depth = latent_down_weight.shape[0]
    rank = latent_down_weight.shape[1]

    split_rows = depth % (16 * tp_count) == 0
    own_table = jnp.concatenate([latent_down_weight, w_rope_key], axis=1)
    if split_rows:
        piece = depth // tp_count
        own_table = lax.dynamic_slice_in_dim(own_table, ti * piece, piece, 0)
    own_table, w_value, w_gate = lax.optimization_barrier((own_table, w_value, w_gate))
    table_parts = place.outer_gather(own_table)

    width = w_value.shape[1] // outer
    columns = []
    for j in range(outer):
        start = (zi ^ j) * width
        block = jnp.concatenate(
            [
                lax.dynamic_slice_in_dim(w_value, start, width, 1),
                lax.dynamic_slice_in_dim(w_gate, start, width, 1),
            ],
            axis=1,
        )
        columns.append(block if j == 0 else place.outer_swap(block, j))

    table = jnp.stack(table_parts)
    table, tokens = lax.optimization_barrier((table, tokens))
    tables = place.inner_gather(table)

    gathered = lax.all_gather(tokens, "tp", axis=1, tiled=True)
    features = gathered.astype(jnp.float32)
    normed = (
        features
        * lax.rsqrt(jnp.mean(features * features, axis=-1, keepdims=True) + epsilon)
        * norm_gain
    ).astype(jnp.bfloat16)

    own_rows = lax.dynamic_slice_in_dim(normed, ti * share, share, 0)
    rows = place.outer_forward(own_rows)
    weight_block = jnp.stack(columns)
    weight_block, query_rows = lax.optimization_barrier((weight_block, normed))
    weight_blocks = place.inner_gather(weight_block)

    bf16 = jnp.bfloat16
    model = normed.shape[1]
    head_count = key_up_weight.shape[1] // PLAIN_QK_WIDTH
    query_index = lax.axis_index("sp") * row_count + jnp.arange(row_count, dtype=jnp.int32)
    back = zi ^ jnp.arange(outer, dtype=jnp.int32)
    key_index = (
        ((back * inner + xi) * row_count + ti * share)[:, None]
        + jnp.arange(share, dtype=jnp.int32)[None, :]
    ).reshape(-1)
    angles = angles_at(
        jnp.concatenate([query_index, key_index]).astype(jnp.float32), QK_ROPE
    )
    cosine, sine = jnp.cos(angles), jnp.sin(angles)

    query_width = w_query.shape[1]
    queries = pl.pallas_call(
        functools.partial(query_kernel, rank),
        out_shape=jax.ShapeDtypeStruct((head_count, row_count, rank + QK_ROPE), bf16),
        in_specs=[whole_vmem()] + [pl.BlockSpec(memory_space=pltpu.HBM)] * 2 + [whole_vmem()] * 2,
        out_specs=whole_vmem(),
        scratch_shapes=[
            pltpu.VMEM((model, query_width), bf16),
            pltpu.VMEM(key_up_weight.shape, bf16),
            pltpu.SemaphoreType.DMA((head_count // 2 + 1,)),
        ],
        compiler_params=pltpu.CompilerParams(vmem_limit_bytes=52 << 20),
        cost_estimate=pl.CostEstimate(
            flops=2 * row_count * model * query_width,
            bytes_accessed=2 * model * query_width,
            transcendentals=0,
        ),
        name="queries",
    )(query_rows, w_query, key_up_weight, cosine, sine)

    tables, _ = lax.optimization_barrier((tables, queries))
    tap_rows = [conv_taps[n].astype(jnp.float32) for n in range(conv_taps.shape[0])]
    rows, tap_rows, _ = lax.optimization_barrier((rows, tap_rows, queries))
    if split_rows:
        tables = sum(place.tp_gather(tables), [])

    latent = pl.pallas_call(
        functools.partial(latent_kernel, place, rank, split_rows),
        out_shape=jax.ShapeDtypeStruct((outer * share, rank + QK_ROPE), bf16),
        in_specs=[whole_vmem()] * (outer + len(tables) + 3),
        out_specs=whole_vmem(),
        scratch_shapes=[
            pltpu.VMEM((outer * share, model), bf16),
            pltpu.VMEM((model, rank + QK_ROPE), bf16),
        ],
        compiler_params=pltpu.CompilerParams(vmem_limit_bytes=16 << 20),
        cost_estimate=pl.CostEstimate(
            flops=2 * outer * share * model * (rank + QK_ROPE),
            bytes_accessed=2 * model * (rank + QK_ROPE + outer * share),
            transcendentals=0,
        ),
        name="latents",
    )(*rows, *tables, latent_norm_gain[None, :], cosine, sine)
    _, *weight_blocks = lax.optimization_barrier((latent, *weight_blocks))
    latents = place.inner_gather(latent)
    own = place.tp_gather(latents[:1])
    others = place.tp_gather(latents[1:])
    latents = sum([a + b for a, b in zip(own, others)], [])

    all_rows = sum(place.tp_gather(rows), [])
    gated = pl.pallas_call(
        functools.partial(gated_kernel, place),
        out_shape=[jax.ShapeDtypeStruct((row_count, width), bf16)] * outer,
        in_specs=[whole_vmem()] * (len(all_rows) + inner),
        out_specs=[whole_vmem()] * outer,
        scratch_shapes=[
            pltpu.VMEM((outer * row_count, model), bf16),
            pltpu.VMEM((model, 2 * width), bf16),
        ],
        compiler_params=pltpu.CompilerParams(vmem_limit_bytes=24 << 20),
        cost_estimate=pl.CostEstimate(
            flops=4 * outer * row_count * model * width,
            bytes_accessed=2 * model * (2 * width + outer * row_count),
            transcendentals=outer * row_count * width,
        ),
        name="gated",
    )(*all_rows, *weight_blocks)
    home = [gated[0]] + [place.outer_swap(gated[j], j) for j in range(1, outer)]
    gated_rows = jnp.zeros((row_count, outer * width), bf16)
    for j in range(outer):
        gated_rows = lax.dynamic_update_slice_in_dim(gated_rows, home[j], (zi ^ j) * width, 1)

    conv_reach = conv_taps.shape[0] - 1
    prior_rows = lax.ppermute(
        gated_rows[row_count - conv_reach :],
        "sp",
        [(i, i + 1) for i in range(place.sp_count - 1)],
    )
    score_scale = (PLAIN_QK_WIDTH + QK_ROPE) ** (-0.5)
    key_total = place.sp_count * row_count
    attention, log_sums = pl.pallas_call(
        functools.partial(attention_kernel, place, score_scale, rank),
        out_shape=[
            jax.ShapeDtypeStruct((row_count, head_count * VALUE_HEAD_WIDTH), bf16),
            jax.ShapeDtypeStruct((head_count, row_count), jnp.float32),
        ],
        in_specs=[whole_vmem()] * (2 + len(latents)),
        out_specs=[whole_vmem()] * 2,
        scratch_shapes=[
            pltpu.VMEM((key_total, rank + QK_ROPE), bf16),
        ],
        compiler_params=pltpu.CompilerParams(vmem_limit_bytes=32 << 20),
        cost_estimate=pl.CostEstimate(
            flops=2 * row_count * head_count * key_total * (2 * rank + QK_ROPE),
            bytes_accessed=2 * key_total * (rank + QK_ROPE),
            transcendentals=row_count * head_count * key_total,
        ),
        name="attention",
    )(queries, value_up_weight, *latents)

    prior_rows, gated_rows, _ = lax.optimization_barrier((prior_rows, gated_rows, attention))
    padded = jnp.concatenate([prior_rows, gated_rows], axis=0).astype(jnp.float32)
    mixed = jnp.zeros(gated_rows.shape, jnp.float32)
    for tap_index in range(conv_taps.shape[0]):
        mixed = (
            mixed
            + tap_rows[tap_index] * padded[tap_index : tap_index + row_count]
        )
    channel_total = mixed.shape[1] * tp_count
    stats = jnp.stack([jnp.sum(mixed, axis=1), jnp.sum(mixed * mixed, axis=1)])
    stats, attention = lax.optimization_barrier((stats, attention))
    attn_part = jnp.dot(attention, w_merge_attn, preferred_element_type=jnp.float32)
    stat_sum, stat_squares = sum(
        [place.tp_shift(stats, t) for t in range(1, tp_count)], start=stats
    )
    channel_mean = stat_sum / channel_total
    channel_var = stat_squares / channel_total - channel_mean * channel_mean
    conv_out = jax.nn.silu(
        (mixed - channel_mean[:, None]) * lax.rsqrt(channel_var + epsilon)[:, None] * conv_gain
    ).astype(bf16)

    partial = (
        attn_part + jnp.dot(conv_out, w_merge_conv, preferred_element_type=jnp.float32)
    ).astype(bf16)
    merged = lax.dynamic_slice_in_dim(partial, ti * share, share, 0).astype(jnp.float32)
    for t in range(1, tp_count):
        away = lax.dynamic_slice_in_dim(partial, lax.rem(ti + t, tp_count) * share, share, 0)
        merged = merged + place.tp_shift(away, t).astype(jnp.float32)
    return (merged.astype(bf16), log_sums.T)


def solution(mesh):
    return jax.shard_map(
        local,
        mesh=mesh,
        in_specs=(
            P("sp", "tp"),
            P(),
            P("sp", "tp"),
            P("sp", "tp"),
            P(None, "tp"),
            P("tp"),
            P(None, "tp"),
            P("sp", None),
            P(),
            P("sp", None),
            P(None, "tp"),
            P(None, "tp"),
            P("tp", None),
            P("tp", None),
        ),
        out_specs=(P(("sp", "tp"), None), P("sp", "tp")),
        check_vma=False,
    )
```

```python
import functools
import math

import jax
import jax.numpy as jnp
from jax import lax
from jax.experimental import pallas as pl
from jax.experimental.pallas import tpu as pltpu
from jax.sharding import PartitionSpec as P


PLAIN_QK_WIDTH = 128
QK_ROPE = 64
VALUE_HEAD_WIDTH = 128


epsilon = 1e-06
rope_base = 10000.0
masked_score = -1e30


def angles_at(positions, width):
    inverse = rope_base ** (-2.0 * jnp.arange(width // 2, dtype=jnp.float32) / width)
    return positions[:, None] * inverse[None, :]


class Place:
    def __init__(self):
        self.sp_count = lax.axis_size("sp")
        self.tp_count = lax.axis_size("tp")
        self.inner = math.gcd(self.sp_count, 4)
        self.outer = self.sp_count // self.inner

    def indices(self):
        index = lax.axis_index("sp")
        return index // self.inner, index % self.inner, lax.axis_index("tp")

    def outer_swap(self, block, mask):
        mask = mask * self.inner
        return lax.ppermute(block, "sp", [(i, i ^ mask) for i in range(self.sp_count)])

    def inner_swap(self, block, mask):
        return lax.ppermute(block, "sp", [(i, i ^ mask) for i in range(self.sp_count)])

    def tp_shift(self, block, distance):
        route = [(i, (i + distance) % self.tp_count) for i in range(self.tp_count)]
        return lax.ppermute(block, "tp", route)

    def outer_gather(self, block):
        return [block] + [self.outer_swap(block, j) for j in range(1, self.outer)]

    def outer_forward(self, block):
        blocks = [block]
        for j in range(1, self.outer):
            near = j & -j
            blocks.append(self.outer_swap(blocks[j ^ near], near))
        return blocks

    def inner_gather(self, block):
        return [block] + [self.inner_swap(block, k) for k in range(1, self.inner)]

    def tp_gather(self, blocks):
        return [blocks] + [
            [self.tp_shift(b, t) for b in blocks] for t in range(1, self.tp_count)
        ]


def behind(index, distance, count):
    return lax.rem(index - distance + count, count)


def copy_all(pairs, sem):
    copies = [pltpu.make_async_copy(s, d, sem.at[n]) for n, (s, d) in enumerate(pairs)]
    for c in copies:
        c.start()
    return copies


def whole_vmem():
    return pl.BlockSpec(memory_space=pltpu.VMEM)


def turned(first, second, cosine, sine):
    return jnp.concatenate(
        [first * cosine - second * sine, first * sine + second * cosine], axis=-1
    ).astype(jnp.bfloat16)


def query_kernel(rank, normed_ref, w_ref, up_ref, cos_ref, sin_ref, out_ref, w, up, sem):
    heads, count, _ = out_ref.shape
    plain, half = PLAIN_QK_WIDTH, QK_ROPE // 2
    head = plain + QK_ROPE
    span = 2 * head
    pairs = heads // 2
    copies = copy_all(
        [
            (w_ref.at[:, p * span : (p + 1) * span], w.at[:, p * span : (p + 1) * span])
            for p in range(pairs)
        ]
        + [(up_ref, up)],
        sem,
    )
    cosine, sine = cos_ref[:count], sin_ref[:count]
    for p in range(pairs):
        copies[p].wait()
        query = jnp.dot(
            normed_ref[...], w[:, p * span : (p + 1) * span], preferred_element_type=jnp.float32
        ).astype(jnp.bfloat16)
        if p == 0:
            copies[pairs].wait()
        for i in range(2):
            h = 2 * p + i
            own = query[:, i * head : (i + 1) * head]
            out_ref[h, :, :rank] = lax.dot_general(
                own[:, :plain],
                up[:, h * plain : (h + 1) * plain],
                (((1,), (1,)), ((), ())),
                preferred_element_type=jnp.float32,
            ).astype(jnp.bfloat16)
            rope = own[:, plain:].astype(jnp.float32)
            out_ref[h, :, rank:] = turned(rope[:, :half], rope[:, half:], cosine, sine)


def latent_kernel(place, rank, share, *refs):
    outer, inner, tp = place.outer, place.inner, place.tp_count
    tables = tp if share else 1
    n_rows, n_w = outer, tables * inner
    row_refs, w_refs = refs[:n_rows], refs[n_rows : n_rows + n_w]
    gain_ref, cos_ref, sin_ref, out_ref, rows, weight = refs[n_rows + n_w :]
    zi, xi, ti = place.indices()
    piece = w_refs[0].shape[1]
    block = piece * tables
    count = row_refs[0].shape[0]
    for t in range(tables):
        owner = behind(ti, t, tp) if share else 0
        for k in range(inner):
            for j in range(outer):
                start = ((zi ^ j) * inner + (xi ^ k)) * block + owner * piece
                weight[pl.ds(pl.multiple_of(start, piece), piece)] = w_refs[t * inner + k][j]
    for j in range(outer):
        rows[j * count : (j + 1) * count] = row_refs[j][...]
    pre = jnp.dot(rows[...], weight[...], preferred_element_type=jnp.float32)
    plain = pre[:, :rank]
    scale = lax.rsqrt(jnp.mean(plain * plain, axis=-1, keepdims=True) + epsilon)
    out_ref[:, :rank] = (plain * scale * gain_ref[...]).astype(jnp.bfloat16)
    rope = pre[:, rank:]
    half = rope.shape[1] // 2
    total = outer * count
    cosine, sine = cos_ref[cos_ref.shape[0] - total :], sin_ref[sin_ref.shape[0] - total :]
    out_ref[:, rank:] = turned(rope[:, :half], rope[:, half:], cosine, sine)


def gated_kernel(place, *refs):
    outer, inner, tp = place.outer, place.inner, place.tp_count
    n_rows = tp * outer
    row_refs, w_refs = refs[:n_rows], refs[n_rows : n_rows + inner]
    outs = refs[n_rows + inner : n_rows + inner + outer]
    rows, weight = refs[n_rows + inner + outer :]
    zi, xi, ti = place.indices()
    block = w_refs[0].shape[1]
    count = row_refs[0].shape[0]
    for k in range(inner):
        for j in range(outer):
            start = ((zi ^ j) * inner + (xi ^ k)) * block
            weight[pl.ds(pl.multiple_of(start, block), block)] = w_refs[k][j]
    for t in range(tp):
        owner = behind(ti, t, tp)
        for j in range(outer):
            start = j * tp * count + owner * count
            rows[pl.ds(pl.multiple_of(start, count), count)] = row_refs[t * outer + j][...]
    chunk = tp * count
    width = outs[0].shape[1]
    pre = jnp.dot(rows[...], weight[...], preferred_element_type=jnp.float32)
    for j in range(outer):
        part = pre[j * chunk : (j + 1) * chunk]
        value, gate = part[:, :width], part[:, width:]
        outs[j][...] = (value * jax.nn.sigmoid(gate)).astype(jnp.bfloat16)


def attention_kernel(place, scale, rank, q_ref, upper_ref, *refs):
    outer, inner, tp = place.outer, place.inner, place.tp_count
    n_k = tp * inner
    key_refs = refs[:n_k]
    out_ref, lse_ref, keys, up_ref, sem = refs[n_k:]
    up_copy = pltpu.make_async_copy(upper_ref, up_ref, sem.at[n_k])
    up_copy.start()
    zi, xi, ti = place.indices()
    heads, count, depth = q_ref.shape
    piece = key_refs[0].shape[0]
    share = piece // outer
    early = n_k // tp
    copies = copy_all(
        [(key_refs[n], keys.at[n * piece : (n + 1) * piece]) for n in range(early, n_k)], sem
    )
    for n in range(early):
        keys[n * piece : (n + 1) * piece] = key_refs[n][...]
    lane = lax.broadcasted_iota(jnp.int32, (1, piece), 1)
    back = zi ^ lax.shift_right_logical(lane, share.bit_length() - 1)
    within = jnp.bitwise_and(lane, share - 1)
    parts = []
    for t in range(tp):
        owner = behind(ti, t, tp)
        for k in range(inner):
            parts.append((back * inner + (xi ^ k)) * count + owner * share + within)
    key_index = jnp.concatenate(parts, axis=1)
    first_row = (zi * inner + xi) * count
    together = math.gcd(heads, 4)
    size = together * count
    query_index = lax.broadcasted_iota(jnp.int32, (count, 1), 0) + first_row
    allowed = key_index <= jnp.concatenate([query_index] * together, axis=0)
    width = VALUE_HEAD_WIDTH
    sums = []
    for g in range(heads // together):
        queries = q_ref[g * together : (g + 1) * together].reshape(size, depth)
        scores = []
        for n in range(tp):
            if g == 0 and n == 1:
                for c in copies:
                    c.wait()
            scores.append(
                lax.dot_general(
                    queries,
                    keys[n * early * piece : (n + 1) * early * piece],
                    (((1,), (1,)), ((), ())),
                    preferred_element_type=jnp.float32,
                )
            )
        scores = jnp.concatenate(scores, axis=1)
        scores = jnp.where(allowed, scores, masked_score)
        top = jnp.max(scores, axis=-1, keepdims=True)
        weights = jnp.exp2((scores - top) * (scale * math.log2(math.e)))
        total = jnp.sum(weights, axis=-1, keepdims=True)
        weighted = jnp.dot(
            weights.astype(jnp.bfloat16), keys[:, :rank], preferred_element_type=jnp.float32
        )
        if g == 0:
            up_copy.wait()
        latent_out = (weighted / total).astype(jnp.bfloat16)
        group_sums = top * scale + jnp.log(total)
        for i in range(together):
            h = g * together + i
            part = slice(i * count, (i + 1) * count)
            sums.append(group_sums[part])
            out_ref[:, h * width : (h + 1) * width] = jnp.dot(
                latent_out[part],
                up_ref[:, h * width : (h + 1) * width],
                preferred_element_type=jnp.float32,
            ).astype(jnp.bfloat16)
    spare = [jnp.zeros((count, 128 - heads), jnp.float32)]
    lse_ref[...] = jnp.concatenate(sums + spare, axis=1).T[:heads]


def local(
    tokens,
    norm_gain,
    w_value,
    w_gate,
    conv_taps,
    conv_gain,
    w_query,
    latent_down_weight,
    latent_norm_gain,
    w_rope_key,
    key_up_weight,
    value_up_weight,
    w_merge_conv,
    w_merge_attn,
):
    place = Place()
    outer, inner, tp_count = place.outer, place.inner, place.tp_count
    zi, xi, ti = place.indices()
    row_count = tokens.shape[0]
    share = row_count // tp_count
    depth = latent_down_weight.shape[0]
    rank = latent_down_weight.shape[1]

    split_rows = depth % (16 * tp_count) == 0
    own_table = jnp.concatenate([latent_down_weight, w_rope_key], axis=1)
    if split_rows:
        piece = depth // tp_count
        own_table = lax.dynamic_slice_in_dim(own_table, ti * piece, piece, 0)
    own_table, w_value, w_gate = lax.optimization_barrier((own_table, w_value, w_gate))
    table_parts = place.outer_gather(own_table)

    width = w_value.shape[1] // outer
    columns = []
    for j in range(outer):
        start = (zi ^ j) * width
        block = jnp.concatenate(
            [
                lax.dynamic_slice_in_dim(w_value, start, width, 1),
                lax.dynamic_slice_in_dim(w_gate, start, width, 1),
            ],
            axis=1,
        )
        columns.append(block if j == 0 else place.outer_swap(block, j))

    table = jnp.stack(table_parts)
    table, tokens = lax.optimization_barrier((table, tokens))
    tables = place.inner_gather(table)

    gathered = lax.all_gather(tokens, "tp", axis=1, tiled=True)
    features = gathered.astype(jnp.float32)
    normed = (
        features
        * lax.rsqrt(jnp.mean(features * features, axis=-1, keepdims=True) + epsilon)
        * norm_gain
    ).astype(jnp.bfloat16)

    own_rows = lax.dynamic_slice_in_dim(normed, ti * share, share, 0)
    rows = place.outer_forward(own_rows)
    weight_block = jnp.stack(columns)
    weight_block, query_rows = lax.optimization_barrier((weight_block, normed))
    weight_blocks = place.inner_gather(weight_block)

    bf16 = jnp.bfloat16
    model = normed.shape[1]
    head_count = key_up_weight.shape[1] // PLAIN_QK_WIDTH
    query_index = lax.axis_index("sp") * row_count + jnp.arange(row_count, dtype=jnp.int32)
    back = zi ^ jnp.arange(outer, dtype=jnp.int32)
    key_index = (
        ((back * inner + xi) * row_count + ti * share)[:, None]
        + jnp.arange(share, dtype=jnp.int32)[None, :]
    ).reshape(-1)
    angles = angles_at(
        jnp.concatenate([query_index, key_index]).astype(jnp.float32), QK_ROPE
    )
    cosine, sine = jnp.cos(angles), jnp.sin(angles)

    query_width = w_query.shape[1]
    queries = pl.pallas_call(
        functools.partial(query_kernel, rank),
        out_shape=jax.ShapeDtypeStruct((head_count, row_count, rank + QK_ROPE), bf16),
        in_specs=[whole_vmem()] + [pl.BlockSpec(memory_space=pltpu.HBM)] * 2 + [whole_vmem()] * 2,
        out_specs=whole_vmem(),
        scratch_shapes=[
            pltpu.VMEM((model, query_width), bf16),
            pltpu.VMEM(key_up_weight.shape, bf16),
            pltpu.SemaphoreType.DMA((head_count // 2 + 1,)),
        ],
        compiler_params=pltpu.CompilerParams(vmem_limit_bytes=52 << 20),
        cost_estimate=pl.CostEstimate(
            flops=2 * row_count * model * query_width,
            bytes_accessed=2 * model * query_width,
            transcendentals=0,
        ),
        name="queries",
    )(query_rows, w_query, key_up_weight, cosine, sine)

    tables, _ = lax.optimization_barrier((tables, queries))
    tap_rows = [conv_taps[n].astype(jnp.float32) for n in range(conv_taps.shape[0])]
    rows, tap_rows, _ = lax.optimization_barrier((rows, tap_rows, queries))
    if split_rows:
        tables = sum(place.tp_gather(tables), [])

    latent = pl.pallas_call(
        functools.partial(latent_kernel, place, rank, split_rows),
        out_shape=jax.ShapeDtypeStruct((outer * share, rank + QK_ROPE), bf16),
        in_specs=[whole_vmem()] * (outer + len(tables) + 3),
        out_specs=whole_vmem(),
        scratch_shapes=[
            pltpu.VMEM((outer * share, model), bf16),
            pltpu.VMEM((model, rank + QK_ROPE), bf16),
        ],
        compiler_params=pltpu.CompilerParams(vmem_limit_bytes=16 << 20),
        cost_estimate=pl.CostEstimate(
            flops=2 * outer * share * model * (rank + QK_ROPE),
            bytes_accessed=2 * model * (rank + QK_ROPE + outer * share),
            transcendentals=0,
        ),
        name="latents",
    )(*rows, *tables, latent_norm_gain[None, :], cosine, sine)
    _, *weight_blocks = lax.optimization_barrier((latent, *weight_blocks))
    latents = place.inner_gather(latent)
    own = place.tp_gather(latents[:1])
    others = place.tp_gather(latents[1:])
    latents = sum([a + b for a, b in zip(own, others)], [])

    all_rows = sum(place.tp_gather(rows), [])
    gated = pl.pallas_call(
        functools.partial(gated_kernel, place),
        out_shape=[jax.ShapeDtypeStruct((row_count, width), bf16)] * outer,
        in_specs=[whole_vmem()] * (len(all_rows) + inner),
        out_specs=[whole_vmem()] * outer,
        scratch_shapes=[
            pltpu.VMEM((outer * row_count, model), bf16),
            pltpu.VMEM((model, 2 * width), bf16),
        ],
        compiler_params=pltpu.CompilerParams(vmem_limit_bytes=24 << 20),
        cost_estimate=pl.CostEstimate(
            flops=4 * outer * row_count * model * width,
            bytes_accessed=2 * model * (2 * width + outer * row_count),
            transcendentals=outer * row_count * width,
        ),
        name="gated",
    )(*all_rows, *weight_blocks)
    home = [gated[0]] + [place.outer_swap(gated[j], j) for j in range(1, outer)]
    gated_rows = jnp.zeros((row_count, outer * width), bf16)
    for j in range(outer):
        gated_rows = lax.dynamic_update_slice_in_dim(gated_rows, home[j], (zi ^ j) * width, 1)

    conv_reach = conv_taps.shape[0] - 1
    prior_rows = lax.ppermute(
        gated_rows[row_count - conv_reach :],
        "sp",
        [(i, i + 1) for i in range(place.sp_count - 1)],
    )
    score_scale = (PLAIN_QK_WIDTH + QK_ROPE) ** (-0.5)
    key_total = place.sp_count * row_count
    attention, log_sums = pl.pallas_call(
        functools.partial(attention_kernel, place, score_scale, rank),
        out_shape=[
            jax.ShapeDtypeStruct((row_count, head_count * VALUE_HEAD_WIDTH), bf16),
            jax.ShapeDtypeStruct((head_count, row_count), jnp.float32),
        ],
        in_specs=[whole_vmem()]
        + [pl.BlockSpec(memory_space=pl.ANY)]
        + [whole_vmem()] * inner
        + [pl.BlockSpec(memory_space=pl.ANY)] * (len(latents) - inner),
        out_specs=[whole_vmem()] * 2,
        scratch_shapes=[
            pltpu.VMEM((key_total, rank + QK_ROPE), bf16),
            pltpu.VMEM(value_up_weight.shape, bf16),
            pltpu.SemaphoreType.DMA((len(latents) + 1,)),
        ],
        compiler_params=pltpu.CompilerParams(vmem_limit_bytes=32 << 20),
        cost_estimate=pl.CostEstimate(
            flops=2 * row_count * head_count * key_total * (2 * rank + QK_ROPE),
            bytes_accessed=2 * key_total * (rank + QK_ROPE),
            transcendentals=row_count * head_count * key_total,
        ),
        name="attention",
    )(queries, value_up_weight, *latents)

    prior_rows, gated_rows, _ = lax.optimization_barrier((prior_rows, gated_rows, attention))
    padded = jnp.concatenate([prior_rows, gated_rows], axis=0).astype(jnp.float32)
    mixed = jnp.zeros(gated_rows.shape, jnp.float32)
    for tap_index in range(conv_taps.shape[0]):
        mixed = (
            mixed
            + tap_rows[tap_index] * padded[tap_index : tap_index + row_count]
        )
    channel_total = mixed.shape[1] * tp_count
    stats = jnp.stack([jnp.sum(mixed, axis=1), jnp.sum(mixed * mixed, axis=1)])
    stats, attention = lax.optimization_barrier((stats, attention))
    attn_part = jnp.dot(attention, w_merge_attn, preferred_element_type=jnp.float32)
    stat_sum, stat_squares = sum(
        [place.tp_shift(stats, t) for t in range(1, tp_count)], start=stats
    )
    channel_mean = stat_sum / channel_total
    channel_var = stat_squares / channel_total - channel_mean * channel_mean
    conv_out = jax.nn.silu(
        (mixed - channel_mean[:, None]) * lax.rsqrt(channel_var + epsilon)[:, None] * conv_gain
    ).astype(bf16)

    partial = (
        attn_part + jnp.dot(conv_out, w_merge_conv, preferred_element_type=jnp.float32)
    ).astype(bf16)
    merged = lax.dynamic_slice_in_dim(partial, ti * share, share, 0).astype(jnp.float32)
    for t in range(1, tp_count):
        away = lax.dynamic_slice_in_dim(partial, lax.rem(ti + t, tp_count) * share, share, 0)
        merged = merged + place.tp_shift(away, t).astype(jnp.float32)
    return (merged.astype(bf16), log_sums.T)


def solution(mesh):
    return jax.shard_map(
        local,
        mesh=mesh,
        in_specs=(
            P("sp", "tp"),
            P(),
            P("sp", "tp"),
            P("sp", "tp"),
            P(None, "tp"),
            P("tp"),
            P(None, "tp"),
            P("sp", None),
            P(),
            P("sp", None),
            P(None, "tp"),
            P(None, "tp"),
            P("tp", None),
            P("tp", None),
        ),
        out_specs=(P(("sp", "tp"), None), P("sp", "tp")),
        check_vma=False,
    )
```
